32 devices in a mesh: sp: 4 (over z), fs: 4 (over y, x), tp: 2 (over core).
Axes of the slice: x: 2, y: 2, z: 4, core: 2. Of those that a mesh axis runs over, the one named last changes fastest.
Arguments:
- state_head_inputs: bfloat16 [4, 512, 1024], P('fs', 'sp', 'tp'), may hold values from -6 to 6
- state_write_vectors: bfloat16 [4, 512, 256], P('fs', 'sp', 'tp'), may hold values from -3 to 3
- state_read_vectors: bfloat16 [4, 512, 256], P('fs', 'sp', 'tp'), may hold values from -3 to 3
- state_output_gate: bfloat16 [4, 512, 1024], P('fs', 'sp', 'tp'), may hold values from -6 to 6
- presoftplus_steps: float32 [4, 16, 512], P('fs', 'tp', 'sp'), may hold values from -6 to 6
- extra_decay_log: float32 [4, 16, 512], P('fs', 'tp', 'sp'), may hold values from -2.1 to 0, as said below
- lane_shrinkage_powers: float32 [16], P('tp')
- bypass_coefficient_vector: float32 [16], P('tp'), may hold values from 0.5 to 4
- feeder_smoothing_stencil: bfloat16 [4, 1024], P(None, 'tp'), may hold values from -3 to 3
- stored_smoothing_stencil: bfloat16 [4, 256], P(None, 'tp'), may hold values from -3 to 3
- lookup_smoothing_stencil: bfloat16 [4, 256], P(None, 'tp'), may hold values from -3 to 3
- bundled_rescaling_vector: float32 [1024], P('tp'), may hold values from 0.1 to 1.9
- queries: bfloat16 [4, 512, 1024], P('fs', 'sp', 'tp'), may hold values from -8 to 8
- attention_keys: bfloat16 [4, 512, 256], P('fs', 'sp', 'tp'), may hold values from -8 to 8
- attention_values: bfloat16 [4, 512, 256], P('fs', 'sp', 'tp'), may hold values from -6 to 6
- forget_gate_cumsum: float32 [4, 512, 16], P('fs', 'sp', 'tp'), as said below
- state_out_weight: bfloat16 [1024, 2048], P('tp', 'fs'), may hold values from -0.1875 to 0.1875
- attention_out_weight: bfloat16 [1024, 2048], P('tp', 'fs'), may hold values from -0.75 to 0.75
Outputs:
- layer_output: bfloat16 [4, 512, 2048], P('fs', ('sp', 'tp'))
The draws below stay inside these ranges and needn't reach their ends.
Inputs may be any that keep to these rules, and one draw needn't show every extreme that they name: `extra_decay_log`: nonpositive. `forget_gate_cumsum`: never rises along the positions of a sequence.
All inputs are finite; a program needn't handle non-finite values.
Results may differ from the reference program's by a relative error of at most 0.019.
Values may be sent and summed in bfloat16 or wider, within the bound.
A program may use at most 64 MiB of HBM per device.

```python
import math
import jax
import jax.numpy as jnp
from jax import lax

D = 2048
SPACE_MODEL_LANES = 16
FOX_QUESTIONERS = 16
KV_HEADS = 4
HEAD_DIM = 64
STATE = 128
GROUPS = 2
CONV = 4
TOKENS_PER_SHARD = 128
SEQS = 4
LENGTH = 512
SSD_WIDTH = 1024
FOX_WIDTH = 1024


def fast_rate():
    return 1.0 / min(40, max(TOKENS_PER_SHARD // 4, 2))


def head_rates(plain_quantity, lane_tally):
    order_key, slow_key, quick_key = jax.random.split(plain_quantity, 3)
    order = jax.random.permutation(order_key, lane_tally)
    lingering_shrinkage = order < lane_tally // 2
    slow_rate = jax.random.uniform(slow_key, (lane_tally,), jnp.float32, 0.1, 0.6) / LENGTH
    quick = fast_rate() * jnp.exp(jax.random.uniform(quick_key, (lane_tally,), jnp.float32, -0.35, 0.35))
    return (jnp.where(lingering_shrinkage, slow_rate, quick), lingering_shrinkage)


def sudden_line_selector(plain_quantity, lane_tally):
    place_key, depth_key = jax.random.split(plain_quantity, 2)
    places = jax.random.randint(place_key, (SEQS, lane_tally, 3), 0, LENGTH)
    depth = jnp.log(jax.random.uniform(depth_key, (SEQS, lane_tally, 3), jnp.float32, 0.5, 0.8))
    positions = jnp.arange(LENGTH)
    hits = positions[None, None, None, :] == places[..., None]
    return jnp.sum(jnp.where(hits, depth[..., None], 0.0), axis=2)


def drawn_pairs(key):
    plain_quantity = jax.random.fold_in(key, 7)
    query_key, keys_key = jax.random.split(plain_quantity, 2)
    queries = jnp.clip(jax.random.normal(query_key, (SEQS, LENGTH, FOX_QUESTIONERS * HEAD_DIM), jnp.float32), -6.0, 6.0)
    keys = jnp.clip(jax.random.normal(keys_key, (SEQS, LENGTH, KV_HEADS * HEAD_DIM), jnp.float32), -6.0, 6.0)
    return (queries.astype(jnp.bfloat16), keys.astype(jnp.bfloat16))


def draw_queries(key, part):
    return drawn_pairs(key)[0]


def draw_attention_keys(key, part):
    return drawn_pairs(key)[1]


def draw_forget_gate_cumsum(key, part):
    plain_quantity = jax.random.fold_in(key, 31)
    ratio_generator, portion_generator, sample_generator_start, sudden_generator = jax.random.split(plain_quantity, 4)
    shrinkage_ratios, lingering_shrinkage = head_rates(ratio_generator, FOX_QUESTIONERS)
    blocks = LENGTH // TOKENS_PER_SHARD
    stretch_coefficient = jnp.exp(jax.random.uniform(portion_generator, (SEQS, blocks, FOX_QUESTIONERS), jnp.float32, math.log(0.5), math.log(2.0)))
    stretch_coefficient = jnp.repeat(stretch_coefficient, TOKENS_PER_SHARD, axis=1)
    scatter_breadth = jnp.exp(0.7 * jnp.clip(jax.random.normal(sample_generator_start, (SEQS, LENGTH, FOX_QUESTIONERS), jnp.float32), -4.0, 4.0))
    sudden_arrivals = sudden_line_selector(sudden_generator, FOX_QUESTIONERS).transpose(0, 2, 1) * lingering_shrinkage.astype(jnp.float32)
    return jnp.cumsum(-shrinkage_ratios * stretch_coefficient * scatter_breadth + sudden_arrivals, axis=1)


def draw_lane_shrinkage_powers(key, part):
    shrinkage_ratios, _ = head_rates(jax.random.fold_in(key, 41), SPACE_MODEL_LANES)
    return jnp.log(shrinkage_ratios)


def draw_presoftplus_steps(key, part):
    plain_quantity = jax.random.fold_in(key, 47)
    offset_key, noise_key = jax.random.split(plain_quantity, 2)
    blocks = LENGTH // TOKENS_PER_SHARD
    offset = jax.random.uniform(offset_key, (SEQS, SPACE_MODEL_LANES, blocks), jnp.float32, -1.2, 1.2)
    offset = jnp.repeat(offset, TOKENS_PER_SHARD, axis=2)
    noise = jnp.clip(jax.random.normal(noise_key, (SEQS, SPACE_MODEL_LANES, LENGTH), jnp.float32), -4.0, 4.0)
    return offset + 0.8 * noise


def draw_extra_decay_log(key, part):
    return sudden_line_selector(jax.random.fold_in(key, 53), SPACE_MODEL_LANES)


def block_levels(key, extent, cuts, smallest, largest):
    def one(dim, blocks):
        draws = jax.random.uniform(jax.random.fold_in(jax.random.fold_in(key, 6), dim), (blocks,), jnp.float32, smallest / len(cuts), largest / len(cuts))
        return jnp.repeat(jnp.exp(draws), extent[dim] // blocks).reshape((-1,) + (1,) * (len(extent) - dim - 1))

    gain = one(*cuts[0])
    for cut in cuts[1:]:
        gain = gain * one(*cut)
    return gain


def gaussian(key, extent, scale, limit, cuts=(), held_as=jnp.bfloat16):
    gain = block_levels(key, extent, cuts, -0.22, 0.18) if cuts else 1.0
    drawn = jax.random.normal(key, extent, jnp.float32) * scale * gain
    return jnp.minimum(jnp.maximum(drawn, -limit), limit).astype(held_as)


def setup_inputs(seed: int = 0) -> dict:
    key_list = jax.random.split(jax.random.key(seed), 19)
    state_head_inputs = gaussian(key_list[0], (SEQS, LENGTH, SSD_WIDTH), 1.0, 6.0, ((0, 4), (1, 4), (2, 2)))
    state_write_vectors = gaussian(key_list[1], (SEQS, LENGTH, GROUPS * STATE), 0.5, 3.0, ((0, 4), (1, 4), (2, 2)))
    state_read_vectors = gaussian(key_list[2], (SEQS, LENGTH, GROUPS * STATE), 0.5, 3.0, ((0, 4), (1, 4), (2, 2)))
    state_output_gate = gaussian(key_list[3], (SEQS, LENGTH, SSD_WIDTH), 1.0, 6.0, ((0, 4), (1, 4), (2, 2)))
    presoftplus_steps = draw_presoftplus_steps(jax.random.fold_in(key_list[18], 71), 0)
    extra_decay_log = draw_extra_decay_log(jax.random.fold_in(key_list[18], 71), 0)
    lane_shrinkage_powers = draw_lane_shrinkage_powers(jax.random.fold_in(key_list[18], 71), 0)
    bypass_coefficient_vector = jnp.clip(jnp.exp(math.log(4.0) - 2.0794415 * jax.random.uniform(key_list[7], (SPACE_MODEL_LANES,), jnp.float32) ** block_levels(key_list[7], (SPACE_MODEL_LANES,), ((0, 2),), -0.2, 0.2)), 0.5, 4.0)
    feeder_smoothing_stencil = gaussian(key_list[8], (CONV, SSD_WIDTH), CONV ** -0.5, 3.0, ((1, 2),))
    stored_smoothing_stencil = gaussian(key_list[9], (CONV, GROUPS * STATE), CONV ** -0.5, 3.0, ((1, 2),))
    lookup_smoothing_stencil = gaussian(key_list[10], (CONV, GROUPS * STATE), CONV ** -0.5, 3.0, ((1, 2),))
    bundled_rescaling_vector = jnp.clip(1.0 + 0.18 * jax.random.normal(key_list[11], (SSD_WIDTH,), jnp.float32), 0.1, 1.9)
    queries = draw_queries(jax.random.fold_in(key_list[18], 71), 0)
    attention_keys = draw_attention_keys(jax.random.fold_in(key_list[18], 71), 0)
    attention_values = gaussian(key_list[14], (SEQS, LENGTH, KV_HEADS * HEAD_DIM), 1.0, 6.0, ((0, 4), (1, 4), (2, 2)))
    forget_gate_cumsum = draw_forget_gate_cumsum(jax.random.fold_in(key_list[18], 71), 0)
    state_out_weight = gaussian(key_list[16], (SSD_WIDTH, D), SSD_WIDTH ** -0.5, 0.1875, ((0, 2), (1, 4)))
    attention_out_weight = gaussian(key_list[17], (FOX_WIDTH, D), HEAD_DIM ** -0.5, 0.75, ((0, 2), (1, 4)))
    return {"state_head_inputs": state_head_inputs, "state_write_vectors": state_write_vectors, "state_read_vectors": state_read_vectors, "state_output_gate": state_output_gate, "presoftplus_steps": presoftplus_steps, "extra_decay_log": extra_decay_log, "lane_shrinkage_powers": lane_shrinkage_powers, "bypass_coefficient_vector": bypass_coefficient_vector, "feeder_smoothing_stencil": feeder_smoothing_stencil, "stored_smoothing_stencil": stored_smoothing_stencil, "lookup_smoothing_stencil": lookup_smoothing_stencil, "bundled_rescaling_vector": bundled_rescaling_vector, "queries": queries, "attention_keys": attention_keys, "attention_values": attention_values, "forget_gate_cumsum": forget_gate_cumsum, "state_out_weight": state_out_weight, "attention_out_weight": attention_out_weight}


EPSILON = 1e-06
NEGATIVE = -1e+30

def rounded_value(values):
    return lax.optimization_barrier(values.astype(jnp.bfloat16)).astype(jnp.float32)

def causal_filter(feeder_quantities, taps):
    length = feeder_quantities.shape[0]
    tap_count = taps.shape[0]
    padded = jnp.concatenate([jnp.zeros((tap_count - 1, feeder_quantities.shape[1]), jnp.float32), feeder_quantities.astype(jnp.float32)], axis=0)
    summed = jnp.zeros((length, feeder_quantities.shape[1]), jnp.float32)
    for offset in range(tap_count):
        summed = summed + taps[offset].astype(jnp.float32) * padded[offset:offset + length]
    return jax.nn.silu(summed).astype(jnp.bfloat16)

def memory_series_yield(feeder_quantities, stored_quantity, fetched_quantity, opening_quantity, bare_stride, sudden_arrivals, lane_shrinkage_powers, bypass_coefficient_vector, feeder_smoothing_stencil, stored_smoothing_stencil, lookup_smoothing_stencil, bundled_rescaling_vector):
    conv_values = causal_filter(feeder_quantities, feeder_smoothing_stencil)
    conv_write = causal_filter(stored_quantity, stored_smoothing_stencil)
    conv_read = causal_filter(fetched_quantity, lookup_smoothing_stencil)
    stride_duration = jax.nn.softplus(bare_stride)
    shrinkage_natural_power = stride_duration * (-jnp.exp(lane_shrinkage_powers))[:, None] + sudden_arrivals
    lane_tally = stride_duration.shape[0]
    per_group = lane_tally // GROUPS
    blocks = LENGTH // TOKENS_PER_SHARD
    positions = jnp.arange(TOKENS_PER_SHARD, dtype=jnp.int32)
    causal = positions[:, None] >= positions[None, :]

    def advance(carried, pieces):
        values, writes, reads, steps, decays = pieces
        cumulative = jnp.cumsum(decays, axis=1)
        input_heads = values.reshape(TOKENS_PER_SHARD, GROUPS, per_group, HEAD_DIM).astype(jnp.float32)
        write_groups = writes.reshape(TOKENS_PER_SHARD, GROUPS, STATE).astype(jnp.float32)
        read_groups = reads.reshape(TOKENS_PER_SHARD, GROUPS, STATE).astype(jnp.float32)
        inner_products = jnp.einsum('tgn,sgn->gts', read_groups, write_groups)
        log_gap = jnp.where(causal[None], cumulative[:, :, None] - cumulative[:, None, :], -jnp.inf)
        weights = jnp.exp(log_gap) * steps[:, None, :]
        mix_weights = rounded_value(inner_products[:, None] * weights.reshape(GROUPS, per_group, TOKENS_PER_SHARD, TOKENS_PER_SHARD))
        local_part = jnp.einsum('ghts,sghp->tghp', mix_weights, input_heads)
        end_scale = (jnp.exp(cumulative[:, -1:] - cumulative) * steps).T.reshape(TOKENS_PER_SHARD, GROUPS, per_group)
        weighted = rounded_value(input_heads * end_scale[..., None])
        block_state = jnp.einsum('sghp,sgn->ghpn', weighted, write_groups)
        total_decay = jnp.exp(cumulative[:, -1]).reshape(GROUPS, per_group)
        carried_part = jnp.einsum('tgn,ghpn->tghp', read_groups, rounded_value(carried))
        carried_part = carried_part * jnp.exp(cumulative).T.reshape(TOKENS_PER_SHARD, GROUPS, per_group)[..., None]
        mixer_sum = local_part + carried_part + bypass_coefficient_vector.reshape(GROUPS, per_group)[None, :, :, None] * input_heads
        following = total_decay[..., None, None] * carried + block_state
        return (following, mixer_sum)
    pieces = (conv_values.reshape(blocks, TOKENS_PER_SHARD, -1), conv_write.reshape(blocks, TOKENS_PER_SHARD, -1), conv_read.reshape(blocks, TOKENS_PER_SHARD, -1), stride_duration.reshape(lane_tally, blocks, TOKENS_PER_SHARD).transpose(1, 0, 2), shrinkage_natural_power.reshape(lane_tally, blocks, TOKENS_PER_SHARD).transpose(1, 0, 2))
    starting = jnp.zeros((GROUPS, per_group, HEAD_DIM, STATE), jnp.float32)
    _, sums = lax.scan(advance, starting, pieces)
    gated_rows = sums.reshape(LENGTH, GROUPS, per_group * HEAD_DIM) * jax.nn.silu(opening_quantity.astype(jnp.float32)).reshape(LENGTH, GROUPS, -1)
    stretch_coefficient = lax.rsqrt(lax.optimization_barrier(jnp.mean(gated_rows * gated_rows, axis=-1, keepdims=True)) + EPSILON)
    return (gated_rows * stretch_coefficient * bundled_rescaling_vector.reshape(GROUPS, -1)).reshape(LENGTH, -1).astype(jnp.bfloat16)

def attend_sequence(queries, keys, values, gates):
    blocks = LENGTH // TOKENS_PER_SHARD
    lane_tally = gates.shape[1]
    key_group_count = keys.shape[1] // HEAD_DIM
    repeat_factor = lane_tally // key_group_count
    query_blocks = queries.reshape(blocks, TOKENS_PER_SHARD, key_group_count, repeat_factor, HEAD_DIM)
    key_blocks = keys.reshape(blocks, TOKENS_PER_SHARD, key_group_count, HEAD_DIM)
    value_blocks = values.reshape(blocks, TOKENS_PER_SHARD, key_group_count, HEAD_DIM)
    gate_blocks = gates.reshape(blocks, TOKENS_PER_SHARD, lane_tally)
    attention_score_scale = HEAD_DIM ** (-0.5)

    def one_block(pieces):
        query_block, query_gates, block_index = pieces
        query_head_count = query_block.astype(jnp.float32)
        query_index = block_index * TOKENS_PER_SHARD + jnp.arange(TOKENS_PER_SHARD, dtype=jnp.int32)

        def advance(key_index, partial_value):
            running_max, running_sum, weighted_sum = partial_value
            key_tile = key_blocks[key_index].astype(jnp.float32)
            value_tile = value_blocks[key_index].astype(jnp.float32)
            key_gates = gate_blocks[key_index]
            attention_scores = jnp.einsum('ezxp,czp->zxec', query_head_count, key_tile).reshape(lane_tally, TOKENS_PER_SHARD, TOKENS_PER_SHARD) * attention_score_scale
            attention_scores = attention_scores + query_gates.T[:, :, None] - key_gates.T[:, None, :]
            key_place = key_index * TOKENS_PER_SHARD + jnp.arange(TOKENS_PER_SHARD, dtype=jnp.int32)
            visible = key_place[None, :] <= query_index[:, None]
            attention_scores = jnp.where(visible[None], attention_scores, NEGATIVE)
            new_max = jnp.maximum(running_max, lax.optimization_barrier(jnp.max(attention_scores, axis=-1)))
            shrink = jnp.exp(running_max - new_max)
            attention_probs = jnp.where(visible[None], jnp.exp(attention_scores - new_max[..., None]), 0.0)
            running_sum = running_sum * shrink + lax.optimization_barrier(jnp.sum(attention_probs, axis=-1))
            weighted_value_sum = jnp.einsum('fljx,xfc->fljc', rounded_value(attention_probs).reshape(key_group_count, repeat_factor, TOKENS_PER_SHARD, TOKENS_PER_SHARD), value_tile)
            weighted_sum = weighted_sum * shrink[..., None] + weighted_value_sum.reshape(lane_tally, TOKENS_PER_SHARD, HEAD_DIM)
            return (new_max, running_sum, weighted_sum)
        starting = (jnp.full((lane_tally, TOKENS_PER_SHARD), NEGATIVE, jnp.float32), jnp.zeros((lane_tally, TOKENS_PER_SHARD), jnp.float32), jnp.zeros((lane_tally, TOKENS_PER_SHARD, HEAD_DIM), jnp.float32))
        _, running_sum, weighted_sum = lax.fori_loop(0, block_index + 1, advance, starting)
        return (weighted_sum / running_sum[..., None]).transpose(1, 0, 2).reshape(TOKENS_PER_SHARD, -1).astype(jnp.bfloat16)
    outputs = lax.map(one_block, (query_blocks, gate_blocks, jnp.arange(blocks, dtype=jnp.int32)))
    return outputs.reshape(LENGTH, -1)

def reference(state_head_inputs, state_write_vectors, state_read_vectors, state_output_gate, presoftplus_steps, extra_decay_log, lane_shrinkage_powers, bypass_coefficient_vector, feeder_smoothing_stencil, stored_smoothing_stencil, lookup_smoothing_stencil, bundled_rescaling_vector, queries, attention_keys, attention_values, forget_gate_cumsum, state_out_weight, attention_out_weight):
    results = []
    for sequence_input in range(SEQS):
        state_result = memory_series_yield(state_head_inputs[sequence_input], state_write_vectors[sequence_input], state_read_vectors[sequence_input], state_output_gate[sequence_input], presoftplus_steps[sequence_input], extra_decay_log[sequence_input], lane_shrinkage_powers, bypass_coefficient_vector, feeder_smoothing_stencil, stored_smoothing_stencil, lookup_smoothing_stencil, bundled_rescaling_vector)
        attend_out = attend_sequence(queries[sequence_input], attention_keys[sequence_input], attention_values[sequence_input], forget_gate_cumsum[sequence_input])
        merged = jnp.dot(state_result, state_out_weight, preferred_element_type=jnp.float32) + jnp.dot(attend_out, attention_out_weight, preferred_element_type=jnp.float32)
        results.append(merged.astype(jnp.bfloat16))
    return jnp.stack(results)
```

```python
import functools
import math

import jax
import jax.numpy as jnp
from jax import lax
from jax.experimental import pallas as pl
from jax.experimental.pallas import tpu as pltpu
from jax.sharding import PartitionSpec as P

HEAD_DIM = 64
STATE = 128


EPSILON = 1e-06
NEGATIVE = -1e30


def passed_along(shard, axis, by):
    devices = lax.axis_size(axis)
    pairs = [(i, i + by) for i in range(devices) if 0 <= i + by < devices]
    return lax.ppermute(shard, axis, pairs)


def entering(shard, axis, join, neutral):
    place = lax.axis_index(axis)
    gathered = jax.tree.map(
        lambda a, kind: lax.all_gather(a.astype(kind), axis), shard, (jnp.bfloat16, jnp.bfloat16)
    )
    state = jax.tree.map(lambda a, e: jnp.zeros_like(a) + jnp.asarray(e, a.dtype), shard, neutral)

    def one(hop, state):
        return join(
            state,
            jax.tree.map(
                lambda a, own: lax.dynamic_index_in_dim(a, hop, 0, False).astype(own.dtype),
                gathered,
                shard,
            ),
        )

    return lax.fori_loop(0, place, one, state)


def causal_filter(feeder_quantities, before, taps):
    length = feeder_quantities.shape[0]
    padded = jnp.concatenate([before, feeder_quantities], axis=0).astype(jnp.float32)
    summed = jnp.zeros(feeder_quantities.shape, jnp.float32)
    for offset in range(taps.shape[0]):
        summed = summed + taps[offset].astype(jnp.float32) * padded[offset : offset + length]
    return jax.nn.silu(summed).astype(jnp.bfloat16)


def compose(earlier, later):
    return (earlier[0] * later[0], earlier[1] * later[0][..., None, None] + later[1])


def shards(
    state_head_inputs,
    state_write_vectors,
    state_read_vectors,
    state_output_gate,
    presoftplus_steps,
    extra_decay_log,
    lane_shrinkage_powers,
    bypass_coefficient_vector,
    feeder_smoothing_stencil,
    stored_smoothing_stencil,
    lookup_smoothing_stencil,
    bundled_rescaling_vector,
    queries,
    attention_keys,
    attention_values,
    forget_gate_cumsum,
    state_out_weight,
    attention_out_weight,
):
    shard_rows = state_head_inputs.shape[1]
    input_rows = state_head_inputs[0]
    write_rows = state_write_vectors[0]
    read_rows = state_read_vectors[0]
    tap_rows = feeder_smoothing_stencil.shape[0] - 1
    value_width = input_rows.shape[1]
    vector_width = write_rows.shape[1]
    tail_rows = jnp.concatenate(
        [input_rows[-tap_rows:], write_rows[-tap_rows:], read_rows[-tap_rows:]], axis=1
    )
    before = passed_along(tail_rows, "sp", 1)
    conv_values = causal_filter(input_rows, before[:, :value_width], feeder_smoothing_stencil)
    conv_write = causal_filter(
        write_rows, before[:, value_width : value_width + vector_width], stored_smoothing_stencil
    )
    conv_read = causal_filter(
        read_rows, before[:, value_width + vector_width :], lookup_smoothing_stencil
    )
    stride_duration = jax.nn.softplus(presoftplus_steps[0])
    shrinkage_natural_power = (
        stride_duration * (-jnp.exp(lane_shrinkage_powers))[:, None] + extra_decay_log[0]
    )
    lane_tally = stride_duration.shape[0]
    groups = vector_width // STATE
    per_group = lane_tally // groups
    cumulative = jnp.cumsum(shrinkage_natural_power, axis=1)
    input_heads = conv_values.reshape(shard_rows, groups, per_group, HEAD_DIM)
    write_groups = conv_write.reshape(shard_rows, groups, STATE)
    read_groups = conv_read.reshape(shard_rows, groups, STATE)
    inner_products = jnp.einsum(
        "tgn,sgn->gts", read_groups, write_groups, preferred_element_type=jnp.float32
    )
    positions = jnp.arange(shard_rows)
    causal = positions[:, None] >= positions[None, :]
    log_gap = jnp.where(causal[None], cumulative[:, :, None] - cumulative[:, None, :], -jnp.inf)
    weights = jnp.exp(log_gap) * stride_duration[:, None, :]
    mix_weights = (
        inner_products[:, None] * weights.reshape(groups, per_group, shard_rows, shard_rows)
    ).astype(jnp.bfloat16)
    local_part = jnp.einsum(
        "ghts,sghp->tghp", mix_weights, input_heads, preferred_element_type=jnp.float32
    )
    end_scale = (jnp.exp(cumulative[:, -1:] - cumulative) * stride_duration).T.reshape(
        shard_rows, groups, per_group
    )
    weighted = (input_heads.astype(jnp.float32) * end_scale[..., None]).astype(jnp.bfloat16)
    block_state = jnp.einsum(
        "sghp,sgn->ghpn", weighted, write_groups, preferred_element_type=jnp.float32
    )
    total_decay = jnp.exp(cumulative[:, -1]).reshape(groups, per_group)
    identity = (jnp.ones_like(total_decay), jnp.zeros_like(block_state))
    carried = entering((total_decay, block_state), "sp", compose, identity)[1]
    carried_part = jnp.einsum(
        "tgn,ghpn->tghp",
        read_groups,
        carried.astype(jnp.bfloat16),
        preferred_element_type=jnp.float32,
    )
    carried_part = (
        carried_part * jnp.exp(cumulative).T.reshape(shard_rows, groups, per_group)[..., None]
    )
    mixer_sum = (
        local_part
        + carried_part
        + bypass_coefficient_vector.reshape(groups, per_group)[None, :, :, None]
        * input_heads.astype(jnp.float32)
    )
    gated_rows = mixer_sum.reshape(shard_rows, groups, per_group * HEAD_DIM) * jax.nn.silu(
        state_output_gate[0].astype(jnp.float32)
    ).reshape(shard_rows, groups, -1)
    stretch_coefficient = lax.rsqrt(
        jnp.mean(gated_rows * gated_rows, axis=-1, keepdims=True) + EPSILON
    )
    state_result = (
        (gated_rows * stretch_coefficient * bundled_rescaling_vector.reshape(groups, -1))
        .reshape(shard_rows, -1)
        .astype(jnp.bfloat16)
    )
    attend_heads = forget_gate_cumsum.shape[2]
    key_group_count = attention_keys.shape[2] // HEAD_DIM
    repeat_factor = attend_heads // key_group_count
    query_head_count = queries[0].reshape(shard_rows, key_group_count, repeat_factor, HEAD_DIM)
    first_query = lax.axis_index("sp") * shard_rows
    query_index = first_query + jnp.arange(shard_rows)
    last_query = first_query + shard_rows - 1
    query_gates = forget_gate_cumsum[0].T
    all_gates = lax.all_gather(forget_gate_cumsum[0], "sp", axis=0, tiled=True)
    attention_score_scale = HEAD_DIM ** (-0.5)
    starting = (
        jnp.full((attend_heads, shard_rows), NEGATIVE, jnp.float32),
        jnp.zeros((attend_heads, shard_rows), jnp.float32),
        jnp.zeros((attend_heads, shard_rows, HEAD_DIM), jnp.float32),
    )
    key_rows = lax.all_gather(attention_keys[0], "sp", axis=0, tiled=True)
    value_rows = lax.all_gather(attention_values[0], "sp", axis=0, tiled=True)
    span = key_rows.shape[0]
    sub_block = math.gcd(span, 512)

    def advance(sub_index, running):
        first_key = sub_index * sub_block

        def attend(running):
            running_max, running_sum, weighted_sum = running
            key_tile = lax.dynamic_slice_in_dim(
                key_rows, sub_index * sub_block, sub_block, 0
            ).reshape(sub_block, key_group_count, HEAD_DIM)
            value_tile = lax.dynamic_slice_in_dim(
                value_rows, sub_index * sub_block, sub_block, 0
            ).reshape(sub_block, key_group_count, HEAD_DIM)
            key_gates = lax.dynamic_slice_in_dim(all_gates, first_key, sub_block, 0)
            attention_scores = jnp.einsum(
                "ezxp,czp->zxec", query_head_count, key_tile, preferred_element_type=jnp.float32
            )
            attention_scores = (
                attention_scores.reshape(attend_heads, shard_rows, sub_block)
                * attention_score_scale
            )
            attention_scores = attention_scores + query_gates[:, :, None] - key_gates.T[:, None, :]
            visible = (first_key + jnp.arange(sub_block))[None, :] <= query_index[:, None]
            attention_scores = jnp.where(visible[None], attention_scores, NEGATIVE)
            new_max = jnp.maximum(running_max, jnp.max(attention_scores, axis=-1))
            shrink = jnp.exp(running_max - new_max)
            attention_probs = jnp.where(
                visible[None], jnp.exp(attention_scores - new_max[..., None]), 0.0
            )
            running_sum = running_sum * shrink + jnp.sum(attention_probs, axis=-1)
            weighted_value_sum = jnp.einsum(
                "fljx,xfc->fljc",
                attention_probs.astype(jnp.bfloat16).reshape(
                    key_group_count, repeat_factor, shard_rows, sub_block
                ),
                value_tile,
                preferred_element_type=jnp.float32,
            )
            weighted_sum = weighted_sum * shrink[..., None] + weighted_value_sum.reshape(
                attend_heads, shard_rows, HEAD_DIM
            )
            return (new_max, running_sum, weighted_sum)

        return lax.cond(first_key <= last_query, attend, lambda kept: kept, running)

    _, running_sum, weighted_sum = lax.fori_loop(0, span // sub_block, advance, starting)
    attend_out = (
        (weighted_sum / running_sum[..., None])
        .transpose(1, 0, 2)
        .reshape(shard_rows, -1)
        .astype(jnp.bfloat16)
    )
    state_columns, attend_columns = (
        lax.all_gather(state_out_weight, "fs", axis=1, tiled=True),
        lax.all_gather(attention_out_weight, "fs", axis=1, tiled=True),
    )
    summed = lax.psum_scatter(
        (
            jnp.dot(state_result, state_columns, preferred_element_type=jnp.float32)
            + jnp.dot(attend_out, attend_columns, preferred_element_type=jnp.float32)
        ).astype(jnp.bfloat16),
        "tp",
        scatter_dimension=0,
        tiled=True,
    )
    return summed[None]


MESH = pl.DeviceIdType.MESH
LANES = 128
BF16, F32 = jnp.bfloat16, jnp.float32


def mixer_kernel(
    sp,
    fs,
    x_far,
    w_far,
    r_far,
    gate_far,
    step_far,
    extra_far,
    shrink_far,
    bypass_far,
    tapx_far,
    tapw_far,
    tapr_far,
    gain_far,
    q_far,
    k_far,
    v_far,
    forget_far,
    wst_far,
    wat_far,
    out_ref,
    x_ref,
    w_ref,
    r_ref,
    gate_ref,
    step_ref,
    extra_ref,
    shrink_ref,
    bypass_ref,
    tapx_ref,
    tapw_ref,
    tapr_ref,
    gain_ref,
    q_ref,
    k_ref,
    v_ref,
    forget_ref,
    load_sem,
    pad_ref,
    tails,
    conv,
    end_wide,
    kall,
    vall,
    gall,
    qs,
    own_state,
    state_in,
    state_out,
    side_in,
    decay_out,
    decay_in,
    mix,
    wst,
    wat,
    wst_x,
    wat_x,
    wst_y,
    wat_y,
    acts_mine,
    acts_in,
    pieces_mine,
    pieces_in,
    scales_mine,
    scales_in,
    acc,
    acc_state,
    returned,
    tail_send,
    tail_recv,
    kv_send,
    kv_recv,
    st_send,
    st_recv,
    side_recv,
    weight_send,
    weight_recv,
    act_send,
    act_recv,
    piece_send,
    piece_recv,
    sum_send,
    sum_recv,
):
    me = lax.axis_index("sp")
    f = lax.axis_index("fs")
    t = lax.axis_index("tp")
    rows, width = x_ref.shape[1], x_ref.shape[2]
    heads = step_ref.shape[1]
    kv_heads = k_ref.shape[2] // HEAD_DIM
    repeat = heads // kv_heads
    pairs = heads // 2
    taps = tapx_ref.shape[0]
    cols = wst_far.shape[1]
    part = cols // 2
    half = rows // 2

    barrier = pltpu.get_barrier_semaphore()
    for d in range(1, sp):
        pl.semaphore_signal(
            barrier, inc=1, device_id={"sp": lax.rem(me + d, sp)}, device_id_type=MESH
        )
    for d in (1, 2):
        for r in range(2):
            pl.semaphore_signal(
                barrier, inc=1, device_id={"fs": f ^ d, "tp": r}, device_id_type=MESH
            )
    pl.semaphore_signal(barrier, inc=1, device_id={"tp": 1 - t}, device_id_type=MESH)

    near = {
        "x": (x_far, x_ref),
        "w": (w_far, w_ref),
        "r": (r_far, r_ref),
        "tapx": (tapx_far, tapx_ref),
        "tapw": (tapw_far, tapw_ref),
        "tapr": (tapr_far, tapr_ref),
        "step": (step_far, step_ref),
        "extra": (extra_far, extra_ref),
        "shrink": (shrink_far, shrink_ref),
        "k": (k_far, k_ref),
        "v": (v_far, v_ref),
        "forget": (forget_far, forget_ref),
        "q": (q_far, q_ref),
        "wst": (wst_far, wst.at[t]),
        "wat": (wat_far, wat.at[t]),
        "gate": (gate_far, gate_ref),
        "gain": (gain_far, gain_ref),
        "bypass": (bypass_far, bypass_ref),
    }
    loads = {
        name: pltpu.make_async_copy(far, here, load_sem.at[i])
        for i, (name, (far, here)) in enumerate(near.items())
    }
    for load in loads.values():
        load.start()

    def loaded(*names):
        for name in names:
            loads[name].wait()

    def remote(src, dst, send, recv, where):
        return pltpu.make_async_remote_copy(
            src_ref=src,
            dst_ref=dst,
            send_sem=send,
            recv_sem=recv,
            device_id=where,
            device_id_type=MESH,
        )

    lane = lax.broadcasted_iota(jnp.int32, (1, LANES), 1)
    low = lane < HEAD_DIM
    row_id = lax.broadcasted_iota(jnp.int32, (rows, rows), 0)
    col_id = lax.broadcasted_iota(jnp.int32, (rows, rows), 1)

    def expand(columns, j):
        return jnp.where(low, columns[:, 2 * j : 2 * j + 1], columns[:, 2 * j + 1 : 2 * j + 2])

    inputs = (
        (x_ref, tapx_ref, slice(0, width)),
        (w_ref, tapw_ref, slice(width, width + STATE)),
        (r_ref, tapr_ref, slice(width + STATE, width + 2 * STATE)),
    )

    def filtered(count):
        for _, tap_ref, at in inputs:
            total = jnp.zeros((count, at.stop - at.start), F32)
            for i in range(taps):
                first = 8 - (taps - 1) + i
                total = total + tap_ref[i : i + 1, :].astype(F32) * pad_ref[first : first + count, at]
            conv[0:count, at] = (total * jax.nn.sigmoid(total)).astype(BF16)

    pad_ref[0:8, :] = jnp.zeros((8, pad_ref.shape[1]), F32)
    loaded("x", "w", "r", "tapx", "tapw", "tapr")
    for ref, _, at in inputs:
        pad_ref[8 : 8 + rows, at] = ref[0].astype(F32)
    filtered(rows)

    loaded("step", "extra", "shrink")
    head_row = lax.broadcasted_iota(jnp.int32, (heads, rows), 0)
    power = jnp.zeros((heads, rows), F32)
    for h in range(heads):
        power = jnp.where(head_row == h, shrink_ref[h], power)
    presoft = step_ref[0]
    step = jnp.maximum(presoft, 0.0) + jnp.log1p(jnp.exp(-jnp.abs(presoft)))
    log_decay = extra_ref[0] - jnp.exp(power) * step
    upper = (row_id <= col_id).astype(F32)
    cum = jnp.dot(log_decay, upper, precision=lax.Precision.HIGHEST, preferred_element_type=F32)
    cum_end = cum[:, rows - 1 : rows]
    decay_out[...] = jnp.broadcast_to(jnp.exp(cum_end), (heads, LANES))

    end_scale = (jnp.exp(cum_end - cum) * step).T
    for j in range(pairs):
        end_wide[:, j * LANES : (j + 1) * LANES] = expand(end_scale, j)

    odd = lax.rem(me, 2) == 1
    follows = me + 1 < sp

    def own_states():
        turned_write = conv[:, width : width + STATE].astype(F32).T.astype(BF16)
        for p in range(pairs):
            at = slice(p * LANES, (p + 1) * LANES)
            weighted = (conv[:, at].astype(F32) * end_wide[:, at]).astype(BF16)
            own_state[p] = jnp.dot(turned_write, weighted, preferred_element_type=F32)

    def state_copy(p, hop):
        there = {"sp": lax.rem(me + hop, sp)}
        return remote(
            state_out.at[p], state_in.at[p], st_send.at[p, hop - 1], st_recv.at[p], there
        )

    def side_copy(p):
        there = {"sp": lax.rem(me + 1, sp)}
        return remote(state_out.at[p], side_in.at[p], st_send.at[p, 0], side_recv.at[p], there)

    def side_decay_copy():
        there = {"sp": lax.rem(me + 1, sp)}
        return remote(decay_out, decay_in, st_send.at[pairs, 0], side_recv.at[pairs], there)

    def widened(decays, p):
        return jnp.where(low, decays[2 * p : 2 * p + 1, :], decays[2 * p + 1 : 2 * p + 2, :])

    @pl.when(me == 0)
    def _():
        state_in[...] = jnp.zeros(state_in.shape, BF16)
        own_states()
        for p in range(pairs):
            state_out[p] = own_state[p].astype(BF16)

    loaded("k", "v", "forget")
    gall[me] = forget_ref[0]
    gate_cols = forget_ref[0].T
    kall[me] = k_ref[0]
    vall[me] = v_ref[0]
    loaded("wst", "wat")

    pl.semaphore_wait(barrier, sp - 1 + 4 + 1)

    tail = [
        remote(
            ref.at[0, rows - 16 : rows, :],
            tails.at[:, at],
            tail_send.at[i],
            tail_recv.at[i],
            {"sp": lax.rem(me + 1, sp)},
        )
        for i, (ref, _, at) in enumerate(inputs)
    ]

    @pl.when(follows)
    def _():
        for copy in tail:
            copy.start()

    @pl.when(me == 0)
    def _():
        for p in range(pairs):
            state_copy(p, 1).start()

    def kv_copies(d, source):
        there = {"sp": lax.rem(me + d, sp)}
        return [
            remote(src, dst.at[source], kv_send.at[d, i], kv_recv.at[source, i], there)
            for i, (src, dst) in enumerate(
                ((k_ref.at[0], kall), (v_ref.at[0], vall), (gall.at[me], gall))
            )
        ]

    for d in range(1, sp):

        @pl.when(me + d < sp)
        def _(d=d):
            for copy in kv_copies(d, me):
                copy.start()

    first, second = slice(0, part), slice(part, cols)
    matrices = ((wst, wst_x, wst_y), (wat, wat_x, wat_y))

    def weight_copy(kind, i):
        whole, from_x, from_y = matrices[i]
        src, dst, where = (
            (whole.at[t], whole.at[t], {"tp": 1 - t}),
            (whole.at[t, :, first], from_x.at[t], {"fs": f ^ 1}),
            (whole.at[t, :, second], from_y.at[t], {"fs": f ^ 2}),
            (from_x.at[t], from_x.at[t], {"tp": 1 - t}),
            (from_y.at[t], from_y.at[t], {"tp": 1 - t}),
        )[kind]
        return remote(src, dst, weight_send.at[kind, i], weight_recv.at[kind, i], where)

    for i in range(2):
        for kind in (1, 2, 0):
            weight_copy(kind, 1 - i).start()

    for j in range(1, sp):

        @pl.when(j > me)
        def _(j=j):
            kall[j] = jnp.zeros(kall.shape[1:], BF16)
            vall[j] = jnp.zeros(vall.shape[1:], BF16)
            gall[j] = jnp.zeros(gall.shape[1:], F32)

    loaded("q")
    for h in range(heads):
        kv = h // repeat
        piece = (q_ref[0, :, h * HEAD_DIM : (h + 1) * HEAD_DIM].astype(F32) * HEAD_DIM**-0.5).astype(
            BF16
        )
        zero = jnp.zeros((rows, HEAD_DIM), BF16)
        parts = [piece if i == kv else zero for i in range(kv_heads)]
        qs[kv, (h % repeat) * rows : (h % repeat + 1) * rows, :] = jnp.concatenate(parts, axis=1)

    @pl.when(me > 0)
    def _():
        for copy in tail:
            copy.wait_recv()
        pad_ref[0:8, :] = tails[...].astype(F32)[8:16]
        filtered(16)
        own_states()

    @pl.when(jnp.logical_and(jnp.logical_not(odd), jnp.logical_and(me > 0, follows)))
    def _():
        for p in range(pairs):
            state_out[p] = own_state[p].astype(BF16)
            side_copy(p).start()
        side_decay_copy().start()

    def entered(p):
        @pl.when(jnp.logical_and(odd, me > 1))
        def _():
            if p == 0:
                side_decay_copy().wait_recv()
            side_copy(p).wait_recv()
            state_in[p] = (
                state_in[p].astype(F32) * widened(decay_in[...], p) + side_in[p].astype(F32)
            ).astype(BF16)

    relays = jnp.logical_and(odd, follows)

    @pl.when(relays)
    def _():
        for p in range(pairs):
            state_copy(p, 1).wait_recv()
            entered(p)
            state_out[p] = (
                state_in[p].astype(F32) * widened(decay_out[...], p) + own_state[p]
            ).astype(BF16)

            @pl.when(me + 2 < sp)
            def _(p=p):
                state_copy(p, 2).start()

            state_copy(p, 1).start()

    for j in range(sp - 1):

        @pl.when(j < me)
        def _(j=j):
            for copy in kv_copies(1, j):
                copy.wait_recv()

    keys = kall[...].reshape(sp * rows, -1)
    values = vall[...].reshape(sp * rows, -1)
    visible = [j * rows + col_id <= me * rows + row_id for j in range(sp)]
    for kv in range(kv_heads):
        own = lane // HEAD_DIM == kv
        summed_values = jnp.where(own, values, jnp.ones_like(values))
        scores = lax.dot_general(
            qs[kv], keys, (((1,), (1,)), ((), ())), preferred_element_type=F32
        )
        outs = []
        for i in range(repeat):
            h = kv * repeat + i
            gate_col = gate_cols[:, h : h + 1]
            tiles = [
                jnp.where(
                    visible[j],
                    scores[i * rows : (i + 1) * rows, j * rows : (j + 1) * rows]
                    + (gate_col - gall[j, h : h + 1, :]),
                    NEGATIVE,
                )
                for j in range(sp)
            ]
            top = tiles[0]
            for tile in tiles[1:]:
                top = jnp.maximum(top, tile)
            top = jnp.max(top, axis=1, keepdims=True)
            probs = jnp.concatenate([jnp.exp(tile - top).astype(BF16) for tile in tiles], axis=1)
            both = jnp.dot(probs, summed_values, preferred_element_type=F32)
            turned = pltpu.roll(both, HEAD_DIM, 1)
            outs.append(both / turned if h % 2 == kv else turned / both)
        for i in range(0, repeat, 2):
            at = slice((kv * repeat + i) * HEAD_DIM, (kv * repeat + i + 2) * HEAD_DIM)
            merged = jnp.where(low, outs[i], outs[i + 1]).astype(BF16)
            for r in range(2):
                acts_mine[r, :, at] = merged[r * half : (r + 1) * half]

    def targets(slot):
        if slot == 0:
            return [(1 - t, {"tp": 1 - t}, 0)]
        return [(r, {"fs": f ^ slot, "tp": r}, r) for r in range(2)]

    def act_copies(slot):
        return [
            remote(
                acts_mine.at[r],
                acts_in.at[slot, t],
                act_send.at[slot, lanes],
                act_recv.at[slot, t],
                where,
            )
            for r, where, lanes in targets(slot)
        ]

    def act_wait(slot, source):
        remote(
            acts_mine.at[0],
            acts_in.at[slot, source],
            act_send.at[slot, 0],
            act_recv.at[slot, source],
            {"tp": 1 - t},
        ).wait_recv()

    def piece_copies(p, slot):
        src, dst = (pieces_mine, pieces_in) if p < pairs else (scales_mine, scales_in)
        return [
            remote(
                src.at[(r, p) if p < pairs else (r,)],
                dst.at[(slot, t, p) if p < pairs else (slot, t)],
                piece_send.at[p, slot, lanes],
                piece_recv.at[p, slot, t],
                where,
            )
            for r, where, lanes in targets(slot)
        ]

    def piece_wait(p, slot, source):
        src, dst = (pieces_mine, pieces_in) if p < pairs else (scales_mine, scales_in)
        remote(
            src.at[(0, p) if p < pairs else (0,)],
            dst.at[(slot, source, p) if p < pairs else (slot, source)],
            piece_send.at[p, slot, 0],
            piece_recv.at[p, slot, source],
            {"tp": 1 - t},
        ).wait_recv()

    slots = (1, 2, 0)
    for slot in slots:
        for copy in act_copies(slot):
            copy.start()

    loaded("gate", "gain", "bypass")
    exp_cum = jnp.exp(cum).T
    cum_col = cum.T
    conv_write = conv[:, width : width + STATE]
    conv_read = conv[:, width + STATE :]
    inner = lax.dot_general(
        conv_read, conv_write, (((1,), (1,)), ((), ())), preferred_element_type=F32
    )
    causal = row_id >= col_id
    for j in range(pairs):
        tile = conv[:, j * LANES : (j + 1) * LANES]
        parts = []
        for h in (2 * j, 2 * j + 1):
            gap = jnp.where(causal, cum_col[:, h : h + 1] - cum[h : h + 1, :], NEGATIVE)
            weights = (inner * (jnp.exp(gap) * step[h : h + 1, :])).astype(BF16)
            parts.append(jnp.dot(weights, tile, preferred_element_type=F32))
        bypass = jnp.where(low, bypass_ref[2 * j], bypass_ref[2 * j + 1])
        mix[:, j * LANES : (j + 1) * LANES] = (
            jnp.where(low, parts[0], parts[1]) + bypass * tile.astype(F32)
        )

    squares = []
    for p in range(pairs):
        at = slice(p * LANES, (p + 1) * LANES)

        @pl.when(jnp.logical_and(me > 0, jnp.logical_not(relays)))
        def _(p=p):
            state_copy(p, 1).wait_recv()
            entered(p)

        carried = jnp.dot(conv_read, state_in[p], preferred_element_type=F32)
        gate = gate_ref[0, :, at].astype(F32)
        u = (mix[:, at] + carried * expand(exp_cum, p)) * (gate * jax.nn.sigmoid(gate))
        squares.append(u * u)
        sent = (u * gain_ref[0:1, at]).astype(BF16)
        for r in range(2):
            pieces_mine[r, p] = sent[r * half : (r + 1) * half]
        for slot in slots:
            for copy in piece_copies(p, slot):
                copy.start()

    total = functools.reduce(jnp.add, squares)
    mean = (
        lax.dot_general(
            jnp.ones((8, LANES), F32),
            total,
            (((1,), (1,)), ((), ())),
            precision=lax.Precision.HIGHEST,
            preferred_element_type=F32,
        )
        / width
    )
    scale = lax.rsqrt(mean + EPSILON)
    scales_mine[0] = scale
    scales_mine[1] = pltpu.roll(scale, half, 1)
    for slot in slots:
        for copy in piece_copies(pairs, slot):
            copy.start()

    acts_in[0, t] = acts_mine[t]
    for p in range(pairs):
        pieces_in[0, t, p] = pieces_mine[t, p]
    scales_in[0, t] = scales_mine[t]

    for i in (1, 0):
        for kind in (1, 2):
            weight_copy(kind, i).wait_recv()
            weight_copy(kind + 2, i).start()

    groups = (
        (2, wst, wat, first),
        (2, wst_x, wat_x, slice(0, part)),
        (1, wst, wat, second),
        (1, wst_y, wat_y, slice(0, part)),
    )
    needs = (0, 3, 0, 4)

    def from_peer(kind, i):
        whole, from_x, from_y = matrices[i]
        ref = (whole, None, None, from_x, from_y)[kind]
        remote(
            ref.at[1 - t],
            ref.at[1 - t],
            weight_send.at[kind, i],
            weight_recv.at[kind, i],
            {"tp": 1 - t},
        ).wait_recv()

    act_wait(0, 1 - t)
    for slot in (2, 1):
        for source in range(2):
            act_wait(slot, source)
    for kind in (0, 3, 4):
        from_peer(kind, 1)
    for g, (slot, _, weights, at) in enumerate(groups):
        left = jnp.concatenate(
            [
                jnp.concatenate([acts_in[0, s], acts_in[slot, s]], axis=0)
                for s in range(2)
            ],
            axis=1,
        )
        right = jnp.concatenate([weights[s, :, at] for s in range(2)], axis=0)
        acc[g] = jnp.dot(left, right, preferred_element_type=F32)

    for kind in (0, 3, 4):
        from_peer(kind, 0)
    for p in range(pairs - 1):
        piece_wait(p, 0, 1 - t)
        for slot in (2, 1):
            for source in range(2):
                piece_wait(p, slot, source)

    cut = (pairs - 1) * LANES

    def stacked(slot, s, p):
        return jnp.concatenate([pieces_in[0, s, p], pieces_in[slot, s, p]], axis=0)

    for g, (slot, weights, _, at) in enumerate(groups):
        for s in range(2):
            left = jnp.concatenate([stacked(slot, s, p) for p in range(pairs - 1)], axis=1)
            acc_state[g, s] = jnp.dot(left, weights[s, 0:cut, at], preferred_element_type=F32)

    for p in (pairs - 1, pairs):
        piece_wait(p, 0, 1 - t)
        for slot in (2, 1):
            for source in range(2):
                piece_wait(p, slot, source)

    def columns(owner, at):
        return pl.ds(pl.multiple_of(owner * cols + at.start, part), part)

    def sum_copy(g):
        slot = groups[g][0]
        owner = (f, f ^ 1, f, f ^ 2)[g]
        at = (first, first, second, second)[g]
        return remote(
            returned.at[g],
            out_ref.at[0, :, columns(owner, at)],
            sum_send.at[g],
            sum_recv.at[g],
            {"fs": f ^ slot},
        )

    turned = [[scales_in[slot, s].T[0:half, 0:1] for s in range(2)] for slot in range(3)]
    for g, (slot, weights, _, at) in enumerate(groups):
        merged = acc[g]
        for s in range(2):
            last = jnp.dot(
                stacked(slot, s, pairs - 1), weights[s, cut:, at], preferred_element_type=F32
            )
            by = jnp.concatenate([turned[0][s], turned[slot][s]], axis=0)
            merged = merged + (acc_state[g, s] + last) * by
        merged = merged.astype(BF16)
        returned[g] = merged[half:]
        sum_copy(g).start()
        owner = (f, f ^ 1, f, f ^ 2)[g]
        out_ref[0, :, columns(owner, (first, first, second, second)[g])] = merged[0:half]

    for g in range(4):
        sum_copy(g).wait_recv()

    @pl.when(follows)
    def _():
        for copy in tail:
            copy.wait_send()

    @pl.when(jnp.logical_and(follows, jnp.logical_or(odd, me == 0)))
    def _():
        for p in range(pairs):
            state_copy(p, 1).wait_send()

    @pl.when(jnp.logical_and(odd, me + 2 < sp))
    def _():
        for p in range(pairs):
            state_copy(p, 2).wait_send()

    @pl.when(jnp.logical_and(jnp.logical_not(odd), jnp.logical_and(me > 0, follows)))
    def _():
        for p in range(pairs):
            side_copy(p).wait_send()
        side_decay_copy().wait_send()

    for d in range(1, sp):

        @pl.when(me + d < sp)
        def _(d=d):
            for copy in kv_copies(d, me):
                copy.wait_send()

    for kind in range(5):
        for i in range(2):
            weight_copy(kind, i).wait_send()
    for slot in slots:
        for copy in act_copies(slot):
            copy.wait_send()
        for p in range(pairs + 1):
            for copy in piece_copies(p, slot):
                copy.wait_send()
    for g in range(4):
        sum_copy(g).wait_send()


def fused(sp, fs, *args):
    rows, width = args[0].shape[1:]
    heads = args[4].shape[1]
    deep, cols = args[16].shape
    half, part = rows // 2, cols // 2
    args = list(args)
    args[11] = args[11].reshape(1, -1)
    args[15] = jnp.swapaxes(args[15], 1, 2)
    vmem = pl.BlockSpec(memory_space=pltpu.VMEM)
    far = pl.BlockSpec(memory_space=pl.ANY)
    dma = pltpu.SemaphoreType.DMA
    kv_width = args[13].shape[2]
    kv_heads = kv_width // HEAD_DIM
    pairs = heads // 2
    near = [
        (pltpu.SMEM if i in (6, 7) else pltpu.VMEM)(a.shape, a.dtype)
        for i, a in enumerate(args[:16])
    ]
    return pl.pallas_call(
        functools.partial(mixer_kernel, sp, fs),
        out_shape=jax.ShapeDtypeStruct((1, half, cols * fs), BF16),
        in_specs=[far] * len(args),
        out_specs=vmem,
        scratch_shapes=near
        + [
            dma((len(args),)),
            pltpu.VMEM((8 + rows, width + 2 * STATE), F32),
            pltpu.VMEM((16, width + 2 * STATE), BF16),
            pltpu.VMEM((rows, width + 2 * STATE), BF16),
            pltpu.VMEM((rows, width), F32),
            pltpu.VMEM((sp, rows, kv_width), BF16),
            pltpu.VMEM((sp, rows, kv_width), BF16),
            pltpu.VMEM((sp, heads, rows), F32),
            pltpu.VMEM((kv_heads, heads // kv_heads * rows, kv_width), BF16),
            pltpu.VMEM((pairs, STATE, LANES), F32),
            pltpu.VMEM((pairs, STATE, LANES), BF16),
            pltpu.VMEM((pairs, STATE, LANES), BF16),
            pltpu.VMEM((pairs, STATE, LANES), BF16),
            pltpu.VMEM((heads, LANES), F32),
            pltpu.VMEM((heads, LANES), F32),
            pltpu.VMEM((rows, width), F32),
            pltpu.VMEM((2, deep, cols), BF16),
            pltpu.VMEM((2, deep, cols), BF16),
            pltpu.VMEM((2, deep, part), BF16),
            pltpu.VMEM((2, deep, part), BF16),
            pltpu.VMEM((2, deep, part), BF16),
            pltpu.VMEM((2, deep, part), BF16),
            pltpu.VMEM((2, half, width), BF16),
            pltpu.VMEM((3, 2, half, width), BF16),
            pltpu.VMEM((2, pairs, half, LANES), BF16),
            pltpu.VMEM((3, 2, pairs, half, LANES), BF16),
            pltpu.VMEM((2, 8, rows), F32),
            pltpu.VMEM((3, 2, 8, rows), F32),
            pltpu.VMEM((4, rows, part), F32),
            pltpu.VMEM((4, 2, rows, part), F32),
            pltpu.VMEM((4, half, part), BF16),
            dma((3,)),
            dma((3,)),
            dma((sp, 3)),
            dma((sp, 3)),
            dma((pairs + 1, 2)),
            dma((pairs,)),
            dma((pairs + 1,)),
            dma((5, 2)),
            dma((5, 2)),
            dma((3, 2)),
            dma((3, 2)),
            dma((pairs + 1, 3, 2)),
            dma((pairs + 1, 3, 2)),
            dma((4,)),
            dma((4,)),
        ],
        compiler_params=pltpu.CompilerParams(collective_id=0, has_side_effects=True),
    )(*args)


def one_kernel(*args, sp, fs, tp):
    rows, width = args[0].shape[1:]
    heads = args[4].shape[1]
    return (
        1 < sp <= 8
        and fs == 4
        and tp == 2
        and rows == LANES
        and args[1].shape[2] == STATE == LANES
        and width == heads * HEAD_DIM
        and args[12].shape[2] == width
        and args[13].shape[2] == 2 * HEAD_DIM
        and heads % 4 == 0
        and args[16].shape == args[17].shape == (width, args[16].shape[1])
        and args[16].shape[1] % (2 * LANES) == 0
    )


def solution(mesh):
    in_specs = (
        P("fs", "sp", "tp"),
        P("fs", "sp", "tp"),
        P("fs", "sp", "tp"),
        P("fs", "sp", "tp"),
        P("fs", "tp", "sp"),
        P("fs", "tp", "sp"),
        P("tp"),
        P("tp"),
        P(None, "tp"),
        P(None, "tp"),
        P(None, "tp"),
        P("tp"),
        P("fs", "sp", "tp"),
        P("fs", "sp", "tp"),
        P("fs", "sp", "tp"),
        P("fs", "sp", "tp"),
        P("tp", "fs"),
        P("tp", "fs"),
    )
    out_specs = P("fs", ("sp", "tp"), None)
    sp, fs, tp = (mesh.shape[name] for name in ("sp", "fs", "tp"))

    def body(*args):
        if one_kernel(*args, sp=sp, fs=fs, tp=tp):
            return fused(sp, fs, *args)
        return shards(*args)

    return jax.shard_map(body, mesh=mesh, in_specs=in_specs, out_specs=out_specs, check_vma=False)
```

```python
import functools
import math

import jax
import jax.numpy as jnp
from jax import lax
from jax.experimental import pallas as pl
from jax.experimental.pallas import tpu as pltpu
from jax.sharding import PartitionSpec as P

HEAD_DIM = 64
STATE = 128


EPSILON = 1e-06
NEGATIVE = -1e30


def passed_along(shard, axis, by):
    devices = lax.axis_size(axis)
    pairs = [(i, i + by) for i in range(devices) if 0 <= i + by < devices]
    return lax.ppermute(shard, axis, pairs)


def entering(shard, axis, join, neutral):
    place = lax.axis_index(axis)
    gathered = jax.tree.map(
        lambda a, kind: lax.all_gather(a.astype(kind), axis), shard, (jnp.bfloat16, jnp.bfloat16)
    )
    state = jax.tree.map(lambda a, e: jnp.zeros_like(a) + jnp.asarray(e, a.dtype), shard, neutral)

    def one(hop, state):
        return join(
            state,
            jax.tree.map(
                lambda a, own: lax.dynamic_index_in_dim(a, hop, 0, False).astype(own.dtype),
                gathered,
                shard,
            ),
        )

    return lax.fori_loop(0, place, one, state)


def causal_filter(feeder_quantities, before, taps):
    length = feeder_quantities.shape[0]
    padded = jnp.concatenate([before, feeder_quantities], axis=0).astype(jnp.float32)
    summed = jnp.zeros(feeder_quantities.shape, jnp.float32)
    for offset in range(taps.shape[0]):
        summed = summed + taps[offset].astype(jnp.float32) * padded[offset : offset + length]
    return jax.nn.silu(summed).astype(jnp.bfloat16)


def compose(earlier, later):
    return (earlier[0] * later[0], earlier[1] * later[0][..., None, None] + later[1])


def shards(
    state_head_inputs,
    state_write_vectors,
    state_read_vectors,
    state_output_gate,
    presoftplus_steps,
    extra_decay_log,
    lane_shrinkage_powers,
    bypass_coefficient_vector,
    feeder_smoothing_stencil,
    stored_smoothing_stencil,
    lookup_smoothing_stencil,
    bundled_rescaling_vector,
    queries,
    attention_keys,
    attention_values,
    forget_gate_cumsum,
    state_out_weight,
    attention_out_weight,
):
    shard_rows = state_head_inputs.shape[1]
    input_rows = state_head_inputs[0]
    write_rows = state_write_vectors[0]
    read_rows = state_read_vectors[0]
    tap_rows = feeder_smoothing_stencil.shape[0] - 1
    value_width = input_rows.shape[1]
    vector_width = write_rows.shape[1]
    tail_rows = jnp.concatenate(
        [input_rows[-tap_rows:], write_rows[-tap_rows:], read_rows[-tap_rows:]], axis=1
    )
    before = passed_along(tail_rows, "sp", 1)
    conv_values = causal_filter(input_rows, before[:, :value_width], feeder_smoothing_stencil)
    conv_write = causal_filter(
        write_rows, before[:, value_width : value_width + vector_width], stored_smoothing_stencil
    )
    conv_read = causal_filter(
        read_rows, before[:, value_width + vector_width :], lookup_smoothing_stencil
    )
    stride_duration = jax.nn.softplus(presoftplus_steps[0])
    shrinkage_natural_power = (
        stride_duration * (-jnp.exp(lane_shrinkage_powers))[:, None] + extra_decay_log[0]
    )
    lane_tally = stride_duration.shape[0]
    groups = vector_width // STATE
    per_group = lane_tally // groups
    cumulative = jnp.cumsum(shrinkage_natural_power, axis=1)
    input_heads = conv_values.reshape(shard_rows, groups, per_group, HEAD_DIM)
    write_groups = conv_write.reshape(shard_rows, groups, STATE)
    read_groups = conv_read.reshape(shard_rows, groups, STATE)
    inner_products = jnp.einsum(
        "tgn,sgn->gts", read_groups, write_groups, preferred_element_type=jnp.float32
    )
    positions = jnp.arange(shard_rows)
    causal = positions[:, None] >= positions[None, :]
    log_gap = jnp.where(causal[None], cumulative[:, :, None] - cumulative[:, None, :], -jnp.inf)
    weights = jnp.exp(log_gap) * stride_duration[:, None, :]
    mix_weights = (
        inner_products[:, None] * weights.reshape(groups, per_group, shard_rows, shard_rows)
    ).astype(jnp.bfloat16)
    local_part = jnp.einsum(
        "ghts,sghp->tghp", mix_weights, input_heads, preferred_element_type=jnp.float32
    )
    end_scale = (jnp.exp(cumulative[:, -1:] - cumulative) * stride_duration).T.reshape(
        shard_rows, groups, per_group
    )
    weighted = (input_heads.astype(jnp.float32) * end_scale[..., None]).astype(jnp.bfloat16)
    block_state = jnp.einsum(
        "sghp,sgn->ghpn", weighted, write_groups, preferred_element_type=jnp.float32
    )
    total_decay = jnp.exp(cumulative[:, -1]).reshape(groups, per_group)
    identity = (jnp.ones_like(total_decay), jnp.zeros_like(block_state))
    carried = entering((total_decay, block_state), "sp", compose, identity)[1]
    carried_part = jnp.einsum(
        "tgn,ghpn->tghp",
        read_groups,
        carried.astype(jnp.bfloat16),
        preferred_element_type=jnp.float32,
    )
    carried_part = (
        carried_part * jnp.exp(cumulative).T.reshape(shard_rows, groups, per_group)[..., None]
    )
    mixer_sum = (
        local_part
        + carried_part
        + bypass_coefficient_vector.reshape(groups, per_group)[None, :, :, None]
        * input_heads.astype(jnp.float32)
    )
    gated_rows = mixer_sum.reshape(shard_rows, groups, per_group * HEAD_DIM) * jax.nn.silu(
        state_output_gate[0].astype(jnp.float32)
    ).reshape(shard_rows, groups, -1)
    stretch_coefficient = lax.rsqrt(
        jnp.mean(gated_rows * gated_rows, axis=-1, keepdims=True) + EPSILON
    )
    state_result = (
        (gated_rows * stretch_coefficient * bundled_rescaling_vector.reshape(groups, -1))
        .reshape(shard_rows, -1)
        .astype(jnp.bfloat16)
    )
    attend_heads = forget_gate_cumsum.shape[2]
    key_group_count = attention_keys.shape[2] // HEAD_DIM
    repeat_factor = attend_heads // key_group_count
    query_head_count = queries[0].reshape(shard_rows, key_group_count, repeat_factor, HEAD_DIM)
    first_query = lax.axis_index("sp") * shard_rows
    query_index = first_query + jnp.arange(shard_rows)
    last_query = first_query + shard_rows - 1
    query_gates = forget_gate_cumsum[0].T
    all_gates = lax.all_gather(forget_gate_cumsum[0], "sp", axis=0, tiled=True)
    attention_score_scale = HEAD_DIM ** (-0.5)
    starting = (
        jnp.full((attend_heads, shard_rows), NEGATIVE, jnp.float32),
        jnp.zeros((attend_heads, shard_rows), jnp.float32),
        jnp.zeros((attend_heads, shard_rows, HEAD_DIM), jnp.float32),
    )
    key_rows = lax.all_gather(attention_keys[0], "sp", axis=0, tiled=True)
    value_rows = lax.all_gather(attention_values[0], "sp", axis=0, tiled=True)
    span = key_rows.shape[0]
    sub_block = math.gcd(span, 512)

    def advance(sub_index, running):
        first_key = sub_index * sub_block

        def attend(running):
            running_max, running_sum, weighted_sum = running
            key_tile = lax.dynamic_slice_in_dim(
                key_rows, sub_index * sub_block, sub_block, 0
            ).reshape(sub_block, key_group_count, HEAD_DIM)
            value_tile = lax.dynamic_slice_in_dim(
                value_rows, sub_index * sub_block, sub_block, 0
            ).reshape(sub_block, key_group_count, HEAD_DIM)
            key_gates = lax.dynamic_slice_in_dim(all_gates, first_key, sub_block, 0)
            attention_scores = jnp.einsum(
                "ezxp,czp->zxec", query_head_count, key_tile, preferred_element_type=jnp.float32
            )
            attention_scores = (
                attention_scores.reshape(attend_heads, shard_rows, sub_block)
                * attention_score_scale
            )
            attention_scores = attention_scores + query_gates[:, :, None] - key_gates.T[:, None, :]
            visible = (first_key + jnp.arange(sub_block))[None, :] <= query_index[:, None]
            attention_scores = jnp.where(visible[None], attention_scores, NEGATIVE)
            new_max = jnp.maximum(running_max, jnp.max(attention_scores, axis=-1))
            shrink = jnp.exp(running_max - new_max)
            attention_probs = jnp.where(
                visible[None], jnp.exp(attention_scores - new_max[..., None]), 0.0
            )
            running_sum = running_sum * shrink + jnp.sum(attention_probs, axis=-1)
            weighted_value_sum = jnp.einsum(
                "fljx,xfc->fljc",
                attention_probs.astype(jnp.bfloat16).reshape(
                    key_group_count, repeat_factor, shard_rows, sub_block
                ),
                value_tile,
                preferred_element_type=jnp.float32,
            )
            weighted_sum = weighted_sum * shrink[..., None] + weighted_value_sum.reshape(
                attend_heads, shard_rows, HEAD_DIM
            )
            return (new_max, running_sum, weighted_sum)

        return lax.cond(first_key <= last_query, attend, lambda kept: kept, running)

    _, running_sum, weighted_sum = lax.fori_loop(0, span // sub_block, advance, starting)
    attend_out = (
        (weighted_sum / running_sum[..., None])
        .transpose(1, 0, 2)
        .reshape(shard_rows, -1)
        .astype(jnp.bfloat16)
    )
    state_columns, attend_columns = (
        lax.all_gather(state_out_weight, "fs", axis=1, tiled=True),
        lax.all_gather(attention_out_weight, "fs", axis=1, tiled=True),
    )
    summed = lax.psum_scatter(
        (
            jnp.dot(state_result, state_columns, preferred_element_type=jnp.float32)
            + jnp.dot(attend_out, attend_columns, preferred_element_type=jnp.float32)
        ).astype(jnp.bfloat16),
        "tp",
        scatter_dimension=0,
        tiled=True,
    )
    return summed[None]


MESH = pl.DeviceIdType.MESH
LANES = 128
BF16, F32 = jnp.bfloat16, jnp.float32


def mixer_kernel(
    sp,
    fs,
    x_far,
    w_far,
    r_far,
    gate_far,
    step_far,
    extra_far,
    shrink_far,
    bypass_far,
    tapx_far,
    tapw_far,
    tapr_far,
    gain_far,
    q_far,
    k_far,
    v_far,
    forget_far,
    wst_far,
    wat_far,
    out_ref,
    x_ref,
    w_ref,
    r_ref,
    gate_ref,
    step_ref,
    extra_ref,
    shrink_ref,
    bypass_ref,
    tapx_ref,
    tapw_ref,
    tapr_ref,
    gain_ref,
    q_ref,
    forget_ref,
    load_sem,
    ready,
    pad_ref,
    tails,
    conv,
    end_wide,
    kvall,
    gall,
    qs,
    own_state,
    state_in,
    state_out,
    mix,
    wst,
    wat,
    wst_y,
    wat_x,
    acts_mine,
    acts_in,
    pieces_mine,
    pieces_in,
    scales_mine,
    scales_in,
    acc,
    acc_state,
    att_out,
    att_in,
    sum_out,
    sum_in,
    tail_sem,
    kv_sem,
    st_send,
    st_recv,
    weight_send,
    weight_recv,
    act_sem,
    piece_send,
    piece_recv,
    sum_send,
    sum_recv,
):
    me = lax.axis_index("sp")
    f = lax.axis_index("fs")
    t = lax.axis_index("tp")
    rows, width = x_ref.shape[1], x_ref.shape[2]
    heads = step_ref.shape[1]
    kv_width = k_far.shape[2]
    kv_heads = kv_width // HEAD_DIM
    repeat = heads // kv_heads
    pairs = heads // 2
    taps = tapx_ref.shape[0]
    cols = wst_far.shape[1]
    part = cols // 2
    half = rows // 2
    peer = {"tp": 1 - t}

    barrier = pltpu.get_barrier_semaphore()
    for d in (1, 2):
        for r in range(2):
            pl.semaphore_signal(
                barrier, inc=1, device_id={"fs": f ^ d, "tp": r}, device_id_type=MESH
            )
    pl.semaphore_signal(barrier, inc=1, device_id=peer, device_id_type=MESH)
    for d in range(1, sp):

        @pl.when(me + d < sp)
        def _(d=d):
            pl.semaphore_signal(barrier, inc=1, device_id={"sp": me + d}, device_id_type=MESH)

    near = {
        "x": (x_far, x_ref),
        "w": (w_far, w_ref),
        "r": (r_far, r_ref),
        "tapx": (tapx_far, tapx_ref),
        "tapw": (tapw_far, tapw_ref),
        "tapr": (tapr_far, tapr_ref),
        "k": (k_far.at[0], kvall.at[me, :, 0:kv_width]),
        "v": (v_far.at[0], kvall.at[me, :, kv_width:]),
        "wat": (wat_far, wat.at[t]),
        "wst": (wst_far, wst.at[t]),
        "step": (step_far, step_ref),
        "extra": (extra_far, extra_ref),
        "shrink": (shrink_far, shrink_ref),
        "forget": (forget_far, forget_ref),
        "q": (q_far, q_ref),
        "gate": (gate_far, gate_ref),
        "gain": (gain_far, gain_ref),
        "bypass": (bypass_far, bypass_ref),
    }
    loads = {
        name: pltpu.make_async_copy(far, here, load_sem.at[i])
        for i, (name, (far, here)) in enumerate(near.items())
    }
    for load in loads.values():
        load.start()

    def loaded(*names):
        for name in names:
            loads[name].wait()

    def remote(src, dst, send, recv, where):
        return pltpu.make_async_remote_copy(
            src_ref=src,
            dst_ref=dst,
            send_sem=send,
            recv_sem=recv,
            device_id=where,
            device_id_type=MESH,
        )

    def arrived(ref, sem):
        remote(ref, ref, sem, sem, peer).wait_recv()

    def departed(ref, sem):
        remote(ref, ref, sem, sem, peer).wait_send()

    lane = lax.broadcasted_iota(jnp.int32, (1, LANES), 1)
    low = lane < HEAD_DIM
    row_id = lax.broadcasted_iota(jnp.int32, (rows, rows), 0)
    col_id = lax.broadcasted_iota(jnp.int32, (rows, rows), 1)

    def expand(columns, j):
        return jnp.where(low, columns[:, 2 * j : 2 * j + 1], columns[:, 2 * j + 1 : 2 * j + 2])

    inputs = (
        (x_ref, tapx_ref, slice(0, width)),
        (w_ref, tapw_ref, slice(width, width + STATE)),
        (r_ref, tapr_ref, slice(width + STATE, width + 2 * STATE)),
    )

    def filtered(count):
        for _, tap_ref, at in inputs:
            total = jnp.zeros((count, at.stop - at.start), F32)
            for i in range(taps):
                first = 8 - (taps - 1) + i
                total = total + tap_ref[i : i + 1, :].astype(F32) * pad_ref[first : first + count, at]
            conv[0:count, at] = (total * jax.nn.sigmoid(total)).astype(BF16)

    pad_ref[0:8, :] = jnp.zeros((8, pad_ref.shape[1]), F32)
    loaded("x", "w", "r", "tapx", "tapw", "tapr")
    for ref, _, at in inputs:
        pad_ref[8 : 8 + rows, at] = ref[0].astype(F32)
    filtered(rows)

    loaded("wat", "wst")
    pl.semaphore_wait(barrier, 5 + me)

    def weight_copies(kind):
        return (
            (
                remote(wat.at[t], wat_x.at[t], weight_send.at[0], weight_recv.at[0], {"fs": f ^ 1}),
                remote(wst.at[t], wst_y.at[t], weight_send.at[0], weight_recv.at[1], {"fs": f ^ 2}),
            ),
            (
                remote(wat.at[t], wat.at[t], weight_send.at[1], weight_recv.at[2], peer),
                remote(wst.at[t], wst.at[t], weight_send.at[1], weight_recv.at[3], peer),
            ),
            (
                remote(wat_x.at[t], wat_x.at[t], weight_send.at[2], weight_recv.at[2], peer),
                remote(wst_y.at[t], wst_y.at[t], weight_send.at[2], weight_recv.at[3], peer),
            ),
        )[kind]

    for kind in range(2):
        for copy in weight_copies(kind):
            copy.start()

    for d in range(1, sp):

        @pl.when(me - d >= 0)
        def _(d=d):
            pl.semaphore_signal(
                ready.at[d - 1], inc=1, device_id={"sp": me - d}, device_id_type=MESH
            )

    loaded("step", "extra", "shrink")
    head_row = lax.broadcasted_iota(jnp.int32, (heads, rows), 0)
    power = jnp.zeros((heads, rows), F32)
    for h in range(heads):
        power = jnp.where(head_row == h, shrink_ref[h], power)
    presoft = step_ref[0]
    step = jnp.maximum(presoft, 0.0) + jnp.log1p(jnp.exp(-jnp.abs(presoft)))
    log_decay = extra_ref[0] - jnp.exp(power) * step
    upper = (row_id <= col_id).astype(F32)
    cum = jnp.dot(log_decay, upper, precision=lax.Precision.HIGHEST, preferred_element_type=F32)
    cum_end = cum[:, rows - 1 : rows]
    decays = jnp.broadcast_to(jnp.exp(cum_end), (heads, LANES))

    end_scale = (jnp.exp(cum_end - cum) * step).T
    for j in range(pairs):
        end_wide[:, j * LANES : (j + 1) * LANES] = expand(end_scale, j)

    follows = me + 1 < sp

    def own_states():
        turned_write = conv[:, width : width + STATE].astype(F32).T.astype(BF16)
        for p in range(pairs):
            at = slice(p * LANES, (p + 1) * LANES)
            weighted = (conv[:, at].astype(F32) * end_wide[:, at]).astype(BF16)
            own_state[p] = jnp.dot(turned_write, weighted, preferred_element_type=F32)

    def state_copy(p):
        there = {"sp": lax.rem(me + 1, sp)}
        return remote(state_out.at[p], state_in.at[p], st_send, st_recv.at[p], there)

    @pl.when(me == 0)
    def _():
        state_in[...] = jnp.zeros(state_in.shape, BF16)
        own_states()
        for p in range(pairs):
            state_out[p] = own_state[p].astype(BF16)

    loaded("k", "v", "forget")
    gall[me] = forget_ref[0]
    gate_cols = forget_ref[0].T

    tail = [
        remote(
            ref.at[0, rows - 16 : rows, :],
            tails.at[:, at],
            tail_sem.at[0],
            tail_sem.at[1],
            {"sp": lax.rem(me + 1, sp)},
        )
        for ref, _, at in inputs
    ]

    def kv_copies(d):
        there = {"sp": lax.rem(me + d, sp)}
        return [
            remote(kvall.at[me], kvall.at[me], kv_sem.at[0], kv_sem.at[1], there),
            remote(gall.at[me], gall.at[me], kv_sem.at[2], kv_sem.at[3], there),
        ]

    @pl.when(follows)
    def _():
        pl.semaphore_wait(ready.at[0], 1)
        for copy in tail:
            copy.start()

    @pl.when(me == 0)
    def _():
        for p in range(pairs):
            state_copy(p).start()

    for d in range(1, sp):

        @pl.when(me + d < sp)
        def _(d=d):
            if d > 1:
                pl.semaphore_wait(ready.at[d - 1], 1)
            for copy in kv_copies(d):
                copy.start()

    for j in range(1, sp):

        @pl.when(j > me)
        def _(j=j):
            kvall[j] = jnp.zeros(kvall.shape[1:], BF16)
            gall[j] = jnp.zeros(gall.shape[1:], F32)

    loaded("q")
    for h in range(heads):
        kv = h // repeat
        piece = (q_ref[0, :, h * HEAD_DIM : (h + 1) * HEAD_DIM].astype(F32) * HEAD_DIM**-0.5).astype(
            BF16
        )
        zero = jnp.zeros((rows, HEAD_DIM), BF16)
        parts = [piece if i == kv else zero for i in range(kv_heads)]
        qs[kv, (h % repeat) * rows : (h % repeat + 1) * rows, :] = jnp.concatenate(parts, axis=1)

    loaded("gate", "gain", "bypass")
    exp_cum = jnp.exp(cum).T
    cum_col = cum.T

    def within():
        conv_write = conv[:, width : width + STATE]
        conv_read = conv[:, width + STATE :]
        inner = lax.dot_general(
            conv_read, conv_write, (((1,), (1,)), ((), ())), preferred_element_type=F32
        )
        causal = row_id >= col_id
        for j in range(pairs):
            tile = conv[:, j * LANES : (j + 1) * LANES]
            parts = []
            for h in (2 * j, 2 * j + 1):
                gap = jnp.where(causal, cum_col[:, h : h + 1] - cum[h : h + 1, :], NEGATIVE)
                weights = (inner * (jnp.exp(gap) * step[h : h + 1, :])).astype(BF16)
                parts.append(jnp.dot(weights, tile, preferred_element_type=F32))
            bypass = jnp.where(low, bypass_ref[2 * j], bypass_ref[2 * j + 1])
            mix[:, j * LANES : (j + 1) * LANES] = (
                jnp.where(low, parts[0], parts[1]) + bypass * tile.astype(F32)
            )

    @pl.when(me > 0)
    def _():
        arrived(tails, tail_sem.at[1])
        pad_ref[0:8, :] = tails[...].astype(F32)[8:16]
        filtered(16)
        own_states()

    @pl.when(me != 1)
    def _():
        within()

    relays = jnp.logical_and(me > 0, follows)

    @pl.when(relays)
    def _():
        for p in range(pairs):
            state_copy(p).wait_recv()
            decay = jnp.where(low, decays[2 * p : 2 * p + 1, :], decays[2 * p + 1 : 2 * p + 2, :])
            state_out[p] = (state_in[p].astype(F32) * decay + own_state[p]).astype(BF16)
            state_copy(p).start()

    @pl.when(me == 1)
    def _():
        within()

    for j in range(1, sp):

        @pl.when(me == j)
        def _(j=j):
            arrived(kvall.at[0:j], kv_sem.at[1])
            arrived(gall.at[0:j], kv_sem.at[3])

    keys = kvall[:, :, 0:kv_width].reshape(sp * rows, -1)
    values = kvall[:, :, kv_width:].reshape(sp * rows, -1)
    visible = [j * rows + col_id <= me * rows + row_id for j in range(sp)]
    for kv in range(kv_heads):
        own = lane // HEAD_DIM == kv
        summed_values = jnp.where(own, values, jnp.ones_like(values))
        scores = lax.dot_general(
            qs[kv], keys, (((1,), (1,)), ((), ())), preferred_element_type=F32
        )
        outs = []
        for i in range(repeat):
            h = kv * repeat + i
            gate_col = gate_cols[:, h : h + 1]
            tiles = [
                jnp.where(
                    visible[j],
                    scores[i * rows : (i + 1) * rows, j * rows : (j + 1) * rows]
                    + (gate_col - gall[j, h : h + 1, :]),
                    NEGATIVE,
                )
                for j in range(sp)
            ]
            top = tiles[0]
            for tile in tiles[1:]:
                top = jnp.maximum(top, tile)
            top = jnp.max(top, axis=1, keepdims=True)
            probs = jnp.concatenate([jnp.exp(tile - top).astype(BF16) for tile in tiles], axis=1)
            both = jnp.dot(probs, summed_values, preferred_element_type=F32)
            turned = pltpu.roll(both, HEAD_DIM, 1)
            outs.append(both / turned if h % 2 == kv else turned / both)
        for i in range(0, repeat, 2):
            at = slice((kv * repeat + i) * HEAD_DIM, (kv * repeat + i + 2) * HEAD_DIM)
            merged = jnp.where(low, outs[i], outs[i + 1]).astype(BF16)
            for r in range(2):
                acts_mine[r, :, at] = merged[r * half : (r + 1) * half]

    def spread(src, dst, send, recv, hop):
        return [
            remote(src.at[r], dst.at[2 + t], send, recv, {"fs": f ^ hop, "tp": r})
            for r in range(2)
        ] + [remote(src.at[1 - t], dst.at[t], send, recv, peer)]

    for copy in spread(acts_mine, acts_in, act_sem.at[0], act_sem.at[1], 2):
        copy.start()

    conv_read = conv[:, width + STATE :]
    squares = []
    for p in range(pairs):
        at = slice(p * LANES, (p + 1) * LANES)

        @pl.when(me == sp - 1)
        def _(p=p):
            state_copy(p).wait_recv()

        carried = jnp.dot(conv_read, state_in[p], preferred_element_type=F32)
        gate = gate_ref[0, :, at].astype(F32)
        u = (mix[:, at] + carried * expand(exp_cum, p)) * (gate * jax.nn.sigmoid(gate))
        squares.append(u * u)
        sent = (u * gain_ref[0:1, at]).astype(BF16)
        for r in range(2):
            pieces_mine[p, r] = sent[r * half : (r + 1) * half]
        recv = piece_recv.at[0 if p < pairs - 1 else 1]
        for copy in spread(pieces_mine.at[p], pieces_in.at[p], piece_send.at[0], recv, 1):
            copy.start()

    total = functools.reduce(jnp.add, squares)
    mean = (
        lax.dot_general(
            jnp.ones((8, LANES), F32),
            total,
            (((1,), (1,)), ((), ())),
            precision=lax.Precision.HIGHEST,
            preferred_element_type=F32,
        )
        / width
    )
    scale = lax.rsqrt(mean + EPSILON)
    scales_mine[0] = scale
    scales_mine[1] = pltpu.roll(scale, half, 1)
    for copy in spread(scales_mine, scales_in, piece_send.at[1], piece_recv.at[2], 1):
        copy.start()

    acts_in[t] = acts_mine[t]
    for p in range(pairs):
        pieces_in[p, t] = pieces_mine[p, t]
    scales_in[t] = scales_mine[t]

    for i, ref in enumerate((wat_x, wst_y)):
        arrived(ref.at[t], weight_recv.at[i])
        weight_copies(2)[i].start()

    def groups(own, other):
        return [(ref, slice(h * part, (h + 1) * part)) for ref in (own, other) for h in range(2)]

    def back(out, landing, g, send, recv, hop):
        return remote(out.at[g], landing.at[g], send, recv, {"fs": f ^ hop})

    arrived(acts_in.at[0:3], act_sem.at[1])
    arrived(wat, weight_recv.at[2])
    left = jnp.concatenate(
        [jnp.concatenate([acts_in[s], acts_in[2 + s]], axis=0) for s in range(2)], axis=1
    )
    for g, (weights, at) in enumerate(groups(wat, wat_x)):
        right = jnp.concatenate([weights[s, :, at] for s in range(2)], axis=0)
        product = jnp.dot(left, right, preferred_element_type=F32)
        acc[g] = product[0:half]
        att_out[g] = product[half:].astype(BF16)
        back(att_out, att_in, g, sum_send.at[0], sum_recv.at[0], 2).start()

    arrived(wst, weight_recv.at[3])
    arrived(pieces_in.at[0 : pairs - 1, 0:3], piece_recv.at[0])
    cut = (pairs - 1) * LANES
    for s in range(2):
        left = jnp.concatenate(
            [
                jnp.concatenate([pieces_in[p, s], pieces_in[p, 2 + s]], axis=0)
                for p in range(pairs - 1)
            ],
            axis=1,
        )
        for g, (weights, at) in enumerate(groups(wst, wst_y)):
            acc_state[g, s] = jnp.dot(left, weights[s, 0:cut, at], preferred_element_type=F32)

    arrived(pieces_in.at[pairs - 1, 0:3], piece_recv.at[1])
    arrived(scales_in.at[0:3], piece_recv.at[2])
    by = [scales_in[i].T[0:half, 0:1] for i in range(4)]

    def state_sum(g, weights, at, slot):
        here = slice(slot // 2 * half, (slot // 2 + 1) * half)
        return functools.reduce(
            jnp.add,
            [
                (
                    acc_state[g, s, here]
                    + jnp.dot(
                        pieces_in[pairs - 1, slot + s],
                        weights[s, cut:, at],
                        preferred_element_type=F32,
                    )
                )
                * by[slot + s]
                for s in range(2)
            ],
        )

    for g, (weights, at) in enumerate(groups(wst, wst_y)):
        sum_out[g] = state_sum(g, weights, at, 2).astype(BF16)
        back(sum_out, sum_in, g, sum_send.at[1], sum_recv.at[1], 1).start()

    def place(owner, h, values):
        at = pl.ds(pl.multiple_of(owner * cols + h * part, part), part)
        out_ref[0, :, at] = values.astype(BF16)

    arrived(att_in, sum_recv.at[0])
    for g, (weights, at) in enumerate(groups(wst, wst_y)):
        mine = state_sum(g, weights, at, 0)
        if g < 2:
            place(f, g, acc[g] + mine)
        else:
            place(f ^ 2, g - 2, att_in[g - 2].astype(F32) + mine)
    arrived(sum_in, sum_recv.at[1])
    for h in range(2):
        place(f ^ 1, h, acc[2 + h] + sum_in[h].astype(F32))
        place(f ^ 3, h, att_in[2 + h].astype(F32) + sum_in[2 + h].astype(F32))

    @pl.when(follows)
    def _():
        departed(tails, tail_sem.at[0])
        departed(state_out, st_send)

    for n in range(1, sp):

        @pl.when(sp - 1 - me == n)
        def _(n=n):
            departed(kvall.at[0:n], kv_sem.at[0])
            departed(gall.at[0:n], kv_sem.at[2])

    for kind in range(3):
        departed(wst, weight_send.at[kind])
    departed(acts_in.at[0:3], act_sem.at[0])
    departed(pieces_in.at[:, 0:3], piece_send.at[0])
    departed(scales_in.at[0:3], piece_send.at[1])
    departed(att_out, sum_send.at[0])
    departed(sum_out, sum_send.at[1])


def fused(sp, fs, *args):
    rows, width = args[0].shape[1:]
    heads = args[4].shape[1]
    deep, cols = args[16].shape
    half, part = rows // 2, cols // 2
    args = list(args)
    args[11] = args[11].reshape(1, -1)
    args[15] = jnp.swapaxes(args[15], 1, 2)
    far = pl.BlockSpec(memory_space=pl.ANY)
    dma = pltpu.SemaphoreType.DMA
    kv_width = args[13].shape[2]
    kv_heads = kv_width // HEAD_DIM
    pairs = heads // 2
    near = [
        (pltpu.SMEM if i in (6, 7) else pltpu.VMEM)(a.shape, a.dtype)
        for i, a in enumerate(args[:16])
        if i not in (13, 14)
    ]
    return pl.pallas_call(
        functools.partial(mixer_kernel, sp, fs),
        out_shape=pltpu.VMEM((1, half, cols * fs), BF16),
        in_specs=[far] * len(args),
        out_specs=pl.BlockSpec(memory_space=pltpu.VMEM),
        scratch_shapes=near
        + [
            dma((len(args),)),
            pltpu.SemaphoreType.REGULAR((sp - 1,)),
            pltpu.VMEM((8 + rows, width + 2 * STATE), F32),
            pltpu.VMEM((16, width + 2 * STATE), BF16),
            pltpu.VMEM((rows, width + 2 * STATE), BF16),
            pltpu.VMEM((rows, width), F32),
            pltpu.VMEM((sp, rows, 2 * kv_width), BF16),
            pltpu.VMEM((sp, heads, rows), F32),
            pltpu.VMEM((kv_heads, heads // kv_heads * rows, kv_width), BF16),
            pltpu.VMEM((pairs, STATE, LANES), F32),
            pltpu.VMEM((pairs, STATE, LANES), BF16),
            pltpu.VMEM((pairs, STATE, LANES), BF16),
            pltpu.VMEM((rows, width), F32),
            pltpu.VMEM((2, deep, cols), BF16),
            pltpu.VMEM((2, deep, cols), BF16),
            pltpu.VMEM((2, deep, cols), BF16),
            pltpu.VMEM((2, deep, cols), BF16),
            pltpu.VMEM((2, half, width), BF16),
            pltpu.VMEM((4, half, width), BF16),
            pltpu.VMEM((pairs, 2, half, LANES), BF16),
            pltpu.VMEM((pairs, 4, half, LANES), BF16),
            pltpu.VMEM((2, 8, rows), F32),
            pltpu.VMEM((4, 8, rows), F32),
            pltpu.VMEM((4, half, part), F32),
            pltpu.VMEM((4, 2, rows, part), F32),
            pltpu.VMEM((4, half, part), BF16),
            pltpu.VMEM((4, half, part), BF16),
            pltpu.VMEM((4, half, part), BF16),
            pltpu.VMEM((4, half, part), BF16),
            dma((2,)),
            dma((4,)),
            dma,
            dma((pairs,)),
            dma((3,)),
            dma((4,)),
            dma((2,)),
            dma((2,)),
            dma((3,)),
            dma((2,)),
            dma((2,)),
        ],
        compiler_params=pltpu.CompilerParams(collective_id=0, has_side_effects=True),
    )(*args)


def one_kernel(*args, sp, fs, tp):
    rows, width = args[0].shape[1:]
    heads = args[4].shape[1]
    return (
        1 < sp <= 8
        and fs == 4
        and tp == 2
        and rows == LANES
        and args[1].shape[2] == STATE == LANES
        and width == heads * HEAD_DIM
        and args[12].shape[2] == width
        and args[13].shape[2] == 2 * HEAD_DIM
        and heads % 4 == 0
        and args[16].shape == args[17].shape == (width, args[16].shape[1])
        and args[16].shape[1] % (2 * LANES) == 0
    )


def solution(mesh):
    in_specs = (
        P("fs", "sp", "tp"),
        P("fs", "sp", "tp"),
        P("fs", "sp", "tp"),
        P("fs", "sp", "tp"),
        P("fs", "tp", "sp"),
        P("fs", "tp", "sp"),
        P("tp"),
        P("tp"),
        P(None, "tp"),
        P(None, "tp"),
        P(None, "tp"),
        P("tp"),
        P("fs", "sp", "tp"),
        P("fs", "sp", "tp"),
        P("fs", "sp", "tp"),
        P("fs", "sp", "tp"),
        P("tp", "fs"),
        P("tp", "fs"),
    )
    out_specs = P("fs", ("sp", "tp"), None)
    sp, fs, tp = (mesh.shape[name] for name in ("sp", "fs", "tp"))

    def body(*args):
        if one_kernel(*args, sp=sp, fs=fs, tp=tp):
            return fused(sp, fs, *args)
        return shards(*args)

    return jax.shard_map(body, mesh=mesh, in_specs=in_specs, out_specs=out_specs, check_vma=False)
```

```python
import functools
import math

import jax
import jax.numpy as jnp
from jax import lax
from jax.experimental import pallas as pl
from jax.experimental.pallas import tpu as pltpu
from jax.sharding import PartitionSpec as P

HEAD_DIM = 64
STATE = 128


EPSILON = 1e-06
NEGATIVE = -1e30


def passed_along(shard, axis, by):
    devices = lax.axis_size(axis)
    pairs = [(i, i + by) for i in range(devices) if 0 <= i + by < devices]
    return lax.ppermute(shard, axis, pairs)


def entering(shard, axis, join, neutral):
    place = lax.axis_index(axis)
    gathered = jax.tree.map(
        lambda a, kind: lax.all_gather(a.astype(kind), axis), shard, (jnp.bfloat16, jnp.bfloat16)
    )
    state = jax.tree.map(lambda a, e: jnp.zeros_like(a) + jnp.asarray(e, a.dtype), shard, neutral)

    def one(hop, state):
        return join(
            state,
            jax.tree.map(
                lambda a, own: lax.dynamic_index_in_dim(a, hop, 0, False).astype(own.dtype),
                gathered,
                shard,
            ),
        )

    return lax.fori_loop(0, place, one, state)


def causal_filter(feeder_quantities, before, taps):
    length = feeder_quantities.shape[0]
    padded = jnp.concatenate([before, feeder_quantities], axis=0).astype(jnp.float32)
    summed = jnp.zeros(feeder_quantities.shape, jnp.float32)
    for offset in range(taps.shape[0]):
        summed = summed + taps[offset].astype(jnp.float32) * padded[offset : offset + length]
    return jax.nn.silu(summed).astype(jnp.bfloat16)


def compose(earlier, later):
    return (earlier[0] * later[0], earlier[1] * later[0][..., None, None] + later[1])


def shards(
    state_head_inputs,
    state_write_vectors,
    state_read_vectors,
    state_output_gate,
    presoftplus_steps,
    extra_decay_log,
    lane_shrinkage_powers,
    bypass_coefficient_vector,
    feeder_smoothing_stencil,
    stored_smoothing_stencil,
    lookup_smoothing_stencil,
    bundled_rescaling_vector,
    queries,
    attention_keys,
    attention_values,
    forget_gate_cumsum,
    state_out_weight,
    attention_out_weight,
):
    shard_rows = state_head_inputs.shape[1]
    input_rows = state_head_inputs[0]
    write_rows = state_write_vectors[0]
    read_rows = state_read_vectors[0]
    tap_rows = feeder_smoothing_stencil.shape[0] - 1
    value_width = input_rows.shape[1]
    vector_width = write_rows.shape[1]
    tail_rows = jnp.concatenate(
        [input_rows[-tap_rows:], write_rows[-tap_rows:], read_rows[-tap_rows:]], axis=1
    )
    before = passed_along(tail_rows, "sp", 1)
    conv_values = causal_filter(input_rows, before[:, :value_width], feeder_smoothing_stencil)
    conv_write = causal_filter(
        write_rows, before[:, value_width : value_width + vector_width], stored_smoothing_stencil
    )
    conv_read = causal_filter(
        read_rows, before[:, value_width + vector_width :], lookup_smoothing_stencil
    )
    stride_duration = jax.nn.softplus(presoftplus_steps[0])
    shrinkage_natural_power = (
        stride_duration * (-jnp.exp(lane_shrinkage_powers))[:, None] + extra_decay_log[0]
    )
    lane_tally = stride_duration.shape[0]
    groups = vector_width // STATE
    per_group = lane_tally // groups
    cumulative = jnp.cumsum(shrinkage_natural_power, axis=1)
    input_heads = conv_values.reshape(shard_rows, groups, per_group, HEAD_DIM)
    write_groups = conv_write.reshape(shard_rows, groups, STATE)
    read_groups = conv_read.reshape(shard_rows, groups, STATE)
    inner_products = jnp.einsum(
        "tgn,sgn->gts", read_groups, write_groups, preferred_element_type=jnp.float32
    )
    positions = jnp.arange(shard_rows)
    causal = positions[:, None] >= positions[None, :]
    log_gap = jnp.where(causal[None], cumulative[:, :, None] - cumulative[:, None, :], -jnp.inf)
    weights = jnp.exp(log_gap) * stride_duration[:, None, :]
    mix_weights = (
        inner_products[:, None] * weights.reshape(groups, per_group, shard_rows, shard_rows)
    ).astype(jnp.bfloat16)
    local_part = jnp.einsum(
        "ghts,sghp->tghp", mix_weights, input_heads, preferred_element_type=jnp.float32
    )
    end_scale = (jnp.exp(cumulative[:, -1:] - cumulative) * stride_duration).T.reshape(
        shard_rows, groups, per_group
    )
    weighted = (input_heads.astype(jnp.float32) * end_scale[..., None]).astype(jnp.bfloat16)
    block_state = jnp.einsum(
        "sghp,sgn->ghpn", weighted, write_groups, preferred_element_type=jnp.float32
    )
    total_decay = jnp.exp(cumulative[:, -1]).reshape(groups, per_group)
    identity = (jnp.ones_like(total_decay), jnp.zeros_like(block_state))
    carried = entering((total_decay, block_state), "sp", compose, identity)[1]
    carried_part = jnp.einsum(
        "tgn,ghpn->tghp",
        read_groups,
        carried.astype(jnp.bfloat16),
        preferred_element_type=jnp.float32,
    )
    carried_part = (
        carried_part * jnp.exp(cumulative).T.reshape(shard_rows, groups, per_group)[..., None]
    )
    mixer_sum = (
        local_part
        + carried_part
        + bypass_coefficient_vector.reshape(groups, per_group)[None, :, :, None]
        * input_heads.astype(jnp.float32)
    )
    gated_rows = mixer_sum.reshape(shard_rows, groups, per_group * HEAD_DIM) * jax.nn.silu(
        state_output_gate[0].astype(jnp.float32)
    ).reshape(shard_rows, groups, -1)
    stretch_coefficient = lax.rsqrt(
        jnp.mean(gated_rows * gated_rows, axis=-1, keepdims=True) + EPSILON
    )
    state_result = (
        (gated_rows * stretch_coefficient * bundled_rescaling_vector.reshape(groups, -1))
        .reshape(shard_rows, -1)
        .astype(jnp.bfloat16)
    )
    attend_heads = forget_gate_cumsum.shape[2]
    key_group_count = attention_keys.shape[2] // HEAD_DIM
    repeat_factor = attend_heads // key_group_count
    query_head_count = queries[0].reshape(shard_rows, key_group_count, repeat_factor, HEAD_DIM)
    first_query = lax.axis_index("sp") * shard_rows
    query_index = first_query + jnp.arange(shard_rows)
    last_query = first_query + shard_rows - 1
    query_gates = forget_gate_cumsum[0].T
    all_gates = lax.all_gather(forget_gate_cumsum[0], "sp", axis=0, tiled=True)
    attention_score_scale = HEAD_DIM ** (-0.5)
    starting = (
        jnp.full((attend_heads, shard_rows), NEGATIVE, jnp.float32),
        jnp.zeros((attend_heads, shard_rows), jnp.float32),
        jnp.zeros((attend_heads, shard_rows, HEAD_DIM), jnp.float32),
    )
    key_rows = lax.all_gather(attention_keys[0], "sp", axis=0, tiled=True)
    value_rows = lax.all_gather(attention_values[0], "sp", axis=0, tiled=True)
    span = key_rows.shape[0]
    sub_block = math.gcd(span, 512)

    def advance(sub_index, running):
        first_key = sub_index * sub_block

        def attend(running):
            running_max, running_sum, weighted_sum = running
            key_tile = lax.dynamic_slice_in_dim(
                key_rows, sub_index * sub_block, sub_block, 0
            ).reshape(sub_block, key_group_count, HEAD_DIM)
            value_tile = lax.dynamic_slice_in_dim(
                value_rows, sub_index * sub_block, sub_block, 0
            ).reshape(sub_block, key_group_count, HEAD_DIM)
            key_gates = lax.dynamic_slice_in_dim(all_gates, first_key, sub_block, 0)
            attention_scores = jnp.einsum(
                "ezxp,czp->zxec", query_head_count, key_tile, preferred_element_type=jnp.float32
            )
            attention_scores = (
                attention_scores.reshape(attend_heads, shard_rows, sub_block)
                * attention_score_scale
            )
            attention_scores = attention_scores + query_gates[:, :, None] - key_gates.T[:, None, :]
            visible = (first_key + jnp.arange(sub_block))[None, :] <= query_index[:, None]
            attention_scores = jnp.where(visible[None], attention_scores, NEGATIVE)
            new_max = jnp.maximum(running_max, jnp.max(attention_scores, axis=-1))
            shrink = jnp.exp(running_max - new_max)
            attention_probs = jnp.where(
                visible[None], jnp.exp(attention_scores - new_max[..., None]), 0.0
            )
            running_sum = running_sum * shrink + jnp.sum(attention_probs, axis=-1)
            weighted_value_sum = jnp.einsum(
                "fljx,xfc->fljc",
                attention_probs.astype(jnp.bfloat16).reshape(
                    key_group_count, repeat_factor, shard_rows, sub_block
                ),
                value_tile,
                preferred_element_type=jnp.float32,
            )
            weighted_sum = weighted_sum * shrink[..., None] + weighted_value_sum.reshape(
                attend_heads, shard_rows, HEAD_DIM
            )
            return (new_max, running_sum, weighted_sum)

        return lax.cond(first_key <= last_query, attend, lambda kept: kept, running)

    _, running_sum, weighted_sum = lax.fori_loop(0, span // sub_block, advance, starting)
    attend_out = (
        (weighted_sum / running_sum[..., None])
        .transpose(1, 0, 2)
        .reshape(shard_rows, -1)
        .astype(jnp.bfloat16)
    )
    state_columns, attend_columns = (
        lax.all_gather(state_out_weight, "fs", axis=1, tiled=True),
        lax.all_gather(attention_out_weight, "fs", axis=1, tiled=True),
    )
    summed = lax.psum_scatter(
        (
            jnp.dot(state_result, state_columns, preferred_element_type=jnp.float32)
            + jnp.dot(attend_out, attend_columns, preferred_element_type=jnp.float32)
        ).astype(jnp.bfloat16),
        "tp",
        scatter_dimension=0,
        tiled=True,
    )
    return summed[None]


MESH = pl.DeviceIdType.MESH
LANES = 128
BF16, F32 = jnp.bfloat16, jnp.float32


def mixer_kernel(
    sp,
    fs,
    x_far,
    w_far,
    r_far,
    gate_far,
    step_far,
    extra_far,
    shrink_far,
    bypass_far,
    tapx_far,
    tapw_far,
    tapr_far,
    gain_far,
    q_far,
    k_far,
    v_far,
    forget_far,
    wst_far,
    wat_far,
    out_ref,
    x_ref,
    w_ref,
    r_ref,
    gate_ref,
    step_ref,
    extra_ref,
    shrink_ref,
    bypass_ref,
    tapx_ref,
    tapw_ref,
    tapr_ref,
    gain_ref,
    q_ref,
    forget_ref,
    load_sem,
    ready,
    pad_ref,
    tails,
    conv,
    end_wide,
    kvall,
    gall,
    qs,
    own_state,
    state_in,
    state_out,
    mix,
    wst,
    wat,
    wst_y,
    wat_x,
    acts_mine,
    acts_in,
    pieces_mine,
    pieces_in,
    scales_mine,
    scales_in,
    acc,
    acc_state,
    att_out,
    att_in,
    sum_out,
    sum_in,
    tail_sem,
    kv_sem,
    st_send,
    st_recv,
    weight_send,
    weight_recv,
    act_sem,
    piece_send,
    piece_recv,
    sum_send,
    sum_recv,
):
    me = lax.axis_index("sp")
    f = lax.axis_index("fs")
    t = lax.axis_index("tp")
    rows, width = x_ref.shape[1], x_ref.shape[2]
    heads = step_ref.shape[1]
    kv_width = k_far.shape[2]
    kv_heads = kv_width // HEAD_DIM
    repeat = heads // kv_heads
    pairs = heads // 2
    taps = tapx_ref.shape[0]
    cols = wst_far.shape[1]
    part = cols // 2
    half = rows // 2
    peer = {"tp": 1 - t}

    barrier = pltpu.get_barrier_semaphore()
    for d in (1, 2):
        for r in range(2):
            pl.semaphore_signal(
                barrier, inc=1, device_id={"fs": f ^ d, "tp": r}, device_id_type=MESH
            )
    pl.semaphore_signal(barrier, inc=1, device_id=peer, device_id_type=MESH)
    for d in range(1, sp):

        @pl.when(me + d < sp)
        def _(d=d):
            pl.semaphore_signal(barrier, inc=1, device_id={"sp": me + d}, device_id_type=MESH)

    @pl.when(me > 0)
    def _():
        pl.semaphore_signal(barrier, inc=1, device_id={"sp": me - 1}, device_id_type=MESH)

    near = {
        "x": (x_far, x_ref),
        "w": (w_far, w_ref),
        "r": (r_far, r_ref),
        "tapx": (tapx_far, tapx_ref),
        "tapw": (tapw_far, tapw_ref),
        "tapr": (tapr_far, tapr_ref),
        "k": (k_far.at[0], kvall.at[me, :, 0:kv_width]),
        "v": (v_far.at[0], kvall.at[me, :, kv_width:]),
        "wat": (wat_far, wat.at[t]),
        "wst": (wst_far, wst.at[t]),
        "step": (step_far, step_ref),
        "extra": (extra_far, extra_ref),
        "shrink": (shrink_far, shrink_ref),
        "forget": (forget_far, forget_ref),
        "q": (q_far, q_ref),
        "gate": (gate_far, gate_ref),
        "gain": (gain_far, gain_ref),
        "bypass": (bypass_far, bypass_ref),
    }
    loads = {
        name: pltpu.make_async_copy(far, here, load_sem.at[i])
        for i, (name, (far, here)) in enumerate(near.items())
    }
    for load in loads.values():
        load.start()

    def loaded(*names):
        for name in names:
            loads[name].wait()

    def remote(src, dst, send, recv, where):
        return pltpu.make_async_remote_copy(
            src_ref=src,
            dst_ref=dst,
            send_sem=send,
            recv_sem=recv,
            device_id=where,
            device_id_type=MESH,
        )

    def arrived(ref, sem):
        remote(ref, ref, sem, sem, peer).wait_recv()

    def departed(ref, sem):
        remote(ref, ref, sem, sem, peer).wait_send()

    follows = me + 1 < sp
    pl.semaphore_wait(barrier, 5 + me + jnp.where(follows, 1, 0))

    for d in range(2, sp):

        @pl.when(me - d >= 0)
        def _(d=d):
            pl.semaphore_signal(
                ready.at[d - 2], inc=1, device_id={"sp": me - d}, device_id_type=MESH
            )

    def weight_copies(kind):
        return (
            (
                remote(wat.at[t], wat_x.at[t], weight_send.at[0], weight_recv.at[0], {"fs": f ^ 1}),
                remote(wst.at[t], wst_y.at[t], weight_send.at[0], weight_recv.at[1], {"fs": f ^ 2}),
            ),
            (
                remote(wat.at[t], wat.at[t], weight_send.at[1], weight_recv.at[2], peer),
                remote(wst.at[t], wst.at[t], weight_send.at[1], weight_recv.at[3], peer),
            ),
            (
                remote(wat_x.at[t], wat_x.at[t], weight_send.at[2], weight_recv.at[2], peer),
                remote(wst_y.at[t], wst_y.at[t], weight_send.at[2], weight_recv.at[3], peer),
            ),
        )[kind]

    loaded("wat", "wst")
    for kind in range(2):
        for copy in weight_copies(kind):
            copy.start()

    lane = lax.broadcasted_iota(jnp.int32, (1, LANES), 1)
    low = lane < HEAD_DIM
    row_id = lax.broadcasted_iota(jnp.int32, (rows, rows), 0)
    col_id = lax.broadcasted_iota(jnp.int32, (rows, rows), 1)

    def expand(columns, j):
        return jnp.where(low, columns[:, 2 * j : 2 * j + 1], columns[:, 2 * j + 1 : 2 * j + 2])

    inputs = (
        (x_ref, tapx_ref, slice(0, width)),
        (w_ref, tapw_ref, slice(width, width + STATE)),
        (r_ref, tapr_ref, slice(width + STATE, width + 2 * STATE)),
    )

    def filtered(count):
        for _, tap_ref, at in inputs:
            total = jnp.zeros((count, at.stop - at.start), F32)
            for i in range(taps):
                first = 8 - (taps - 1) + i
                total = total + tap_ref[i : i + 1, :].astype(F32) * pad_ref[first : first + count, at]
            conv[0:count, at] = (total * jax.nn.sigmoid(total)).astype(BF16)

    pad_ref[0:8, :] = jnp.zeros((8, pad_ref.shape[1]), F32)
    loaded("x", "w", "r", "tapx", "tapw", "tapr")
    for ref, _, at in inputs:
        pad_ref[8 : 8 + rows, at] = ref[0].astype(F32)
    filtered(rows)

    loaded("step", "extra", "shrink")
    head_row = lax.broadcasted_iota(jnp.int32, (heads, rows), 0)
    power = jnp.zeros((heads, rows), F32)
    for h in range(heads):
        power = jnp.where(head_row == h, shrink_ref[h], power)
    presoft = step_ref[0]
    step = jnp.maximum(presoft, 0.0) + jnp.log1p(jnp.exp(-jnp.abs(presoft)))
    log_decay = extra_ref[0] - jnp.exp(power) * step
    upper = (row_id <= col_id).astype(F32)
    cum = jnp.dot(log_decay, upper, precision=lax.Precision.HIGHEST, preferred_element_type=F32)
    cum_end = cum[:, rows - 1 : rows]
    decays = jnp.broadcast_to(jnp.exp(cum_end), (heads, LANES))

    end_scale = (jnp.exp(cum_end - cum) * step).T
    for j in range(pairs):
        end_wide[:, j * LANES : (j + 1) * LANES] = expand(end_scale, j)

    def own_states():
        turned_write = conv[:, width : width + STATE].astype(F32).T.astype(BF16)
        for p in range(pairs):
            at = slice(p * LANES, (p + 1) * LANES)
            weighted = (conv[:, at].astype(F32) * end_wide[:, at]).astype(BF16)
            own_state[p] = jnp.dot(turned_write, weighted, preferred_element_type=F32)

    def state_copy(p):
        there = {"sp": lax.rem(me + 1, sp)}
        return remote(state_out.at[p], state_in.at[p], st_send, st_recv.at[p], there)

    @pl.when(me == 0)
    def _():
        state_in[...] = jnp.zeros(state_in.shape, BF16)
        own_states()
        for p in range(pairs):
            state_out[p] = own_state[p].astype(BF16)

    loaded("k", "v", "forget")
    gall[me] = forget_ref[0]
    gate_cols = forget_ref[0].T

    tail = [
        remote(
            ref.at[0, rows - 16 : rows, :],
            tails.at[:, at],
            tail_sem.at[0],
            tail_sem.at[1],
            {"sp": lax.rem(me + 1, sp)},
        )
        for ref, _, at in inputs
    ]

    def kv_copies(d):
        there = {"sp": lax.rem(me + d, sp)}
        return [
            remote(kvall.at[me], kvall.at[me], kv_sem.at[0], kv_sem.at[1], there),
            remote(gall.at[me], gall.at[me], kv_sem.at[2], kv_sem.at[3], there),
        ]

    @pl.when(follows)
    def _():
        for copy in tail:
            copy.start()

    @pl.when(me == 0)
    def _():
        for p in range(pairs):
            state_copy(p).start()

    for d in range(1, sp):

        @pl.when(me + d < sp)
        def _(d=d):
            if d > 1:
                pl.semaphore_wait(ready.at[d - 2], 1)
            for copy in kv_copies(d):
                copy.start()

    for j in range(1, sp):

        @pl.when(j > me)
        def _(j=j):
            kvall[j] = jnp.zeros(kvall.shape[1:], BF16)
            gall[j] = jnp.zeros(gall.shape[1:], F32)

    loaded("q")
    for h in range(heads):
        kv = h // repeat
        piece = (q_ref[0, :, h * HEAD_DIM : (h + 1) * HEAD_DIM].astype(F32) * HEAD_DIM**-0.5).astype(
            BF16
        )
        zero = jnp.zeros((rows, HEAD_DIM), BF16)
        parts = [piece if i == kv else zero for i in range(kv_heads)]
        qs[kv, (h % repeat) * rows : (h % repeat + 1) * rows, :] = jnp.concatenate(parts, axis=1)

    loaded("gate", "gain", "bypass")
    exp_cum = jnp.exp(cum).T
    cum_col = cum.T

    def within():
        conv_write = conv[:, width : width + STATE]
        conv_read = conv[:, width + STATE :]
        inner = lax.dot_general(
            conv_read, conv_write, (((1,), (1,)), ((), ())), preferred_element_type=F32
        )
        causal = row_id >= col_id
        for j in range(pairs):
            tile = conv[:, j * LANES : (j + 1) * LANES]
            parts = []
            for h in (2 * j, 2 * j + 1):
                gap = jnp.where(causal, cum_col[:, h : h + 1] - cum[h : h + 1, :], NEGATIVE)
                weights = (inner * (jnp.exp(gap) * step[h : h + 1, :])).astype(BF16)
                parts.append(jnp.dot(weights, tile, preferred_element_type=F32))
            bypass = jnp.where(low, bypass_ref[2 * j], bypass_ref[2 * j + 1])
            mix[:, j * LANES : (j + 1) * LANES] = (
                jnp.where(low, parts[0], parts[1]) + bypass * tile.astype(F32)
            )

    @pl.when(me > 0)
    def _():
        arrived(tails, tail_sem.at[1])
        pad_ref[0:8, :] = tails[...].astype(F32)[8:16]
        filtered(16)
        own_states()

    @pl.when(me != 1)
    def _():
        within()

    def relay():
        for p in range(pairs):
            state_copy(p).wait_recv()
            decay = jnp.where(low, decays[2 * p : 2 * p + 1, :], decays[2 * p + 1 : 2 * p + 2, :])
            state_out[p] = (state_in[p].astype(F32) * decay + own_state[p]).astype(BF16)
            state_copy(p).start()

    @pl.when(jnp.logical_and(me == 1, follows))
    def _():
        relay()

    @pl.when(me == 1)
    def _():
        within()

    for j in range(1, sp):

        @pl.when(me == j)
        def _(j=j):
            arrived(kvall.at[0:j], kv_sem.at[1])
            arrived(gall.at[0:j], kv_sem.at[3])

    keys = kvall[:, :, 0:kv_width].reshape(sp * rows, -1)
    values = kvall[:, :, kv_width:].reshape(sp * rows, -1)
    visible = [j * rows + col_id <= me * rows + row_id for j in range(sp)]
    for kv in range(kv_heads):
        own = lane // HEAD_DIM == kv
        summed_values = jnp.where(own, values, jnp.ones_like(values))
        scores = lax.dot_general(
            qs[kv], keys, (((1,), (1,)), ((), ())), preferred_element_type=F32
        )
        outs = []
        for i in range(repeat):
            h = kv * repeat + i
            gate_col = gate_cols[:, h : h + 1]
            tiles = [
                jnp.where(
                    visible[j],
                    scores[i * rows : (i + 1) * rows, j * rows : (j + 1) * rows]
                    + (gate_col - gall[j, h : h + 1, :]),
                    NEGATIVE,
                )
                for j in range(sp)
            ]
            top = tiles[0]
            for tile in tiles[1:]:
                top = jnp.maximum(top, tile)
            top = jnp.max(top, axis=1, keepdims=True)
            probs = jnp.concatenate([jnp.exp(tile - top).astype(BF16) for tile in tiles], axis=1)
            both = jnp.dot(probs, summed_values, preferred_element_type=F32)
            turned = pltpu.roll(both, HEAD_DIM, 1)
            outs.append(both / turned if h % 2 == kv else turned / both)
        for i in range(0, repeat, 2):
            at = slice((kv * repeat + i) * HEAD_DIM, (kv * repeat + i + 2) * HEAD_DIM)
            merged = jnp.where(low, outs[i], outs[i + 1]).astype(BF16)
            for r in range(2):
                acts_mine[r, :, at] = merged[r * half : (r + 1) * half]

    def spread(src, dst, send, recv, hop):
        return [
            remote(src.at[r], dst.at[2 + t], send, recv, {"fs": f ^ hop, "tp": r})
            for r in range(2)
        ] + [remote(src.at[1 - t], dst.at[t], send, recv, peer)]

    for copy in spread(acts_mine, acts_in, act_sem.at[0], act_sem.at[1], 2):
        copy.start()

    @pl.when(jnp.logical_and(me > 1, follows))
    def _():
        relay()

    conv_read = conv[:, width + STATE :]
    squares = []
    for p in range(pairs):
        at = slice(p * LANES, (p + 1) * LANES)

        @pl.when(me == sp - 1)
        def _(p=p):
            state_copy(p).wait_recv()

        carried = jnp.dot(conv_read, state_in[p], preferred_element_type=F32)
        gate = gate_ref[0, :, at].astype(F32)
        u = (mix[:, at] + carried * expand(exp_cum, p)) * (gate * jax.nn.sigmoid(gate))
        squares.append(u * u)
        sent = (u * gain_ref[0:1, at]).astype(BF16)
        for r in range(2):
            pieces_mine[p, r] = sent[r * half : (r + 1) * half]
        recv = piece_recv.at[0 if p < pairs - 1 else 1]
        for copy in spread(pieces_mine.at[p], pieces_in.at[p], piece_send.at[0], recv, 1):
            copy.start()

    total = functools.reduce(jnp.add, squares)
    coarse = total.astype(BF16)
    fine = (total - coarse.astype(F32)).astype(BF16)
    mean = (
        lax.dot_general(
            jnp.ones((8, 2 * LANES), BF16),
            jnp.concatenate([coarse, fine], axis=1),
            (((1,), (1,)), ((), ())),
            preferred_element_type=F32,
        )
        / width
    )
    scale = lax.rsqrt(mean + EPSILON)
    scales_mine[0] = scale
    scales_mine[1] = pltpu.roll(scale, half, 1)
    for copy in spread(scales_mine, scales_in, piece_send.at[1], piece_recv.at[2], 1):
        copy.start()

    acts_in[t] = acts_mine[t]
    for p in range(pairs):
        pieces_in[p, t] = pieces_mine[p, t]
    scales_in[t] = scales_mine[t]

    for i, ref in enumerate((wat_x, wst_y)):
        arrived(ref.at[t], weight_recv.at[i])
        weight_copies(2)[i].start()

    def groups(own, other):
        return [(ref, slice(h * part, (h + 1) * part)) for ref in (own, other) for h in range(2)]

    def back(out, landing, g, send, recv, hop):
        return remote(out.at[g], landing.at[g], send, recv, {"fs": f ^ hop})

    arrived(acts_in.at[0:3], act_sem.at[1])
    arrived(wat, weight_recv.at[2])
    left = jnp.concatenate(
        [jnp.concatenate([acts_in[s], acts_in[2 + s]], axis=0) for s in range(2)], axis=1
    )
    for pair in (0, 2):
        for g, (weights, at) in list(enumerate(groups(wat, wat_x)))[pair : pair + 2]:
            right = jnp.concatenate([weights[s, :, at] for s in range(2)], axis=0)
            product = jnp.dot(left, right, preferred_element_type=F32)
            acc[g] = product[0:half]
            att_out[g] = product[half:].astype(BF16)
        for g in (pair, pair + 1):
            back(att_out, att_in, g, sum_send.at[0], sum_recv.at[0], 2).start()

    arrived(wst, weight_recv.at[3])
    arrived(pieces_in.at[0 : pairs - 1, 0:3], piece_recv.at[0])
    cut = (pairs - 1) * LANES
    for s in range(2):
        left = jnp.concatenate(
            [
                jnp.concatenate([pieces_in[p, s], pieces_in[p, 2 + s]], axis=0)
                for p in range(pairs - 1)
            ],
            axis=1,
        )
        for g, (weights, at) in enumerate(groups(wst, wst_y)):
            acc_state[g, s] = jnp.dot(left, weights[s, 0:cut, at], preferred_element_type=F32)

    arrived(pieces_in.at[pairs - 1, 0:3], piece_recv.at[1])
    arrived(scales_in.at[0:3], piece_recv.at[2])
    upright = scales_in[...].reshape(4 * 8, rows).T
    by = [upright[0:half, 8 * i : 8 * i + 1] for i in range(4)]

    def state_sum(g, weights, at, slot):
        here = slice(slot // 2 * half, (slot // 2 + 1) * half)
        return functools.reduce(
            jnp.add,
            [
                (
                    acc_state[g, s, here]
                    + jnp.dot(
                        pieces_in[pairs - 1, slot + s],
                        weights[s, cut:, at],
                        preferred_element_type=F32,
                    )
                )
                * by[slot + s]
                for s in range(2)
            ],
        )

    for pair in (0, 2):
        for g, (weights, at) in list(enumerate(groups(wst, wst_y)))[pair : pair + 2]:
            sum_out[g] = state_sum(g, weights, at, 2).astype(BF16)
        for g in (pair, pair + 1):
            back(sum_out, sum_in, g, sum_send.at[1], sum_recv.at[1], 1).start()

    def place(owner, h, values):
        at = pl.ds(pl.multiple_of(owner * cols + h * part, part), part)
        out_ref[0, :, at] = values.astype(BF16)

    arrived(att_in, sum_recv.at[0])
    for g, (weights, at) in enumerate(groups(wst, wst_y)):
        mine = state_sum(g, weights, at, 0)
        if g < 2:
            place(f, g, acc[g] + mine)
        else:
            place(f ^ 2, g - 2, att_in[g - 2].astype(F32) + mine)
    arrived(sum_in, sum_recv.at[1])
    for h in range(2):
        place(f ^ 1, h, acc[2 + h] + sum_in[h].astype(F32))
        place(f ^ 3, h, att_in[2 + h].astype(F32) + sum_in[2 + h].astype(F32))

    @pl.when(follows)
    def _():
        departed(tails, tail_sem.at[0])
        departed(state_out, st_send)

    for n in range(1, sp):

        @pl.when(sp - 1 - me == n)
        def _(n=n):
            departed(kvall.at[0:n], kv_sem.at[0])
            departed(gall.at[0:n], kv_sem.at[2])

    for kind in range(3):
        departed(wst, weight_send.at[kind])
    departed(acts_in.at[0:3], act_sem.at[0])
    departed(pieces_in.at[:, 0:3], piece_send.at[0])
    departed(scales_in.at[0:3], piece_send.at[1])
    departed(att_out, sum_send.at[0])
    departed(sum_out, sum_send.at[1])


def fused(sp, fs, *args):
    rows, width = args[0].shape[1:]
    heads = args[4].shape[1]
    deep, cols = args[16].shape
    half, part = rows // 2, cols // 2
    args = list(args)
    args[11] = args[11].reshape(1, -1)
    args[15] = jnp.swapaxes(args[15], 1, 2)
    far = pl.BlockSpec(memory_space=pl.ANY)
    dma = pltpu.SemaphoreType.DMA
    kv_width = args[13].shape[2]
    kv_heads = kv_width // HEAD_DIM
    pairs = heads // 2
    near = [
        (pltpu.SMEM if i in (6, 7) else pltpu.VMEM)(a.shape, a.dtype)
        for i, a in enumerate(args[:16])
        if i not in (13, 14)
    ]
    return pl.pallas_call(
        functools.partial(mixer_kernel, sp, fs),
        out_shape=pltpu.VMEM((1, half, cols * fs), BF16),
        in_specs=[far] * len(args),
        out_specs=pl.BlockSpec(memory_space=pltpu.VMEM),
        scratch_shapes=near
        + [
            dma((len(args),)),
            pltpu.SemaphoreType.REGULAR((max(sp - 2, 1),)),
            pltpu.VMEM((8 + rows, width + 2 * STATE), F32),
            pltpu.VMEM((16, width + 2 * STATE), BF16),
            pltpu.VMEM((rows, width + 2 * STATE), BF16),
            pltpu.VMEM((rows, width), F32),
            pltpu.VMEM((sp, rows, 2 * kv_width), BF16),
            pltpu.VMEM((sp, heads, rows), F32),
            pltpu.VMEM((kv_heads, heads // kv_heads * rows, kv_width), BF16),
            pltpu.VMEM((pairs, STATE, LANES), F32),
            pltpu.VMEM((pairs, STATE, LANES), BF16),
            pltpu.VMEM((pairs, STATE, LANES), BF16),
            pltpu.VMEM((rows, width), F32),
            pltpu.VMEM((2, deep, cols), BF16),
            pltpu.VMEM((2, deep, cols), BF16),
            pltpu.VMEM((2, deep, cols), BF16),
            pltpu.VMEM((2, deep, cols), BF16),
            pltpu.VMEM((2, half, width), BF16),
            pltpu.VMEM((4, half, width), BF16),
            pltpu.VMEM((pairs, 2, half, LANES), BF16),
            pltpu.VMEM((pairs, 4, half, LANES), BF16),
            pltpu.VMEM((2, 8, rows), F32),
            pltpu.VMEM((4, 8, rows), F32),
            pltpu.VMEM((4, half, part), F32),
            pltpu.VMEM((4, 2, rows, part), F32),
            pltpu.VMEM((4, half, part), BF16),
            pltpu.VMEM((4, half, part), BF16),
            pltpu.VMEM((4, half, part), BF16),
            pltpu.VMEM((4, half, part), BF16),
            dma((2,)),
            dma((4,)),
            dma,
            dma((pairs,)),
            dma((3,)),
            dma((4,)),
            dma((2,)),
            dma((2,)),
            dma((3,)),
            dma((2,)),
            dma((2,)),
        ],
        compiler_params=pltpu.CompilerParams(collective_id=0, has_side_effects=True),
    )(*args)


def one_kernel(*args, sp, fs, tp):
    rows, width = args[0].shape[1:]
    heads = args[4].shape[1]
    return (
        1 < sp <= 8
        and fs == 4
        and tp == 2
        and rows == LANES
        and args[1].shape[2] == STATE == LANES
        and width == heads * HEAD_DIM
        and args[12].shape[2] == width
        and args[13].shape[2] == 2 * HEAD_DIM
        and heads % 4 == 0
        and args[16].shape == args[17].shape == (width, args[16].shape[1])
        and args[16].shape[1] % (2 * LANES) == 0
    )


def solution(mesh):
    in_specs = (
        P("fs", "sp", "tp"),
        P("fs", "sp", "tp"),
        P("fs", "sp", "tp"),
        P("fs", "sp", "tp"),
        P("fs", "tp", "sp"),
        P("fs", "tp", "sp"),
        P("tp"),
        P("tp"),
        P(None, "tp"),
        P(None, "tp"),
        P(None, "tp"),
        P("tp"),
        P("fs", "sp", "tp"),
        P("fs", "sp", "tp"),
        P("fs", "sp", "tp"),
        P("fs", "sp", "tp"),
        P("tp", "fs"),
        P("tp", "fs"),
    )
    out_specs = P("fs", ("sp", "tp"), None)
    sp, fs, tp = (mesh.shape[name] for name in ("sp", "fs", "tp"))

    def body(*args):
        if one_kernel(*args, sp=sp, fs=fs, tp=tp):
            return fused(sp, fs, *args)
        return shards(*args)

    return jax.shard_map(body, mesh=mesh, in_specs=in_specs, out_specs=out_specs, check_vma=False)
```

```python
import functools
import math

import jax
import jax.numpy as jnp
from jax import lax
from jax.experimental import pallas as pl
from jax.experimental.pallas import tpu as pltpu
from jax.sharding import PartitionSpec as P

HEAD_DIM = 64
STATE = 128


EPSILON = 1e-06
NEGATIVE = -1e30


def passed_along(shard, axis, by):
    devices = lax.axis_size(axis)
    pairs = [(i, i + by) for i in range(devices) if 0 <= i + by < devices]
    return lax.ppermute(shard, axis, pairs)


def entering(shard, axis, join, neutral):
    place = lax.axis_index(axis)
    gathered = jax.tree.map(
        lambda a, kind: lax.all_gather(a.astype(kind), axis), shard, (jnp.bfloat16, jnp.bfloat16)
    )
    state = jax.tree.map(lambda a, e: jnp.zeros_like(a) + jnp.asarray(e, a.dtype), shard, neutral)

    def one(hop, state):
        return join(
            state,
            jax.tree.map(
                lambda a, own: lax.dynamic_index_in_dim(a, hop, 0, False).astype(own.dtype),
                gathered,
                shard,
            ),
        )

    return lax.fori_loop(0, place, one, state)


def causal_filter(feeder_quantities, before, taps):
    length = feeder_quantities.shape[0]
    padded = jnp.concatenate([before, feeder_quantities], axis=0).astype(jnp.float32)
    summed = jnp.zeros(feeder_quantities.shape, jnp.float32)
    for offset in range(taps.shape[0]):
        summed = summed + taps[offset].astype(jnp.float32) * padded[offset : offset + length]
    return jax.nn.silu(summed).astype(jnp.bfloat16)


def compose(earlier, later):
    return (earlier[0] * later[0], earlier[1] * later[0][..., None, None] + later[1])


def shards(
    state_head_inputs,
    state_write_vectors,
    state_read_vectors,
    state_output_gate,
    presoftplus_steps,
    extra_decay_log,
    lane_shrinkage_powers,
    bypass_coefficient_vector,
    feeder_smoothing_stencil,
    stored_smoothing_stencil,
    lookup_smoothing_stencil,
    bundled_rescaling_vector,
    queries,
    attention_keys,
    attention_values,
    forget_gate_cumsum,
    state_out_weight,
    attention_out_weight,
):
    shard_rows = state_head_inputs.shape[1]
    input_rows = state_head_inputs[0]
    write_rows = state_write_vectors[0]
    read_rows = state_read_vectors[0]
    tap_rows = feeder_smoothing_stencil.shape[0] - 1
    value_width = input_rows.shape[1]
    vector_width = write_rows.shape[1]
    tail_rows = jnp.concatenate(
        [input_rows[-tap_rows:], write_rows[-tap_rows:], read_rows[-tap_rows:]], axis=1
    )
    before = passed_along(tail_rows, "sp", 1)
    conv_values = causal_filter(input_rows, before[:, :value_width], feeder_smoothing_stencil)
    conv_write = causal_filter(
        write_rows, before[:, value_width : value_width + vector_width], stored_smoothing_stencil
    )
    conv_read = causal_filter(
        read_rows, before[:, value_width + vector_width :], lookup_smoothing_stencil
    )
    stride_duration = jax.nn.softplus(presoftplus_steps[0])
    shrinkage_natural_power = (
        stride_duration * (-jnp.exp(lane_shrinkage_powers))[:, None] + extra_decay_log[0]
    )
    lane_tally = stride_duration.shape[0]
    groups = vector_width // STATE
    per_group = lane_tally // groups
    cumulative = jnp.cumsum(shrinkage_natural_power, axis=1)
    input_heads = conv_values.reshape(shard_rows, groups, per_group, HEAD_DIM)
    write_groups = conv_write.reshape(shard_rows, groups, STATE)
    read_groups = conv_read.reshape(shard_rows, groups, STATE)
    inner_products = jnp.einsum(
        "tgn,sgn->gts", read_groups, write_groups, preferred_element_type=jnp.float32
    )
    positions = jnp.arange(shard_rows)
    causal = positions[:, None] >= positions[None, :]
    log_gap = jnp.where(causal[None], cumulative[:, :, None] - cumulative[:, None, :], -jnp.inf)
    weights = jnp.exp(log_gap) * stride_duration[:, None, :]
    mix_weights = (
        inner_products[:, None] * weights.reshape(groups, per_group, shard_rows, shard_rows)
    ).astype(jnp.bfloat16)
    local_part = jnp.einsum(
        "ghts,sghp->tghp", mix_weights, input_heads, preferred_element_type=jnp.float32
    )
    end_scale = (jnp.exp(cumulative[:, -1:] - cumulative) * stride_duration).T.reshape(
        shard_rows, groups, per_group
    )
    weighted = (input_heads.astype(jnp.float32) * end_scale[..., None]).astype(jnp.bfloat16)
    block_state = jnp.einsum(
        "sghp,sgn->ghpn", weighted, write_groups, preferred_element_type=jnp.float32
    )
    total_decay = jnp.exp(cumulative[:, -1]).reshape(groups, per_group)
    identity = (jnp.ones_like(total_decay), jnp.zeros_like(block_state))
    carried = entering((total_decay, block_state), "sp", compose, identity)[1]
    carried_part = jnp.einsum(
        "tgn,ghpn->tghp",
        read_groups,
        carried.astype(jnp.bfloat16),
        preferred_element_type=jnp.float32,
    )
    carried_part = (
        carried_part * jnp.exp(cumulative).T.reshape(shard_rows, groups, per_group)[..., None]
    )
    mixer_sum = (
        local_part
        + carried_part
        + bypass_coefficient_vector.reshape(groups, per_group)[None, :, :, None]
        * input_heads.astype(jnp.float32)
    )
    gated_rows = mixer_sum.reshape(shard_rows, groups, per_group * HEAD_DIM) * jax.nn.silu(
        state_output_gate[0].astype(jnp.float32)
    ).reshape(shard_rows, groups, -1)
    stretch_coefficient = lax.rsqrt(
        jnp.mean(gated_rows * gated_rows, axis=-1, keepdims=True) + EPSILON
    )
    state_result = (
        (gated_rows * stretch_coefficient * bundled_rescaling_vector.reshape(groups, -1))
        .reshape(shard_rows, -1)
        .astype(jnp.bfloat16)
    )
    attend_heads = forget_gate_cumsum.shape[2]
    key_group_count = attention_keys.shape[2] // HEAD_DIM
    repeat_factor = attend_heads // key_group_count
    query_head_count = queries[0].reshape(shard_rows, key_group_count, repeat_factor, HEAD_DIM)
    first_query = lax.axis_index("sp") * shard_rows
    query_index = first_query + jnp.arange(shard_rows)
    last_query = first_query + shard_rows - 1
    query_gates = forget_gate_cumsum[0].T
    all_gates = lax.all_gather(forget_gate_cumsum[0], "sp", axis=0, tiled=True)
    attention_score_scale = HEAD_DIM ** (-0.5)
    starting = (
        jnp.full((attend_heads, shard_rows), NEGATIVE, jnp.float32),
        jnp.zeros((attend_heads, shard_rows), jnp.float32),
        jnp.zeros((attend_heads, shard_rows, HEAD_DIM), jnp.float32),
    )
    key_rows = lax.all_gather(attention_keys[0], "sp", axis=0, tiled=True)
    value_rows = lax.all_gather(attention_values[0], "sp", axis=0, tiled=True)
    span = key_rows.shape[0]
    sub_block = math.gcd(span, 512)

    def advance(sub_index, running):
        first_key = sub_index * sub_block

        def attend(running):
            running_max, running_sum, weighted_sum = running
            key_tile = lax.dynamic_slice_in_dim(
                key_rows, sub_index * sub_block, sub_block, 0
            ).reshape(sub_block, key_group_count, HEAD_DIM)
            value_tile = lax.dynamic_slice_in_dim(
                value_rows, sub_index * sub_block, sub_block, 0
            ).reshape(sub_block, key_group_count, HEAD_DIM)
            key_gates = lax.dynamic_slice_in_dim(all_gates, first_key, sub_block, 0)
            attention_scores = jnp.einsum(
                "ezxp,czp->zxec", query_head_count, key_tile, preferred_element_type=jnp.float32
            )
            attention_scores = (
                attention_scores.reshape(attend_heads, shard_rows, sub_block)
                * attention_score_scale
            )
            attention_scores = attention_scores + query_gates[:, :, None] - key_gates.T[:, None, :]
            visible = (first_key + jnp.arange(sub_block))[None, :] <= query_index[:, None]
            attention_scores = jnp.where(visible[None], attention_scores, NEGATIVE)
            new_max = jnp.maximum(running_max, jnp.max(attention_scores, axis=-1))
            shrink = jnp.exp(running_max - new_max)
            attention_probs = jnp.where(
                visible[None], jnp.exp(attention_scores - new_max[..., None]), 0.0
            )
            running_sum = running_sum * shrink + jnp.sum(attention_probs, axis=-1)
            weighted_value_sum = jnp.einsum(
                "fljx,xfc->fljc",
                attention_probs.astype(jnp.bfloat16).reshape(
                    key_group_count, repeat_factor, shard_rows, sub_block
                ),
                value_tile,
                preferred_element_type=jnp.float32,
            )
            weighted_sum = weighted_sum * shrink[..., None] + weighted_value_sum.reshape(
                attend_heads, shard_rows, HEAD_DIM
            )
            return (new_max, running_sum, weighted_sum)

        return lax.cond(first_key <= last_query, attend, lambda kept: kept, running)

    _, running_sum, weighted_sum = lax.fori_loop(0, span // sub_block, advance, starting)
    attend_out = (
        (weighted_sum / running_sum[..., None])
        .transpose(1, 0, 2)
        .reshape(shard_rows, -1)
        .astype(jnp.bfloat16)
    )
    state_columns, attend_columns = (
        lax.all_gather(state_out_weight, "fs", axis=1, tiled=True),
        lax.all_gather(attention_out_weight, "fs", axis=1, tiled=True),
    )
    summed = lax.psum_scatter(
        (
            jnp.dot(state_result, state_columns, preferred_element_type=jnp.float32)
            + jnp.dot(attend_out, attend_columns, preferred_element_type=jnp.float32)
        ).astype(jnp.bfloat16),
        "tp",
        scatter_dimension=0,
        tiled=True,
    )
    return summed[None]


MESH = pl.DeviceIdType.MESH
LANES = 128
BF16, F32 = jnp.bfloat16, jnp.float32


def mixer_kernel(
    sp,
    fs,
    x_far,
    w_far,
    r_far,
    gate_far,
    step_far,
    extra_far,
    shrink_far,
    bypass_far,
    tapx_far,
    tapw_far,
    tapr_far,
    gain_far,
    q_far,
    k_far,
    v_far,
    forget_far,
    wst_far,
    wat_far,
    out_ref,
    x_ref,
    w_ref,
    r_ref,
    gate_ref,
    step_ref,
    extra_ref,
    shrink_ref,
    bypass_ref,
    tapx_ref,
    tapw_ref,
    tapr_ref,
    gain_ref,
    q_ref,
    forget_ref,
    load_sem,
    ready,
    pad_ref,
    tails,
    conv,
    soft_cum,
    end_wide,
    kvall,
    gall,
    qs,
    own_state,
    state_in,
    state_out,
    mix,
    wst,
    wat,
    wst_y,
    wat_x,
    acts_mine,
    acts_in,
    pieces_mine,
    pieces_in,
    scales_mine,
    scales_in,
    acc,
    att_out,
    att_in,
    sum_out,
    sum_in,
    tail_sem,
    kv_sem,
    st_send,
    st_recv,
    weight_send,
    weight_recv,
    peer_recv,
    act_send,
    act_recv,
    piece_send,
    piece_recv,
    scale_recv,
    sum_send,
    sum_recv,
):
    me = lax.axis_index("sp")
    f = lax.axis_index("fs")
    t = lax.axis_index("tp")
    rows, width = x_ref.shape[1], x_ref.shape[2]
    heads = step_ref.shape[1]
    kv_width = k_far.shape[2]
    kv_heads = kv_width // HEAD_DIM
    repeat = heads // kv_heads
    pairs = heads // 2
    taps = tapx_ref.shape[0]
    cols = wst_far.shape[1]
    part = cols // 2
    half = rows // 2
    peer = {"tp": 1 - t}

    barrier = pltpu.get_barrier_semaphore()
    for d in (1, 2):
        for r in range(2):
            pl.semaphore_signal(
                barrier, inc=1, device_id={"fs": f ^ d, "tp": r}, device_id_type=MESH
            )
    pl.semaphore_signal(barrier, inc=1, device_id=peer, device_id_type=MESH)
    for d in range(1, sp):

        @pl.when(me + d < sp)
        def _(d=d):
            pl.semaphore_signal(barrier, inc=1, device_id={"sp": me + d}, device_id_type=MESH)

    @pl.when(me > 0)
    def _():
        pl.semaphore_signal(barrier, inc=1, device_id={"sp": me - 1}, device_id_type=MESH)

    near = {
        "x": (x_far, x_ref),
        "w": (w_far, w_ref),
        "r": (r_far, r_ref),
        "tapx": (tapx_far, tapx_ref),
        "tapw": (tapw_far, tapw_ref),
        "tapr": (tapr_far, tapr_ref),
        "k": (k_far.at[0], kvall.at[me, :, 0:kv_width]),
        "v": (v_far.at[0], kvall.at[me, :, kv_width:]),
        "wat": (wat_far, wat.at[t]),
        "wst": (wst_far, wst.at[t]),
        "step": (step_far, step_ref),
        "extra": (extra_far, extra_ref),
        "shrink": (shrink_far, shrink_ref),
        "forget": (forget_far, forget_ref),
        "q": (q_far, q_ref),
        "gate": (gate_far, gate_ref),
        "gain": (gain_far, gain_ref),
        "bypass": (bypass_far, bypass_ref),
    }
    loads = {
        name: pltpu.make_async_copy(far, here, load_sem.at[i])
        for i, (name, (far, here)) in enumerate(near.items())
    }
    for load in loads.values():
        load.start()

    def loaded(*names):
        for name in names:
            loads[name].wait()

    def remote(src, dst, send, recv, where):
        return pltpu.make_async_remote_copy(
            src_ref=src,
            dst_ref=dst,
            send_sem=send,
            recv_sem=recv,
            device_id=where,
            device_id_type=MESH,
        )

    def arrived(ref, sem):
        remote(ref, ref, sem, sem, peer).wait_recv()

    def departed(ref, sem):
        remote(ref, ref, sem, sem, peer).wait_send()

    lane = lax.broadcasted_iota(jnp.int32, (1, LANES), 1)
    low = lane < HEAD_DIM
    row_id = lax.broadcasted_iota(jnp.int32, (rows, rows), 0)
    col_id = lax.broadcasted_iota(jnp.int32, (rows, rows), 1)

    def expand(columns, j):
        return jnp.where(low, columns[:, 2 * j : 2 * j + 1], columns[:, 2 * j + 1 : 2 * j + 2])

    inputs = (
        (x_ref, tapx_ref, slice(0, width)),
        (w_ref, tapw_ref, slice(width, width + STATE)),
        (r_ref, tapr_ref, slice(width + STATE, width + 2 * STATE)),
    )

    def filtered(count):
        for _, tap_ref, at in inputs:
            total = jnp.zeros((count, at.stop - at.start), F32)
            for i in range(taps):
                first = 8 - (taps - 1) + i
                total = total + tap_ref[i : i + 1, :].astype(F32) * pad_ref[first : first + count, at]
            conv[0:count, at] = (total * jax.nn.sigmoid(total)).astype(BF16)

    pad_ref[0:8, :] = jnp.zeros((8, pad_ref.shape[1]), F32)
    loaded("x", "w", "r", "tapx", "tapw", "tapr")
    for ref, _, at in inputs:
        pad_ref[8 : 8 + rows, at] = ref[0].astype(F32)
    filtered(rows)

    def decay():
        loaded("step", "extra", "shrink")
        head_row = lax.broadcasted_iota(jnp.int32, (heads, rows), 0)
        power = jnp.zeros((heads, rows), F32)
        for h in range(heads):
            power = jnp.where(head_row == h, shrink_ref[h], power)
        presoft = step_ref[0]
        step = jnp.maximum(presoft, 0.0) + jnp.log1p(jnp.exp(-jnp.abs(presoft)))
        log_decay = extra_ref[0] - jnp.exp(power) * step
        upper = (row_id <= col_id).astype(F32)
        cum = jnp.dot(log_decay, upper, precision=lax.Precision.HIGHEST, preferred_element_type=F32)
        soft_cum[0] = step
        soft_cum[1] = cum
        end_scale = (jnp.exp(cum[:, rows - 1 : rows] - cum) * step).T
        for j in range(pairs):
            end_wide[:, j * LANES : (j + 1) * LANES] = expand(end_scale, j)

    def own_states():
        turned_write = conv[:, width : width + STATE].astype(F32).T.astype(BF16)
        for p in range(pairs):
            at = slice(p * LANES, (p + 1) * LANES)
            weighted = (conv[:, at].astype(F32) * end_wide[:, at]).astype(BF16)
            own_state[p] = jnp.dot(turned_write, weighted, preferred_element_type=F32)

    @pl.when(me == 0)
    def _():
        state_in[...] = jnp.zeros(state_in.shape, BF16)
        decay()
        own_states()
        for p in range(pairs):
            state_out[p] = own_state[p].astype(BF16)

    follows = me + 1 < sp
    pl.semaphore_wait(barrier, 5 + me + jnp.where(follows, 1, 0))

    for d in range(2, sp):

        @pl.when(me - d >= 0)
        def _(d=d):
            pl.semaphore_signal(
                ready.at[d - 2], inc=1, device_id={"sp": me - d}, device_id_type=MESH
            )

    deep = wst_far.shape[0]
    chunks = (slice(0, deep * 3 // 4), slice(deep * 3 // 4, deep))

    def weight_copies(chunk):
        at = (t, chunks[chunk])
        return [
            remote(
                src.at[at], dst.at[at], weight_send.at[0], weight_recv.at[i, chunk], {"fs": f ^ hop}
            )
            for i, (src, dst, hop) in enumerate(((wat, wat_x, 1), (wst, wst_y, 2)))
        ]

    def own_copies():
        return [
            remote(w.at[t], w.at[t], weight_send.at[1], peer_recv.at[0], peer) for w in (wat, wst)
        ]

    def relay_copies(chunk):
        at = (t, chunks[chunk])
        return [
            remote(w.at[at], w.at[at], weight_send.at[2], peer_recv.at[1], peer)
            for w in (wat_x, wst_y)
        ]

    loaded("wat", "wst")
    for copy in weight_copies(0) + weight_copies(1) + own_copies():
        copy.start()

    @pl.when(me > 0)
    def _():
        decay()

    step, cum = soft_cum[0], soft_cum[1]
    decays = jnp.broadcast_to(jnp.exp(cum[:, rows - 1 : rows]), (heads, LANES))

    def state_copy(p):
        there = {"sp": lax.rem(me + 1, sp)}
        return remote(state_out.at[p], state_in.at[p], st_send, st_recv.at[p], there)

    loaded("k", "v", "forget")
    gall[me] = forget_ref[0]
    gate_cols = forget_ref[0].T

    tail = [
        remote(
            ref.at[0, rows - 16 : rows, :],
            tails.at[:, at],
            tail_sem.at[0],
            tail_sem.at[1],
            {"sp": lax.rem(me + 1, sp)},
        )
        for ref, _, at in inputs
    ]

    def kv_copies(d):
        there = {"sp": lax.rem(me + d, sp)}
        return [
            remote(kvall.at[me], kvall.at[me], kv_sem.at[0], kv_sem.at[1], there),
            remote(gall.at[me], gall.at[me], kv_sem.at[2], kv_sem.at[3], there),
        ]

    @pl.when(follows)
    def _():
        for copy in tail:
            copy.start()

    @pl.when(me == 0)
    def _():
        for p in range(pairs):
            state_copy(p).start()

    @pl.when(follows)
    def _():
        for copy in kv_copies(1):
            copy.start()

    def far_kv(fits):
        for d in range(2, sp):

            @pl.when(jnp.logical_and(fits, me + d < sp))
            def _(d=d):
                pl.semaphore_wait(ready.at[d - 2], 1)
                for copy in kv_copies(d):
                    copy.start()

    far_kv(me > 0)

    for j in range(1, sp):

        @pl.when(j > me)
        def _(j=j):
            kvall[j] = jnp.zeros(kvall.shape[1:], BF16)
            gall[j] = jnp.zeros(gall.shape[1:], F32)

    loaded("q")
    for h in range(heads):
        kv = h // repeat
        piece = (q_ref[0, :, h * HEAD_DIM : (h + 1) * HEAD_DIM].astype(F32) * HEAD_DIM**-0.5).astype(
            BF16
        )
        zero = jnp.zeros((rows, HEAD_DIM), BF16)
        parts = [piece if i == kv else zero for i in range(kv_heads)]
        qs[kv, (h % repeat) * rows : (h % repeat + 1) * rows, :] = jnp.concatenate(parts, axis=1)

    loaded("gate", "gain", "bypass")
    exp_cum = jnp.exp(cum).T
    cum_col = cum.T

    def within():
        conv_write = conv[:, width : width + STATE]
        conv_read = conv[:, width + STATE :]
        inner = lax.dot_general(
            conv_read, conv_write, (((1,), (1,)), ((), ())), preferred_element_type=F32
        )
        causal = row_id >= col_id
        for j in range(pairs):
            tile = conv[:, j * LANES : (j + 1) * LANES]
            parts = []
            for h in (2 * j, 2 * j + 1):
                gap = jnp.where(causal, cum_col[:, h : h + 1] - cum[h : h + 1, :], NEGATIVE)
                weights = (inner * (jnp.exp(gap) * step[h : h + 1, :])).astype(BF16)
                parts.append(jnp.dot(weights, tile, preferred_element_type=F32))
            bypass = jnp.where(low, bypass_ref[2 * j], bypass_ref[2 * j + 1])
            mix[:, j * LANES : (j + 1) * LANES] = (
                jnp.where(low, parts[0], parts[1]) + bypass * tile.astype(F32)
            )

    @pl.when(me > 0)
    def _():
        arrived(tails, tail_sem.at[1])
        pad_ref[0:8, :] = tails[...].astype(F32)[8:16]
        filtered(16)
        own_states()

    @pl.when(me != 1)
    def _():
        within()

    def relay():
        for p in range(pairs):
            state_copy(p).wait_recv()
            decay = jnp.where(low, decays[2 * p : 2 * p + 1, :], decays[2 * p + 1 : 2 * p + 2, :])
            state_out[p] = (state_in[p].astype(F32) * decay + own_state[p]).astype(BF16)
            state_copy(p).start()

    @pl.when(jnp.logical_and(me == 1, follows))
    def _():
        relay()

    @pl.when(me == 1)
    def _():
        within()

    for j in range(1, sp):

        @pl.when(me == j)
        def _(j=j):
            arrived(kvall.at[0:j], kv_sem.at[1])
            arrived(gall.at[0:j], kv_sem.at[3])

    keys = kvall[:, :, 0:kv_width].reshape(sp * rows, -1)
    values = kvall[:, :, kv_width:].reshape(sp * rows, -1)
    visible = [j * rows + col_id <= me * rows + row_id for j in range(sp)]
    for kv in range(kv_heads):
        own = lane // HEAD_DIM == kv
        summed_values = jnp.where(own, values, jnp.ones_like(values))
        scores = lax.dot_general(
            qs[kv], keys, (((1,), (1,)), ((), ())), preferred_element_type=F32
        )
        outs = []
        for i in range(repeat):
            h = kv * repeat + i
            gate_col = gate_cols[:, h : h + 1]
            tiles = [
                jnp.where(
                    visible[j],
                    scores[i * rows : (i + 1) * rows, j * rows : (j + 1) * rows]
                    + (gate_col - gall[j, h : h + 1, :]),
                    NEGATIVE,
                )
                for j in range(sp)
            ]
            top = tiles[0]
            for tile in tiles[1:]:
                top = jnp.maximum(top, tile)
            top = jnp.max(top, axis=1, keepdims=True)
            probs = jnp.concatenate([jnp.exp(tile - top).astype(BF16) for tile in tiles], axis=1)
            both = jnp.dot(probs, summed_values, preferred_element_type=F32)
            turned = pltpu.roll(both, HEAD_DIM, 1)
            outs.append(both / turned if h % 2 == kv else turned / both)
        for i in range(0, repeat, 2):
            at = slice((kv * repeat + i) * HEAD_DIM, (kv * repeat + i + 2) * HEAD_DIM)
            merged = jnp.where(low, outs[i], outs[i + 1]).astype(BF16)
            for r in range(2):
                acts_mine[r, :, at] = merged[r * half : (r + 1) * half]

    quarter = half // 2
    spans = (slice(0, quarter), slice(quarter, half))

    def spread(src, dst, send, recv, hop, q):
        return [
            remote(
                src.at[r, spans[q]],
                dst.at[2 + t, spans[q]],
                send,
                recv.at[1 + q],
                {"fs": f ^ hop, "tp": r},
            )
            for r in range(2)
        ]

    def across(src, dst, send, recv):
        return remote(src.at[1 - t], dst.at[t], send, recv.at[0], peer)

    for q in range(2):
        for copy in spread(acts_mine, acts_in, act_send, act_recv, 2, q):
            copy.start()
    across(acts_mine, acts_in, act_send, act_recv).start()

    @pl.when(jnp.logical_and(me > 1, follows))
    def _():
        relay()

    conv_read = conv[:, width + STATE :]
    squares = []
    for p in range(pairs):
        at = slice(p * LANES, (p + 1) * LANES)

        @pl.when(me == sp - 1)
        def _(p=p):
            state_copy(p).wait_recv()

        carried = jnp.dot(conv_read, state_in[p], preferred_element_type=F32)
        gate = gate_ref[0, :, at].astype(F32)
        u = (mix[:, at] + carried * expand(exp_cum, p)) * (gate * jax.nn.sigmoid(gate))
        squares.append(u * u)
        sent = (u * gain_ref[0:1, at]).astype(BF16)
        for r in range(2):
            pieces_mine[p, r] = sent[r * half : (r + 1) * half]
        for copy in spread(pieces_mine.at[p], pieces_in.at[p], piece_send.at[0], piece_recv, 1, 0):
            copy.start()
        across(pieces_mine.at[p], pieces_in.at[p], piece_send.at[0], piece_recv).start()

    total = functools.reduce(jnp.add, squares)
    coarse = total.astype(BF16)
    fine = (total - coarse.astype(F32)).astype(BF16)
    mean = (
        lax.dot_general(
            jnp.ones((8, 2 * LANES), BF16),
            jnp.concatenate([coarse, fine], axis=1),
            (((1,), (1,)), ((), ())),
            preferred_element_type=F32,
        )
        / width
    )
    scale = lax.rsqrt(mean + EPSILON)
    scales_mine[0] = scale
    scales_mine[1] = pltpu.roll(scale, half, 1)
    for r in range(2):
        remote(
            scales_mine.at[r],
            scales_in.at[2 + t],
            piece_send.at[1],
            scale_recv.at[1],
            {"fs": f ^ 1, "tp": r},
        ).start()
    across(scales_mine, scales_in, piece_send.at[1], scale_recv).start()
    for p in range(pairs):
        for copy in spread(pieces_mine.at[p], pieces_in.at[p], piece_send.at[0], piece_recv, 1, 1):
            copy.start()

    far_kv(me == 0)

    acts_in[t] = acts_mine[t]
    for p in range(pairs):
        pieces_in[p, t] = pieces_mine[p, t]
    scales_in[t] = scales_mine[t]

    def place(owner, h, values):
        at = pl.ds(pl.multiple_of(owner * cols + h * part, part), part)
        out_ref[0, :, at] = values.astype(BF16)

    def halves(weights):
        return [(weights, slice(h * part, (h + 1) * part)) for h in range(2)]

    def attended(slot, span, weights, at):
        left = jnp.concatenate([acts_in[slot + s, span] for s in range(2)], axis=1)
        right = jnp.concatenate([weights[s, :, at] for s in range(2)], axis=0)
        return jnp.dot(left, right, preferred_element_type=F32)

    def mixed(slot, span, by, weights, at):
        sums = []
        for s in range(2):
            left = jnp.concatenate([pieces_in[p, slot + s, span] for p in range(pairs)], axis=1)
            sums.append(jnp.dot(left, weights[s, :, at], preferred_element_type=F32) * by[s])
        return sums[0] + sums[1]

    whole = slice(0, half)
    arrived(wst, peer_recv.at[0])
    arrived(acts_in.at[0], act_recv.at[0])
    arrived(pieces_in.at[:, 0], piece_recv.at[0])
    arrived(scales_in.at[0], scale_recv.at[0])
    upright = scales_in[0:2].reshape(2 * 8, rows).T
    mine = [upright[0:half, 8 * s : 8 * s + 1] for s in range(2)]
    for h in range(2):
        place(
            f,
            h,
            attended(0, whole, *halves(wat)[h]) + mixed(0, whole, mine, *halves(wst)[h]),
        )

    for chunk in range(2):
        for i, ref in enumerate((wat_x, wst_y)):
            arrived(ref.at[t, chunks[chunk]], weight_recv.at[i, chunk])
            relay_copies(chunk)[i].start()
    arrived(wst, peer_recv.at[1])
    for h in range(2):
        acc[h] = attended(0, whole, *halves(wat_x)[h])
        acc[2 + h] = mixed(0, whole, mine, *halves(wst_y)[h])

    def attended_back(q):
        return remote(
            att_out.at[q], att_in.at[q], sum_send.at[0], sum_recv.at[0], {"fs": f ^ 2}
        )

    def mixed_back(q):
        return remote(
            sum_out.at[q], sum_in.at[q], sum_send.at[1], sum_recv.at[1], {"fs": f ^ 1}
        )

    def attended_step(q):
        arrived(acts_in.at[2:4, spans[q]], act_recv.at[1 + q])
        for g, (weights, at) in enumerate(halves(wat) + halves(wat_x)):
            att_out[q, g] = attended(2, spans[q], weights, at).astype(BF16)
        attended_back(q).start()

    def mixed_step(q):
        arrived(pieces_in.at[:, 2:4, spans[q]], piece_recv.at[1 + q])
        if q == 0:
            arrived(scales_in.at[2:4], scale_recv.at[1])
        upright = scales_in[2:4].reshape(2 * 8, rows).T
        by = [upright[spans[q], 8 * s : 8 * s + 1] for s in range(2)]
        for g, (weights, at) in enumerate(halves(wst) + halves(wst_y)):
            sum_out[q, g] = mixed(2, spans[q], by, weights, at).astype(BF16)
        mixed_back(q).start()

    @pl.when(me < sp - 1)
    def _():
        for q in range(2):
            mixed_step(q)
            attended_step(q)

    @pl.when(me == sp - 1)
    def _():
        for q in range(2):
            attended_step(q)
        for q in range(2):
            mixed_step(q)

    def joined(ref, g):
        return jnp.concatenate([ref[q, g] for q in range(2)], axis=0).astype(F32)

    arrived(att_in, sum_recv.at[0])
    for h in range(2):
        place(f ^ 2, h, acc[2 + h] + joined(att_in, h))
    arrived(sum_in, sum_recv.at[1])
    for h in range(2):
        place(f ^ 1, h, acc[h] + joined(sum_in, h))
        place(f ^ 3, h, joined(att_in, 2 + h) + joined(sum_in, 2 + h))

    @pl.when(follows)
    def _():
        departed(tails, tail_sem.at[0])
        departed(state_out, st_send)

    for n in range(1, sp):

        @pl.when(sp - 1 - me == n)
        def _(n=n):
            departed(kvall.at[0:n], kv_sem.at[0])
            departed(gall.at[0:n], kv_sem.at[2])

    for kind in range(3):
        departed(wst, weight_send.at[kind])
    departed(acts_in.at[0:3], act_send)
    departed(pieces_in.at[:, 0:3], piece_send.at[0])
    departed(scales_in.at[0:3], piece_send.at[1])
    departed(att_out, sum_send.at[0])
    departed(sum_out, sum_send.at[1])


def fused(sp, fs, *args):
    rows, width = args[0].shape[1:]
    heads = args[4].shape[1]
    deep, cols = args[16].shape
    half, part = rows // 2, cols // 2
    args = list(args)
    args[11] = args[11].reshape(1, -1)
    args[15] = jnp.swapaxes(args[15], 1, 2)
    far = pl.BlockSpec(memory_space=pl.ANY)
    dma = pltpu.SemaphoreType.DMA
    kv_width = args[13].shape[2]
    kv_heads = kv_width // HEAD_DIM
    pairs = heads // 2
    near = [
        (pltpu.SMEM if i in (6, 7) else pltpu.VMEM)(a.shape, a.dtype)
        for i, a in enumerate(args[:16])
        if i not in (13, 14)
    ]
    return pl.pallas_call(
        functools.partial(mixer_kernel, sp, fs),
        out_shape=pltpu.VMEM((1, half, cols * fs), BF16),
        in_specs=[far] * len(args),
        out_specs=pl.BlockSpec(memory_space=pltpu.VMEM),
        scratch_shapes=near
        + [
            dma((len(args),)),
            pltpu.SemaphoreType.REGULAR((max(sp - 2, 1),)),
            pltpu.VMEM((8 + rows, width + 2 * STATE), F32),
            pltpu.VMEM((16, width + 2 * STATE), BF16),
            pltpu.VMEM((rows, width + 2 * STATE), BF16),
            pltpu.VMEM((2, heads, rows), F32),
            pltpu.VMEM((rows, width), F32),
            pltpu.VMEM((sp, rows, 2 * kv_width), BF16),
            pltpu.VMEM((sp, heads, rows), F32),
            pltpu.VMEM((kv_heads, heads // kv_heads * rows, kv_width), BF16),
            pltpu.VMEM((pairs, STATE, LANES), F32),
            pltpu.VMEM((pairs, STATE, LANES), BF16),
            pltpu.VMEM((pairs, STATE, LANES), BF16),
            pltpu.VMEM((rows, width), F32),
            pltpu.VMEM((2, deep, cols), BF16),
            pltpu.VMEM((2, deep, cols), BF16),
            pltpu.VMEM((2, deep, cols), BF16),
            pltpu.VMEM((2, deep, cols), BF16),
            pltpu.VMEM((2, half, width), BF16),
            pltpu.VMEM((4, half, width), BF16),
            pltpu.VMEM((pairs, 2, half, LANES), BF16),
            pltpu.VMEM((pairs, 4, half, LANES), BF16),
            pltpu.VMEM((2, 8, rows), F32),
            pltpu.VMEM((4, 8, rows), F32),
            pltpu.VMEM((4, half, part), F32),
            pltpu.VMEM((2, 4, half // 2, part), BF16),
            pltpu.VMEM((2, 4, half // 2, part), BF16),
            pltpu.VMEM((2, 4, half // 2, part), BF16),
            pltpu.VMEM((2, 4, half // 2, part), BF16),
            dma((2,)),
            dma((4,)),
            dma,
            dma((pairs,)),
            dma((3,)),
            dma((2, 2)),
            dma((2,)),
            dma,
            dma((3,)),
            dma((2,)),
            dma((3,)),
            dma((2,)),
            dma((2,)),
            dma((2,)),
        ],
        compiler_params=pltpu.CompilerParams(collective_id=0, has_side_effects=True),
    )(*args)


def one_kernel(*args, sp, fs, tp):
    rows, width = args[0].shape[1:]
    heads = args[4].shape[1]
    return (
        1 < sp <= 8
        and fs == 4
        and tp == 2
        and rows == LANES
        and args[1].shape[2] == STATE == LANES
        and width == heads * HEAD_DIM
        and args[12].shape[2] == width
        and args[13].shape[2] == 2 * HEAD_DIM
        and heads % 4 == 0
        and args[16].shape == args[17].shape == (width, args[16].shape[1])
        and args[16].shape[1] % (2 * LANES) == 0
    )


def solution(mesh):
    in_specs = (
        P("fs", "sp", "tp"),
        P("fs", "sp", "tp"),
        P("fs", "sp", "tp"),
        P("fs", "sp", "tp"),
        P("fs", "tp", "sp"),
        P("fs", "tp", "sp"),
        P("tp"),
        P("tp"),
        P(None, "tp"),
        P(None, "tp"),
        P(None, "tp"),
        P("tp"),
        P("fs", "sp", "tp"),
        P("fs", "sp", "tp"),
        P("fs", "sp", "tp"),
        P("fs", "sp", "tp"),
        P("tp", "fs"),
        P("tp", "fs"),
    )
    out_specs = P("fs", ("sp", "tp"), None)
    sp, fs, tp = (mesh.shape[name] for name in ("sp", "fs", "tp"))

    def body(*args):
        if one_kernel(*args, sp=sp, fs=fs, tp=tp):
            return fused(sp, fs, *args)
        return shards(*args)

    return jax.shard_map(body, mesh=mesh, in_specs=in_specs, out_specs=out_specs, check_vma=False)
```

```python
import functools
import math

import jax
import jax.numpy as jnp
from jax import lax
from jax.experimental import pallas as pl
from jax.experimental.pallas import tpu as pltpu
from jax.sharding import PartitionSpec as P

HEAD_DIM = 64
STATE = 128


EPSILON = 1e-06
NEGATIVE = -1e30


def passed_along(shard, axis, by):
    devices = lax.axis_size(axis)
    pairs = [(i, i + by) for i in range(devices) if 0 <= i + by < devices]
    return lax.ppermute(shard, axis, pairs)


def entering(shard, axis, join, neutral):
    place = lax.axis_index(axis)
    gathered = jax.tree.map(
        lambda a, kind: lax.all_gather(a.astype(kind), axis), shard, (jnp.bfloat16, jnp.bfloat16)
    )
    state = jax.tree.map(lambda a, e: jnp.zeros_like(a) + jnp.asarray(e, a.dtype), shard, neutral)

    def one(hop, state):
        return join(
            state,
            jax.tree.map(
                lambda a, own: lax.dynamic_index_in_dim(a, hop, 0, False).astype(own.dtype),
                gathered,
                shard,
            ),
        )

    return lax.fori_loop(0, place, one, state)


def causal_filter(feeder_quantities, before, taps):
    length = feeder_quantities.shape[0]
    padded = jnp.concatenate([before, feeder_quantities], axis=0).astype(jnp.float32)
    summed = jnp.zeros(feeder_quantities.shape, jnp.float32)
    for offset in range(taps.shape[0]):
        summed = summed + taps[offset].astype(jnp.float32) * padded[offset : offset + length]
    return jax.nn.silu(summed).astype(jnp.bfloat16)


def compose(earlier, later):
    return (earlier[0] * later[0], earlier[1] * later[0][..., None, None] + later[1])


def shards(
    state_head_inputs,
    state_write_vectors,
    state_read_vectors,
    state_output_gate,
    presoftplus_steps,
    extra_decay_log,
    lane_shrinkage_powers,
    bypass_coefficient_vector,
    feeder_smoothing_stencil,
    stored_smoothing_stencil,
    lookup_smoothing_stencil,
    bundled_rescaling_vector,
    queries,
    attention_keys,
    attention_values,
    forget_gate_cumsum,
    state_out_weight,
    attention_out_weight,
):
    shard_rows = state_head_inputs.shape[1]
    input_rows = state_head_inputs[0]
    write_rows = state_write_vectors[0]
    read_rows = state_read_vectors[0]
    tap_rows = feeder_smoothing_stencil.shape[0] - 1
    value_width = input_rows.shape[1]
    vector_width = write_rows.shape[1]
    tail_rows = jnp.concatenate(
        [input_rows[-tap_rows:], write_rows[-tap_rows:], read_rows[-tap_rows:]], axis=1
    )
    before = passed_along(tail_rows, "sp", 1)
    conv_values = causal_filter(input_rows, before[:, :value_width], feeder_smoothing_stencil)
    conv_write = causal_filter(
        write_rows, before[:, value_width : value_width + vector_width], stored_smoothing_stencil
    )
    conv_read = causal_filter(
        read_rows, before[:, value_width + vector_width :], lookup_smoothing_stencil
    )
    stride_duration = jax.nn.softplus(presoftplus_steps[0])
    shrinkage_natural_power = (
        stride_duration * (-jnp.exp(lane_shrinkage_powers))[:, None] + extra_decay_log[0]
    )
    lane_tally = stride_duration.shape[0]
    groups = vector_width // STATE
    per_group = lane_tally // groups
    cumulative = jnp.cumsum(shrinkage_natural_power, axis=1)
    input_heads = conv_values.reshape(shard_rows, groups, per_group, HEAD_DIM)
    write_groups = conv_write.reshape(shard_rows, groups, STATE)
    read_groups = conv_read.reshape(shard_rows, groups, STATE)
    inner_products = jnp.einsum(
        "tgn,sgn->gts", read_groups, write_groups, preferred_element_type=jnp.float32
    )
    positions = jnp.arange(shard_rows)
    causal = positions[:, None] >= positions[None, :]
    log_gap = jnp.where(causal[None], cumulative[:, :, None] - cumulative[:, None, :], -jnp.inf)
    weights = jnp.exp(log_gap) * stride_duration[:, None, :]
    mix_weights = (
        inner_products[:, None] * weights.reshape(groups, per_group, shard_rows, shard_rows)
    ).astype(jnp.bfloat16)
    local_part = jnp.einsum(
        "ghts,sghp->tghp", mix_weights, input_heads, preferred_element_type=jnp.float32
    )
    end_scale = (jnp.exp(cumulative[:, -1:] - cumulative) * stride_duration).T.reshape(
        shard_rows, groups, per_group
    )
    weighted = (input_heads.astype(jnp.float32) * end_scale[..., None]).astype(jnp.bfloat16)
    block_state = jnp.einsum(
        "sghp,sgn->ghpn", weighted, write_groups, preferred_element_type=jnp.float32
    )
    total_decay = jnp.exp(cumulative[:, -1]).reshape(groups, per_group)
    identity = (jnp.ones_like(total_decay), jnp.zeros_like(block_state))
    carried = entering((total_decay, block_state), "sp", compose, identity)[1]
    carried_part = jnp.einsum(
        "tgn,ghpn->tghp",
        read_groups,
        carried.astype(jnp.bfloat16),
        preferred_element_type=jnp.float32,
    )
    carried_part = (
        carried_part * jnp.exp(cumulative).T.reshape(shard_rows, groups, per_group)[..., None]
    )
    mixer_sum = (
        local_part
        + carried_part
        + bypass_coefficient_vector.reshape(groups, per_group)[None, :, :, None]
        * input_heads.astype(jnp.float32)
    )
    gated_rows = mixer_sum.reshape(shard_rows, groups, per_group * HEAD_DIM) * jax.nn.silu(
        state_output_gate[0].astype(jnp.float32)
    ).reshape(shard_rows, groups, -1)
    stretch_coefficient = lax.rsqrt(
        jnp.mean(gated_rows * gated_rows, axis=-1, keepdims=True) + EPSILON
    )
    state_result = (
        (gated_rows * stretch_coefficient * bundled_rescaling_vector.reshape(groups, -1))
        .reshape(shard_rows, -1)
        .astype(jnp.bfloat16)
    )
    attend_heads = forget_gate_cumsum.shape[2]
    key_group_count = attention_keys.shape[2] // HEAD_DIM
    repeat_factor = attend_heads // key_group_count
    query_head_count = queries[0].reshape(shard_rows, key_group_count, repeat_factor, HEAD_DIM)
    first_query = lax.axis_index("sp") * shard_rows
    query_index = first_query + jnp.arange(shard_rows)
    last_query = first_query + shard_rows - 1
    query_gates = forget_gate_cumsum[0].T
    all_gates = lax.all_gather(forget_gate_cumsum[0], "sp", axis=0, tiled=True)
    attention_score_scale = HEAD_DIM ** (-0.5)
    starting = (
        jnp.full((attend_heads, shard_rows), NEGATIVE, jnp.float32),
        jnp.zeros((attend_heads, shard_rows), jnp.float32),
        jnp.zeros((attend_heads, shard_rows, HEAD_DIM), jnp.float32),
    )
    key_rows = lax.all_gather(attention_keys[0], "sp", axis=0, tiled=True)
    value_rows = lax.all_gather(attention_values[0], "sp", axis=0, tiled=True)
    span = key_rows.shape[0]
    sub_block = math.gcd(span, 512)

    def advance(sub_index, running):
        first_key = sub_index * sub_block

        def attend(running):
            running_max, running_sum, weighted_sum = running
            key_tile = lax.dynamic_slice_in_dim(
                key_rows, sub_index * sub_block, sub_block, 0
            ).reshape(sub_block, key_group_count, HEAD_DIM)
            value_tile = lax.dynamic_slice_in_dim(
                value_rows, sub_index * sub_block, sub_block, 0
            ).reshape(sub_block, key_group_count, HEAD_DIM)
            key_gates = lax.dynamic_slice_in_dim(all_gates, first_key, sub_block, 0)
            attention_scores = jnp.einsum(
                "ezxp,czp->zxec", query_head_count, key_tile, preferred_element_type=jnp.float32
            )
            attention_scores = (
                attention_scores.reshape(attend_heads, shard_rows, sub_block)
                * attention_score_scale
            )
            attention_scores = attention_scores + query_gates[:, :, None] - key_gates.T[:, None, :]
            visible = (first_key + jnp.arange(sub_block))[None, :] <= query_index[:, None]
            attention_scores = jnp.where(visible[None], attention_scores, NEGATIVE)
            new_max = jnp.maximum(running_max, jnp.max(attention_scores, axis=-1))
            shrink = jnp.exp(running_max - new_max)
            attention_probs = jnp.where(
                visible[None], jnp.exp(attention_scores - new_max[..., None]), 0.0
            )
            running_sum = running_sum * shrink + jnp.sum(attention_probs, axis=-1)
            weighted_value_sum = jnp.einsum(
                "fljx,xfc->fljc",
                attention_probs.astype(jnp.bfloat16).reshape(
                    key_group_count, repeat_factor, shard_rows, sub_block
                ),
                value_tile,
                preferred_element_type=jnp.float32,
            )
            weighted_sum = weighted_sum * shrink[..., None] + weighted_value_sum.reshape(
                attend_heads, shard_rows, HEAD_DIM
            )
            return (new_max, running_sum, weighted_sum)

        return lax.cond(first_key <= last_query, attend, lambda kept: kept, running)

    _, running_sum, weighted_sum = lax.fori_loop(0, span // sub_block, advance, starting)
    attend_out = (
        (weighted_sum / running_sum[..., None])
        .transpose(1, 0, 2)
        .reshape(shard_rows, -1)
        .astype(jnp.bfloat16)
    )
    state_columns, attend_columns = (
        lax.all_gather(state_out_weight, "fs", axis=1, tiled=True),
        lax.all_gather(attention_out_weight, "fs", axis=1, tiled=True),
    )
    summed = lax.psum_scatter(
        (
            jnp.dot(state_result, state_columns, preferred_element_type=jnp.float32)
            + jnp.dot(attend_out, attend_columns, preferred_element_type=jnp.float32)
        ).astype(jnp.bfloat16),
        "tp",
        scatter_dimension=0,
        tiled=True,
    )
    return summed[None]


MESH = pl.DeviceIdType.MESH
LANES = 128
BF16, F32 = jnp.bfloat16, jnp.float32


def mixer_kernel(
    sp,
    fs,
    x_far,
    w_far,
    r_far,
    gate_far,
    step_far,
    extra_far,
    shrink_far,
    bypass_far,
    tapx_far,
    tapw_far,
    tapr_far,
    gain_far,
    q_far,
    k_far,
    v_far,
    forget_far,
    wst_far,
    wat_far,
    out_ref,
    x_ref,
    w_ref,
    r_ref,
    gate_ref,
    step_ref,
    extra_ref,
    shrink_ref,
    bypass_ref,
    tapx_ref,
    tapw_ref,
    tapr_ref,
    gain_ref,
    q_ref,
    forget_ref,
    load_sem,
    ready,
    pad_ref,
    tails,
    conv,
    soft_cum,
    end_wide,
    kvall,
    gall,
    qs,
    own_state,
    state_in,
    state_out,
    mix,
    wst,
    wat,
    wst_y,
    wat_x,
    acts_mine,
    acts_in,
    pieces_mine,
    pieces_in,
    scales_mine,
    scales_in,
    acc,
    att_out,
    att_in,
    sum_out,
    sum_in,
    tail_sem,
    kv_send,
    kv_recv,
    st_send,
    st_recv,
    weight_send,
    weight_recv,
    peer_recv,
    act_send,
    act_recv,
    piece_send,
    piece_recv,
    scale_recv,
    sum_send,
    sum_recv,
):
    me = lax.axis_index("sp")
    f = lax.axis_index("fs")
    t = lax.axis_index("tp")
    rows, width = x_ref.shape[1], x_ref.shape[2]
    heads = step_ref.shape[1]
    kv_width = k_far.shape[2]
    kv_heads = kv_width // HEAD_DIM
    repeat = heads // kv_heads
    pairs = heads // 2
    taps = tapx_ref.shape[0]
    cols = wst_far.shape[1]
    part = cols // 2
    half = rows // 2
    peer = {"tp": 1 - t}

    barrier = pltpu.get_barrier_semaphore()
    for d in (1, 2):
        for r in range(2):
            pl.semaphore_signal(
                barrier, inc=1, device_id={"fs": f ^ d, "tp": r}, device_id_type=MESH
            )
    pl.semaphore_signal(barrier, inc=1, device_id=peer, device_id_type=MESH)
    for d in range(1, sp):

        @pl.when(me + d < sp)
        def _(d=d):
            pl.semaphore_signal(barrier, inc=1, device_id={"sp": me + d}, device_id_type=MESH)

    @pl.when(me > 0)
    def _():
        pl.semaphore_signal(barrier, inc=1, device_id={"sp": me - 1}, device_id_type=MESH)

    near = {
        "x": (x_far, x_ref),
        "w": (w_far, w_ref),
        "r": (r_far, r_ref),
        "tapx": (tapx_far, tapx_ref),
        "tapw": (tapw_far, tapw_ref),
        "tapr": (tapr_far, tapr_ref),
        "k": (k_far.at[0], kvall.at[me, :, 0:kv_width]),
        "v": (v_far.at[0], kvall.at[me, :, kv_width:]),
        "wat": (wat_far, wat.at[t]),
        "wst": (wst_far, wst.at[t]),
        "step": (step_far, step_ref),
        "extra": (extra_far, extra_ref),
        "shrink": (shrink_far, shrink_ref),
        "forget": (forget_far, forget_ref),
        "q": (q_far, q_ref),
        "gate": (gate_far, gate_ref),
        "gain": (gain_far, gain_ref),
        "bypass": (bypass_far, bypass_ref),
    }
    shared = {"v": "k", "wst": "wat"}
    places = [name for name in near if name not in shared]
    loads = {
        name: pltpu.make_async_copy(
            far, here, load_sem.at[places.index(shared.get(name, name))]
        )
        for name, (far, here) in near.items()
    }
    for load in loads.values():
        load.start()

    def loaded(*names):
        for name in names:
            loads[name].wait()

    def remote(src, dst, send, recv, where):
        return pltpu.make_async_remote_copy(
            src_ref=src,
            dst_ref=dst,
            send_sem=send,
            recv_sem=recv,
            device_id=where,
            device_id_type=MESH,
        )

    def arrived(ref, sem):
        remote(ref, ref, sem, sem, peer).wait_recv()

    def departed(ref, sem):
        remote(ref, ref, sem, sem, peer).wait_send()

    lane = lax.broadcasted_iota(jnp.int32, (1, LANES), 1)
    low = lane < HEAD_DIM
    row_id = lax.broadcasted_iota(jnp.int32, (rows, rows), 0)
    col_id = lax.broadcasted_iota(jnp.int32, (rows, rows), 1)

    def expand(columns, j):
        return jnp.where(low, columns[:, 2 * j : 2 * j + 1], columns[:, 2 * j + 1 : 2 * j + 2])

    inputs = (
        (x_ref, tapx_ref, slice(0, width)),
        (w_ref, tapw_ref, slice(width, width + STATE)),
        (r_ref, tapr_ref, slice(width + STATE, width + 2 * STATE)),
    )

    def filtered(count):
        for _, tap_ref, at in inputs:
            total = jnp.zeros((count, at.stop - at.start), F32)
            for i in range(taps):
                first = 8 - (taps - 1) + i
                total = total + tap_ref[i : i + 1, :].astype(F32) * pad_ref[first : first + count, at]
            conv[0:count, at] = (total * jax.nn.sigmoid(total)).astype(BF16)

    pad_ref[0:8, :] = jnp.zeros((8, pad_ref.shape[1]), F32)
    loaded("x", "w", "r", "tapx", "tapw", "tapr")
    for ref, _, at in inputs:
        pad_ref[8 : 8 + rows, at] = ref[0].astype(F32)
    filtered(rows)

    def decay():
        loaded("step", "extra", "shrink")
        head_row = lax.broadcasted_iota(jnp.int32, (heads, rows), 0)
        power = jnp.zeros((heads, rows), F32)
        for h in range(heads):
            power = jnp.where(head_row == h, shrink_ref[h], power)
        presoft = step_ref[0]
        step = jnp.maximum(presoft, 0.0) + jnp.log1p(jnp.exp(-jnp.abs(presoft)))
        log_decay = extra_ref[0] - jnp.exp(power) * step
        upper = (row_id <= col_id).astype(F32)
        cum = jnp.dot(log_decay, upper, precision=lax.Precision.HIGHEST, preferred_element_type=F32)
        soft_cum[0] = step
        soft_cum[1] = cum
        end_scale = (jnp.exp(cum[:, rows - 1 : rows] - cum) * step).T
        for j in range(pairs):
            end_wide[:, j * LANES : (j + 1) * LANES] = expand(end_scale, j)

    def own_states():
        turned_write = conv[:, width : width + STATE].astype(F32).T.astype(BF16)
        for p in range(pairs):
            at = slice(p * LANES, (p + 1) * LANES)
            weighted = (conv[:, at].astype(F32) * end_wide[:, at]).astype(BF16)
            own_state[p] = jnp.dot(turned_write, weighted, preferred_element_type=F32)

    @pl.when(me == 0)
    def _():
        state_in[...] = jnp.zeros(state_in.shape, BF16)
        decay()
        own_states()
        for p in range(pairs):
            state_out[p] = own_state[p].astype(BF16)

    follows = me + 1 < sp
    pl.semaphore_wait(barrier, 5 + me + jnp.where(follows, 1, 0))

    for d in range(2, sp):

        @pl.when(me - d >= 0)
        def _(d=d):
            pl.semaphore_signal(
                ready.at[d - 2], inc=1, device_id={"sp": me - d}, device_id_type=MESH
            )

    deep = wst_far.shape[0]
    lent = deep * 3 // 16 // 16 * 16
    ends = (0, lent, 2 * lent, deep * 7 // 8, deep)
    chunks = [slice(ends[c], ends[c + 1]) for c in range(4)]
    odd = lax.rem(me, 2) == 1
    even = jnp.logical_not(odd)
    top = me == sp - 1

    def weight_copies(chunk):
        at = (t, chunks[chunk])
        return [
            remote(
                src.at[at],
                dst.at[at],
                weight_send.at[0],
                weight_recv.at[chunk],
                {"fs": f ^ hop},
            )
            for src, dst, hop in ((wat, wat_x, 1), (wst, wst_y, 2))
        ]

    def own_copies():
        return [
            remote(w.at[t], w.at[t], weight_send.at[1], peer_recv.at[0], peer) for w in (wat, wst)
        ]

    def landed(chunk):
        arrived(wat_x.at[:, chunks[chunk]], weight_recv.at[chunk])

    def relay(chunk):
        for w in (wat_x, wst_y):
            at = (t, chunks[chunk])
            remote(w.at[at], w.at[at], weight_send.at[2], peer_recv.at[1], peer).start()

    def lend(chunk):
        at = (t, chunks[chunk])
        return [
            remote(
                w.at[at],
                w.at[at],
                weight_send.at[3],
                weight_recv.at[chunk],
                {"sp": lax.rem(me + sp - 1, sp)},
            )
            for w in (wat_x, wst_y)
        ]

    pltpu.make_async_copy(wst, wst, load_sem.at[places.index("wat")]).wait()
    for chunk, fits in (
        (0, odd),
        (1, even),
        (0, jnp.logical_and(even, top)),
        (1, jnp.logical_and(odd, top)),
        (2, me >= 0),
        (3, me >= 0),
    ):

        @pl.when(fits)
        def _(chunk=chunk):
            for copy in weight_copies(chunk):
                copy.start()

    for copy in own_copies():
        copy.start()

    @pl.when(me > 0)
    def _():
        decay()

    step, cum = soft_cum[0], soft_cum[1]
    decays = jnp.broadcast_to(jnp.exp(cum[:, rows - 1 : rows]), (heads, LANES))

    def state_copy(p):
        there = {"sp": lax.rem(me + 1, sp)}
        return remote(state_out.at[p], state_in.at[p], st_send, st_recv.at[p], there)

    pltpu.make_async_copy(kvall.at[me], kvall.at[me], load_sem.at[places.index("k")]).wait()
    loaded("forget")
    gall[me] = forget_ref[0]
    gate_cols = forget_ref[0].T

    tail = [
        remote(
            ref.at[0, rows - 8 : rows, :],
            tails.at[:, at],
            tail_sem.at[0],
            tail_sem.at[1],
            {"sp": lax.rem(me + 1, sp)},
        )
        for ref, _, at in inputs
    ]

    def kv_copies(d, source, kind):
        there = {"sp": lax.rem(me + d, sp)}
        return [
            remote(kvall.at[source], kvall.at[source], kv_send.at[0], kv_recv.at[kind, 0], there),
            remote(gall.at[source], gall.at[source], kv_send.at[1], kv_recv.at[kind, 1], there),
        ]

    @pl.when(follows)
    def _():
        for copy in tail:
            copy.start()

    @pl.when(me == 0)
    def _():
        for p in range(pairs):
            state_copy(p).start()

    @pl.when(follows)
    def _():
        for copy in kv_copies(1, me, 0):
            copy.start()

    def far_kv(fits):
        for d in range(2, sp):

            @pl.when(jnp.logical_and(fits, me + d < sp))
            def _(d=d):
                pl.semaphore_wait(ready.at[d - 2], 1)

                @pl.when(jnp.logical_or(me == 0, d > 2))
                def _():
                    for copy in kv_copies(d, me, 1):
                        copy.start()

    far_kv(me > 0)

    for j in range(1, sp):

        @pl.when(j > me)
        def _(j=j):
            kvall[j] = jnp.zeros(kvall.shape[1:], BF16)
            gall[j] = jnp.zeros(gall.shape[1:], F32)

    loaded("q")
    for h in range(heads):
        kv = h // repeat
        piece = (q_ref[0, :, h * HEAD_DIM : (h + 1) * HEAD_DIM].astype(F32) * HEAD_DIM**-0.5).astype(
            BF16
        )
        zero = jnp.zeros((rows, HEAD_DIM), BF16)
        parts = [piece if i == kv else zero for i in range(kv_heads)]
        qs[kv, (h % repeat) * rows : (h % repeat + 1) * rows, :] = jnp.concatenate(parts, axis=1)

    loaded("gate", "gain", "bypass")
    exp_cum = jnp.exp(cum).T
    cum_col = cum.T

    def within():
        conv_write = conv[:, width : width + STATE]
        conv_read = conv[:, width + STATE :]
        inner = lax.dot_general(
            conv_read, conv_write, (((1,), (1,)), ((), ())), preferred_element_type=F32
        )
        causal = row_id >= col_id
        for j in range(pairs):
            tile = conv[:, j * LANES : (j + 1) * LANES]
            parts = []
            for h in (2 * j, 2 * j + 1):
                gap = jnp.where(causal, cum_col[:, h : h + 1] - cum[h : h + 1, :], NEGATIVE)
                weights = (inner * (jnp.exp(gap) * step[h : h + 1, :])).astype(BF16)
                parts.append(jnp.dot(weights, tile, preferred_element_type=F32))
            bypass = jnp.where(low, bypass_ref[2 * j], bypass_ref[2 * j + 1])
            mix[:, j * LANES : (j + 1) * LANES] = (
                jnp.where(low, parts[0], parts[1]) + bypass * tile.astype(F32)
            )

    @pl.when(me > 0)
    def _():
        arrived(tails, tail_sem.at[1])
        pad_ref[0:8, :] = tails[...].astype(F32)
        filtered(16)
        own_states()

    @pl.when(me != 1)
    def _():
        within()

    def pass_state(which):
        for p in which:
            state_copy(p).wait_recv()
            decay = jnp.where(low, decays[2 * p : 2 * p + 1, :], decays[2 * p + 1 : 2 * p + 2, :])
            state_out[p] = (state_in[p].astype(F32) * decay + own_state[p]).astype(BF16)
            state_copy(p).start()

    @pl.when(jnp.logical_and(me == 1, follows))
    def _():
        pass_state(range(pairs))

    @pl.when(me == 1)
    def _():
        within()

    for chunk, parity in ((0, odd), (1, even)):

        @pl.when(jnp.logical_and(parity, me > 0))
        def _(chunk=chunk):
            landed(chunk)
            for copy in lend(chunk):
                copy.start()
            relay(chunk)

    @pl.when(me > 0)
    def _():
        arrived(kvall.at[0], kv_recv.at[0, 0])
        arrived(gall.at[0], kv_recv.at[0, 1])

    @pl.when(jnp.logical_and(me > 1, follows))
    def _():
        for copy in kv_copies(1, me - 1, 1):
            copy.start()

    quarter = half // 2
    spans = (slice(0, quarter), slice(quarter, half))

    def spread(src, dst, send, recv, hop, q):
        return [
            remote(
                src.at[r, spans[q]],
                dst.at[2 + t, spans[q]],
                send,
                recv.at[1 + q],
                {"fs": f ^ hop, "tp": r},
            )
            for r in range(2)
        ]

    def across(src, dst, send, recv):
        return remote(src.at[1 - t], dst.at[t], send, recv.at[0], peer)

    def second_quarter(p):
        for copy in spread(pieces_mine.at[p], pieces_in.at[p], piece_send.at[0], piece_recv, 1, 1):
            copy.start()

    def state_part():
        conv_read = conv[:, width + STATE :]
        squares = []
        for p in range(pairs):
            at = slice(p * LANES, (p + 1) * LANES)

            @pl.when(me == sp - 1)
            def _(p=p):
                state_copy(p).wait_recv()

            carried = jnp.dot(conv_read, state_in[p], preferred_element_type=F32)
            gate = gate_ref[0, :, at].astype(F32)
            u = (mix[:, at] + carried * expand(exp_cum, p)) * (gate * jax.nn.sigmoid(gate))
            squares.append(u * u)
            sent = (u * gain_ref[0:1, at]).astype(BF16)
            for r in range(2):
                pieces_mine[p, r] = sent[r * half : (r + 1) * half]
            for copy in spread(pieces_mine.at[p], pieces_in.at[p], piece_send.at[0], piece_recv, 1, 0):
                copy.start()
            across(pieces_mine.at[p], pieces_in.at[p], piece_send.at[0], piece_recv).start()

            @pl.when(top)
            def _(p=p):
                second_quarter(p)

        total = functools.reduce(jnp.add, squares)
        coarse = total.astype(BF16)
        fine = (total - coarse.astype(F32)).astype(BF16)
        mean = (
            lax.dot_general(
                jnp.ones((8, 2 * LANES), BF16),
                jnp.concatenate([coarse, fine], axis=1),
                (((1,), (1,)), ((), ())),
                preferred_element_type=F32,
            )
            / width
        )
        scale = lax.rsqrt(mean + EPSILON)
        scales_mine[0] = scale
        scales_mine[1] = pltpu.roll(scale, half, 1)
        for r in range(2):
            remote(
                scales_mine.at[r],
                scales_in.at[2 + t],
                piece_send.at[1],
                scale_recv.at[1],
                {"fs": f ^ 1, "tp": r},
            ).start()
        across(scales_mine, scales_in, piece_send.at[1], scale_recv).start()

        @pl.when(jnp.logical_not(top))
        def _():
            for p in range(pairs):
                second_quarter(p)

    middle = jnp.logical_and(me > 1, follows)
    ahead = jnp.logical_and(middle, t == 1)
    amid = jnp.logical_and(middle, t == 0)

    @pl.when(ahead)
    def _():
        pass_state(range(pairs))
        state_part()

    for j in range(2, sp):

        @pl.when(me == j)
        def _(j=j):
            arrived(kvall.at[0 : j - 1], kv_recv.at[1, 0])
            arrived(gall.at[0 : j - 1], kv_recv.at[1, 1])

    keys = kvall[:, :, 0:kv_width].reshape(sp * rows, -1)
    values = kvall[:, :, kv_width:].reshape(sp * rows, -1)
    visible = [j * rows + col_id <= me * rows + row_id for j in range(sp)]
    for kv in range(kv_heads):
        if kv == 1:

            @pl.when(amid)
            def _():
                pass_state(range(pairs // 2))

        own = lane // HEAD_DIM == kv
        summed_values = jnp.where(own, values, jnp.ones_like(values))
        scores = lax.dot_general(
            qs[kv], keys, (((1,), (1,)), ((), ())), preferred_element_type=F32
        )
        outs = []
        for i in range(repeat):
            h = kv * repeat + i
            gate_col = gate_cols[:, h : h + 1]
            tiles = [
                jnp.where(
                    visible[j],
                    scores[i * rows : (i + 1) * rows, j * rows : (j + 1) * rows]
                    + (gate_col - gall[j, h : h + 1, :]),
                    NEGATIVE,
                )
                for j in range(sp)
            ]
            peak = tiles[0]
            for tile in tiles[1:]:
                peak = jnp.maximum(peak, tile)
            peak = jnp.max(peak, axis=1, keepdims=True)
            probs = jnp.concatenate([jnp.exp(tile - peak).astype(BF16) for tile in tiles], axis=1)
            both = jnp.dot(probs, summed_values, preferred_element_type=F32)
            turned = pltpu.roll(both, HEAD_DIM, 1)
            outs.append(both / turned if h % 2 == kv else turned / both)
        for i in range(0, repeat, 2):
            at = slice((kv * repeat + i) * HEAD_DIM, (kv * repeat + i + 2) * HEAD_DIM)
            merged = jnp.where(low, outs[i], outs[i + 1]).astype(BF16)
            for r in range(2):
                acts_mine[r, :, at] = merged[r * half : (r + 1) * half]

    @pl.when(amid)
    def _():
        pass_state(range(pairs // 2, pairs))

    for q in range(2):
        for copy in spread(acts_mine, acts_in, act_send, act_recv, 2, q):
            copy.start()
    across(acts_mine, acts_in, act_send, act_recv).start()

    def relay_middle():
        for chunk, parity in ((1, odd), (0, even)):

            @pl.when(jnp.logical_and(parity, top))
            def _(chunk=chunk):
                landed(chunk)
                relay(chunk)

        @pl.when(me == 0)
        def _():
            landed(1)
            relay(1)

        landed(2)
        relay(2)

    @pl.when(jnp.logical_not(ahead))
    def _():
        state_part()

    acts_in[t] = acts_mine[t]
    for p in range(pairs):
        pieces_in[p, t] = pieces_mine[p, t]
    scales_in[t] = scales_mine[t]

    def place(owner, h, values):
        at = pl.ds(pl.multiple_of(owner * cols + h * part, part), part)
        out_ref[0, :, at] = values.astype(BF16)

    def halves(weights):
        return [(weights, slice(h * part, (h + 1) * part)) for h in range(2)]

    def attended(blocks, weights, at):
        left = jnp.concatenate(
            [
                jnp.concatenate([acts_in[slot + s, span] for slot, span in blocks], axis=0)
                for s in range(2)
            ],
            axis=1,
        )
        right = jnp.concatenate([weights[s, :, at] for s in range(2)], axis=0)
        return jnp.dot(left, right, preferred_element_type=F32)

    def mixed(blocks, by, weights, at):
        sums = []
        for s in range(2):
            left = jnp.concatenate(
                [
                    jnp.concatenate([pieces_in[p, slot + s, span] for slot, span in blocks], axis=0)
                    for p in range(pairs)
                ],
                axis=1,
            )
            scale = jnp.concatenate([b[s] for b in by], axis=0)
            sums.append(jnp.dot(left, weights[s, :, at], preferred_element_type=F32) * scale)
        return sums[0] + sums[1]

    whole = slice(0, half)

    def own_product():
        by = columns_of(0)
        for h in range(2):
            attention = attended(((0, whole),), *halves(wat)[h])
            place(f, h, attention + mixed(((0, whole),), (by,), *halves(wst)[h]))

    def columns_of(slot):
        upright = scales_in[slot : slot + 2].reshape(2 * 8, rows).T
        return [upright[0:half, 8 * s : 8 * s + 1] for s in range(2)]

    arrived(wst, peer_recv.at[0])

    @pl.when(jnp.logical_not(top))
    def _():
        arrived(acts_in.at[0], act_recv.at[0])
        arrived(pieces_in.at[:, 0], piece_recv.at[0])
        arrived(scales_in.at[0], scale_recv.at[0])
        own_product()

    far_kv(me == 0)
    relay_middle()

    landed(3)
    relay(3)

    for chunk, parity in ((0, even), (1, odd)):

        @pl.when(jnp.logical_and(parity, jnp.logical_not(top)))
        def _(chunk=chunk):
            landed(chunk)
            relay(chunk)

    def back(out, landing, qs, picked, i, hop):
        at = (slice(qs[0], qs[-1] + 1), slice(picked[0], picked[-1] + 1))
        return remote(out.at[at], landing.at[at], sum_send.at[i], sum_recv.at[i], {"fs": f ^ hop})

    def span_of(qs):
        return slice(spans[qs[0]].start, spans[qs[-1]].stop)

    def put(out, qs, g, product):
        for q in qs:
            start = (q - qs[0]) * quarter
            out[q, g] = product[start : start + quarter].astype(BF16)

    def attended_step(qs, picked):
        if 0 in picked:
            for q in qs:
                arrived(acts_in.at[2:4, spans[q]], act_recv.at[1 + q])
        there = (2, span_of(qs))
        pairings = halves(wat) + halves(wat_x)
        for g in picked:
            if 0 in qs and g >= 2:
                product = attended(((0, whole), there), *pairings[g])
                acc[g - 2] = product[0:half]
                product = product[half:]
            else:
                product = attended((there,), *pairings[g])
            put(att_out, qs, g, product)
        back(att_out, att_in, qs, picked, 0, 2).start()

    def mixed_step(qs, picked):
        if 0 in picked:
            for q in qs:
                arrived(pieces_in.at[:, 2:4, spans[q]], piece_recv.at[1 + q])
            if 0 in qs:
                arrived(scales_in.at[2:4], scale_recv.at[1])
        there = (2, span_of(qs))
        by = [column[span_of(qs)] for column in columns_of(2)]
        pairings = halves(wst) + halves(wst_y)
        for g in picked:
            if 0 in qs and g >= 2:
                product = mixed(((0, whole), there), (columns_of(0), by), *pairings[g])
                acc[g] = product[0:half]
                product = product[half:]
            else:
                product = mixed((there,), (by,), *pairings[g])
            put(sum_out, qs, g, product)
        back(sum_out, sum_in, qs, picked, 1, 1).start()

    low_groups, high_groups = (0, 1), (2, 3)

    @pl.when(jnp.logical_not(top))
    def _():
        mixed_step((0,), low_groups)
        attended_step((0,), low_groups)
        arrived(wat, peer_recv.at[1])
        mixed_step((0,), high_groups)
        attended_step((0,), high_groups)
        mixed_step((1,), low_groups)
        mixed_step((1,), high_groups)
        attended_step((1,), low_groups)
        attended_step((1,), high_groups)

    @pl.when(top)
    def _():
        attended_step((0, 1), low_groups)
        arrived(wat, peer_recv.at[1])
        arrived(acts_in.at[0], act_recv.at[0])
        attended_step((0, 1), high_groups)
        mixed_step((0, 1), low_groups)
        arrived(pieces_in.at[:, 0], piece_recv.at[0])
        arrived(scales_in.at[0], scale_recv.at[0])
        mixed_step((0, 1), high_groups)
        own_product()

    def joined(ref, g):
        return jnp.concatenate([ref[q, g] for q in range(2)], axis=0).astype(F32)

    arrived(att_in, sum_recv.at[0])
    for h in range(2):
        place(f ^ 2, h, acc[2 + h] + joined(att_in, h))
    arrived(sum_in, sum_recv.at[1])
    for h in range(2):
        place(f ^ 1, h, acc[h] + joined(sum_in, h))
        place(f ^ 3, h, joined(att_in, 2 + h) + joined(sum_in, 2 + h))

    @pl.when(follows)
    def _():
        departed(tails, tail_sem.at[0])
        departed(state_out, st_send)

    for j in range(sp - 1):
        n = sum(1 for d in range(1, sp - j) if d != 2 or j == 0) + (j > 1)

        @pl.when(me == j)
        def _(n=n):
            departed(kvall.at[0:n], kv_send.at[0])
            departed(gall.at[0:n], kv_send.at[1])

    @pl.when(top)
    def _():
        departed(wat, weight_send.at[0])

    @pl.when(jnp.logical_not(top))
    def _():
        departed(wat.at[:, lent:], weight_send.at[0])

    departed(wst, weight_send.at[1])
    departed(wst, weight_send.at[2])

    @pl.when(me > 0)
    def _():
        departed(wat.at[:, chunks[0]], weight_send.at[3])

    departed(acts_in.at[0:3], act_send)
    departed(pieces_in.at[:, 0:3], piece_send.at[0])
    departed(scales_in.at[0:3], piece_send.at[1])
    departed(att_out, sum_send.at[0])
    departed(sum_out, sum_send.at[1])


def fused(sp, fs, *args):
    rows, width = args[0].shape[1:]
    heads = args[4].shape[1]
    deep, cols = args[16].shape
    half, part = rows // 2, cols // 2
    args = list(args)
    args[11] = args[11].reshape(1, -1)
    args[15] = jnp.swapaxes(args[15], 1, 2)
    far = pl.BlockSpec(memory_space=pl.ANY)
    dma = pltpu.SemaphoreType.DMA
    kv_width = args[13].shape[2]
    kv_heads = kv_width // HEAD_DIM
    pairs = heads // 2
    near = [
        (pltpu.SMEM if i in (6, 7) else pltpu.VMEM)(a.shape, a.dtype)
        for i, a in enumerate(args[:16])
        if i not in (13, 14)
    ]
    return pl.pallas_call(
        functools.partial(mixer_kernel, sp, fs),
        out_shape=pltpu.VMEM((1, half, cols * fs), BF16),
        in_specs=[far] * len(args),
        out_specs=pl.BlockSpec(memory_space=pltpu.VMEM),
        scratch_shapes=near
        + [
            dma((len(args) - 2,)),
            pltpu.SemaphoreType.REGULAR((max(sp - 2, 1),)),
            pltpu.VMEM((8 + rows, width + 2 * STATE), F32),
            pltpu.VMEM((8, width + 2 * STATE), BF16),
            pltpu.VMEM((rows, width + 2 * STATE), BF16),
            pltpu.VMEM((2, heads, rows), F32),
            pltpu.VMEM((rows, width), F32),
            pltpu.VMEM((sp, rows, 2 * kv_width), BF16),
            pltpu.VMEM((sp, heads, rows), F32),
            pltpu.VMEM((kv_heads, heads // kv_heads * rows, kv_width), BF16),
            pltpu.VMEM((pairs, STATE, LANES), F32),
            pltpu.VMEM((pairs, STATE, LANES), BF16),
            pltpu.VMEM((pairs, STATE, LANES), BF16),
            pltpu.VMEM((rows, width), F32),
            pltpu.VMEM((2, deep, cols), BF16),
            pltpu.VMEM((2, deep, cols), BF16),
            pltpu.VMEM((2, deep, cols), BF16),
            pltpu.VMEM((2, deep, cols), BF16),
            pltpu.VMEM((2, half, width), BF16),
            pltpu.VMEM((4, half, width), BF16),
            pltpu.VMEM((pairs, 2, half, LANES), BF16),
            pltpu.VMEM((pairs, 4, half, LANES), BF16),
            pltpu.VMEM((2, 8, rows), F32),
            pltpu.VMEM((4, 8, rows), F32),
            pltpu.VMEM((4, half, part), F32),
            pltpu.VMEM((2, 4, half // 2, part), BF16),
            pltpu.VMEM((2, 4, half // 2, part), BF16),
            pltpu.VMEM((2, 4, half // 2, part), BF16),
            pltpu.VMEM((2, 4, half // 2, part), BF16),
            dma((2,)),
            dma((2,)),
            dma((2, 2)),
            dma,
            dma((pairs,)),
            dma((4,)),
            dma((4,)),
            dma((2,)),
            dma,
            dma((3,)),
            dma((2,)),
            dma((3,)),
            dma((2,)),
            dma((2,)),
            dma((2,)),
        ],
        compiler_params=pltpu.CompilerParams(collective_id=0, has_side_effects=True),
    )(*args)


def one_kernel(*args, sp, fs, tp):
    rows, width = args[0].shape[1:]
    heads = args[4].shape[1]
    return (
        1 < sp <= 8
        and fs == 4
        and tp == 2
        and rows == LANES
        and args[1].shape[2] == STATE == LANES
        and width == heads * HEAD_DIM
        and args[12].shape[2] == width
        and args[13].shape[2] == 2 * HEAD_DIM
        and heads % 4 == 0
        and args[16].shape == args[17].shape == (width, args[16].shape[1])
        and args[16].shape[1] % (2 * LANES) == 0
    )


def solution(mesh):
    in_specs = (
        P("fs", "sp", "tp"),
        P("fs", "sp", "tp"),
        P("fs", "sp", "tp"),
        P("fs", "sp", "tp"),
        P("fs", "tp", "sp"),
        P("fs", "tp", "sp"),
        P("tp"),
        P("tp"),
        P(None, "tp"),
        P(None, "tp"),
        P(None, "tp"),
        P("tp"),
        P("fs", "sp", "tp"),
        P("fs", "sp", "tp"),
        P("fs", "sp", "tp"),
        P("fs", "sp", "tp"),
        P("tp", "fs"),
        P("tp", "fs"),
    )
    out_specs = P("fs", ("sp", "tp"), None)
    sp, fs, tp = (mesh.shape[name] for name in ("sp", "fs", "tp"))

    def body(*args):
        if one_kernel(*args, sp=sp, fs=fs, tp=tp):
            return fused(sp, fs, *args)
        return shards(*args)

    return jax.shard_map(body, mesh=mesh, in_specs=in_specs, out_specs=out_specs, check_vma=False)
```

```python
import functools
import math

import jax
import jax.numpy as jnp
from jax import lax
from jax.experimental import pallas as pl
from jax.experimental.pallas import tpu as pltpu
from jax.sharding import PartitionSpec as P

HEAD_DIM = 64
STATE = 128


EPSILON = 1e-06
NEGATIVE = -1e30


def passed_along(shard, axis, by):
    devices = lax.axis_size(axis)
    pairs = [(i, i + by) for i in range(devices) if 0 <= i + by < devices]
    return lax.ppermute(shard, axis, pairs)


def entering(shard, axis, join, neutral):
    place = lax.axis_index(axis)
    gathered = jax.tree.map(
        lambda a, kind: lax.all_gather(a.astype(kind), axis), shard, (jnp.bfloat16, jnp.bfloat16)
    )
    state = jax.tree.map(lambda a, e: jnp.zeros_like(a) + jnp.asarray(e, a.dtype), shard, neutral)

    def one(hop, state):
        return join(
            state,
            jax.tree.map(
                lambda a, own: lax.dynamic_index_in_dim(a, hop, 0, False).astype(own.dtype),
                gathered,
                shard,
            ),
        )

    return lax.fori_loop(0, place, one, state)


def causal_filter(feeder_quantities, before, taps):
    length = feeder_quantities.shape[0]
    padded = jnp.concatenate([before, feeder_quantities], axis=0).astype(jnp.float32)
    summed = jnp.zeros(feeder_quantities.shape, jnp.float32)
    for offset in range(taps.shape[0]):
        summed = summed + taps[offset].astype(jnp.float32) * padded[offset : offset + length]
    return jax.nn.silu(summed).astype(jnp.bfloat16)


def compose(earlier, later):
    return (earlier[0] * later[0], earlier[1] * later[0][..., None, None] + later[1])


def shards(
    state_head_inputs,
    state_write_vectors,
    state_read_vectors,
    state_output_gate,
    presoftplus_steps,
    extra_decay_log,
    lane_shrinkage_powers,
    bypass_coefficient_vector,
    feeder_smoothing_stencil,
    stored_smoothing_stencil,
    lookup_smoothing_stencil,
    bundled_rescaling_vector,
    queries,
    attention_keys,
    attention_values,
    forget_gate_cumsum,
    state_out_weight,
    attention_out_weight,
):
    shard_rows = state_head_inputs.shape[1]
    input_rows = state_head_inputs[0]
    write_rows = state_write_vectors[0]
    read_rows = state_read_vectors[0]
    tap_rows = feeder_smoothing_stencil.shape[0] - 1
    value_width = input_rows.shape[1]
    vector_width = write_rows.shape[1]
    tail_rows = jnp.concatenate(
        [input_rows[-tap_rows:], write_rows[-tap_rows:], read_rows[-tap_rows:]], axis=1
    )
    before = passed_along(tail_rows, "sp", 1)
    conv_values = causal_filter(input_rows, before[:, :value_width], feeder_smoothing_stencil)
    conv_write = causal_filter(
        write_rows, before[:, value_width : value_width + vector_width], stored_smoothing_stencil
    )
    conv_read = causal_filter(
        read_rows, before[:, value_width + vector_width :], lookup_smoothing_stencil
    )
    stride_duration = jax.nn.softplus(presoftplus_steps[0])
    shrinkage_natural_power = (
        stride_duration * (-jnp.exp(lane_shrinkage_powers))[:, None] + extra_decay_log[0]
    )
    lane_tally = stride_duration.shape[0]
    groups = vector_width // STATE
    per_group = lane_tally // groups
    cumulative = jnp.cumsum(shrinkage_natural_power, axis=1)
    input_heads = conv_values.reshape(shard_rows, groups, per_group, HEAD_DIM)
    write_groups = conv_write.reshape(shard_rows, groups, STATE)
    read_groups = conv_read.reshape(shard_rows, groups, STATE)
    inner_products = jnp.einsum(
        "tgn,sgn->gts", read_groups, write_groups, preferred_element_type=jnp.float32
    )
    positions = jnp.arange(shard_rows)
    causal = positions[:, None] >= positions[None, :]
    log_gap = jnp.where(causal[None], cumulative[:, :, None] - cumulative[:, None, :], -jnp.inf)
    weights = jnp.exp(log_gap) * stride_duration[:, None, :]
    mix_weights = (
        inner_products[:, None] * weights.reshape(groups, per_group, shard_rows, shard_rows)
    ).astype(jnp.bfloat16)
    local_part = jnp.einsum(
        "ghts,sghp->tghp", mix_weights, input_heads, preferred_element_type=jnp.float32
    )
    end_scale = (jnp.exp(cumulative[:, -1:] - cumulative) * stride_duration).T.reshape(
        shard_rows, groups, per_group
    )
    weighted = (input_heads.astype(jnp.float32) * end_scale[..., None]).astype(jnp.bfloat16)
    block_state = jnp.einsum(
        "sghp,sgn->ghpn", weighted, write_groups, preferred_element_type=jnp.float32
    )
    total_decay = jnp.exp(cumulative[:, -1]).reshape(groups, per_group)
    identity = (jnp.ones_like(total_decay), jnp.zeros_like(block_state))
    carried = entering((total_decay, block_state), "sp", compose, identity)[1]
    carried_part = jnp.einsum(
        "tgn,ghpn->tghp",
        read_groups,
        carried.astype(jnp.bfloat16),
        preferred_element_type=jnp.float32,
    )
    carried_part = (
        carried_part * jnp.exp(cumulative).T.reshape(shard_rows, groups, per_group)[..., None]
    )
    mixer_sum = (
        local_part
        + carried_part
        + bypass_coefficient_vector.reshape(groups, per_group)[None, :, :, None]
        * input_heads.astype(jnp.float32)
    )
    gated_rows = mixer_sum.reshape(shard_rows, groups, per_group * HEAD_DIM) * jax.nn.silu(
        state_output_gate[0].astype(jnp.float32)
    ).reshape(shard_rows, groups, -1)
    stretch_coefficient = lax.rsqrt(
        jnp.mean(gated_rows * gated_rows, axis=-1, keepdims=True) + EPSILON
    )
    state_result = (
        (gated_rows * stretch_coefficient * bundled_rescaling_vector.reshape(groups, -1))
        .reshape(shard_rows, -1)
        .astype(jnp.bfloat16)
    )
    attend_heads = forget_gate_cumsum.shape[2]
    key_group_count = attention_keys.shape[2] // HEAD_DIM
    repeat_factor = attend_heads // key_group_count
    query_head_count = queries[0].reshape(shard_rows, key_group_count, repeat_factor, HEAD_DIM)
    first_query = lax.axis_index("sp") * shard_rows
    query_index = first_query + jnp.arange(shard_rows)
    last_query = first_query + shard_rows - 1
    query_gates = forget_gate_cumsum[0].T
    all_gates = lax.all_gather(forget_gate_cumsum[0], "sp", axis=0, tiled=True)
    attention_score_scale = HEAD_DIM ** (-0.5)
    starting = (
        jnp.full((attend_heads, shard_rows), NEGATIVE, jnp.float32),
        jnp.zeros((attend_heads, shard_rows), jnp.float32),
        jnp.zeros((attend_heads, shard_rows, HEAD_DIM), jnp.float32),
    )
    key_rows = lax.all_gather(attention_keys[0], "sp", axis=0, tiled=True)
    value_rows = lax.all_gather(attention_values[0], "sp", axis=0, tiled=True)
    span = key_rows.shape[0]
    sub_block = math.gcd(span, 512)

    def advance(sub_index, running):
        first_key = sub_index * sub_block

        def attend(running):
            running_max, running_sum, weighted_sum = running
            key_tile = lax.dynamic_slice_in_dim(
                key_rows, sub_index * sub_block, sub_block, 0
            ).reshape(sub_block, key_group_count, HEAD_DIM)
            value_tile = lax.dynamic_slice_in_dim(
                value_rows, sub_index * sub_block, sub_block, 0
            ).reshape(sub_block, key_group_count, HEAD_DIM)
            key_gates = lax.dynamic_slice_in_dim(all_gates, first_key, sub_block, 0)
            attention_scores = jnp.einsum(
                "ezxp,czp->zxec", query_head_count, key_tile, preferred_element_type=jnp.float32
            )
            attention_scores = (
                attention_scores.reshape(attend_heads, shard_rows, sub_block)
                * attention_score_scale
            )
            attention_scores = attention_scores + query_gates[:, :, None] - key_gates.T[:, None, :]
            visible = (first_key + jnp.arange(sub_block))[None, :] <= query_index[:, None]
            attention_scores = jnp.where(visible[None], attention_scores, NEGATIVE)
            new_max = jnp.maximum(running_max, jnp.max(attention_scores, axis=-1))
            shrink = jnp.exp(running_max - new_max)
            attention_probs = jnp.where(
                visible[None], jnp.exp(attention_scores - new_max[..., None]), 0.0
            )
            running_sum = running_sum * shrink + jnp.sum(attention_probs, axis=-1)
            weighted_value_sum = jnp.einsum(
                "fljx,xfc->fljc",
                attention_probs.astype(jnp.bfloat16).reshape(
                    key_group_count, repeat_factor, shard_rows, sub_block
                ),
                value_tile,
                preferred_element_type=jnp.float32,
            )
            weighted_sum = weighted_sum * shrink[..., None] + weighted_value_sum.reshape(
                attend_heads, shard_rows, HEAD_DIM
            )
            return (new_max, running_sum, weighted_sum)

        return lax.cond(first_key <= last_query, attend, lambda kept: kept, running)

    _, running_sum, weighted_sum = lax.fori_loop(0, span // sub_block, advance, starting)
    attend_out = (
        (weighted_sum / running_sum[..., None])
        .transpose(1, 0, 2)
        .reshape(shard_rows, -1)
        .astype(jnp.bfloat16)
    )
    state_columns, attend_columns = (
        lax.all_gather(state_out_weight, "fs", axis=1, tiled=True),
        lax.all_gather(attention_out_weight, "fs", axis=1, tiled=True),
    )
    summed = lax.psum_scatter(
        (
            jnp.dot(state_result, state_columns, preferred_element_type=jnp.float32)
            + jnp.dot(attend_out, attend_columns, preferred_element_type=jnp.float32)
        ).astype(jnp.bfloat16),
        "tp",
        scatter_dimension=0,
        tiled=True,
    )
    return summed[None]


MESH = pl.DeviceIdType.MESH
LANES = 128
BF16, F32 = jnp.bfloat16, jnp.float32


def mixer_kernel(
    sp,
    fs,
    x_far,
    w_far,
    r_far,
    gate_far,
    step_far,
    extra_far,
    shrink_far,
    bypass_far,
    tapx_far,
    tapw_far,
    tapr_far,
    gain_far,
    q_far,
    k_far,
    v_far,
    forget_far,
    wst_far,
    wat_far,
    out_ref,
    x_ref,
    w_ref,
    r_ref,
    gate_ref,
    step_ref,
    extra_ref,
    shrink_ref,
    bypass_ref,
    tapx_ref,
    tapw_ref,
    tapr_ref,
    gain_ref,
    q_ref,
    forget_ref,
    load_sem,
    ready,
    pad_ref,
    tails,
    conv,
    soft_cum,
    end_wide,
    kvall,
    gall,
    qs,
    early,
    peaks,
    own_state,
    state_in,
    state_out,
    mix,
    wst,
    wat,
    wst_y,
    wat_x,
    acts_mine,
    acts_in,
    pieces_mine,
    pieces_in,
    scales_mine,
    scales_in,
    acc,
    att_out,
    att_in,
    sum_out,
    sum_in,
    tail_sem,
    kv_send,
    kv_recv,
    st_send,
    st_recv,
    weight_send,
    weight_recv,
    peer_recv,
    act_send,
    act_recv,
    piece_send,
    piece_recv,
    scale_recv,
    sum_send,
    sum_recv,
):
    me = lax.axis_index("sp")
    f = lax.axis_index("fs")
    t = lax.axis_index("tp")
    rows, width = x_ref.shape[1], x_ref.shape[2]
    heads = step_ref.shape[1]
    kv_width = k_far.shape[2]
    kv_heads = kv_width // HEAD_DIM
    repeat = heads // kv_heads
    pairs = heads // 2
    taps = tapx_ref.shape[0]
    cols = wst_far.shape[1]
    part = cols // 2
    half = rows // 2
    peer = {"tp": 1 - t}

    barrier = pltpu.get_barrier_semaphore()
    for d in (1, 2):
        for r in range(2):
            pl.semaphore_signal(
                barrier, inc=1, device_id={"fs": f ^ d, "tp": r}, device_id_type=MESH
            )
    pl.semaphore_signal(barrier, inc=1, device_id=peer, device_id_type=MESH)
    for d in range(1, sp):

        @pl.when(me + d < sp)
        def _(d=d):
            pl.semaphore_signal(barrier, inc=1, device_id={"sp": me + d}, device_id_type=MESH)

    @pl.when(me > 0)
    def _():
        pl.semaphore_signal(barrier, inc=1, device_id={"sp": me - 1}, device_id_type=MESH)

    near = {
        "x": (x_far, x_ref),
        "w": (w_far, w_ref),
        "r": (r_far, r_ref),
        "tapx": (tapx_far, tapx_ref),
        "tapw": (tapw_far, tapw_ref),
        "tapr": (tapr_far, tapr_ref),
        "k": (k_far.at[0], kvall.at[me, :, 0:kv_width]),
        "v": (v_far.at[0], kvall.at[me, :, kv_width:]),
        "wat": (wat_far, wat.at[t]),
        "wst": (wst_far, wst.at[t]),
        "step": (step_far, step_ref),
        "extra": (extra_far, extra_ref),
        "shrink": (shrink_far, shrink_ref),
        "forget": (forget_far, forget_ref),
        "q": (q_far, q_ref),
        "gate": (gate_far, gate_ref),
        "gain": (gain_far, gain_ref),
        "bypass": (bypass_far, bypass_ref),
    }
    shared = {"v": "k", "wst": "wat"}
    places = [name for name in near if name not in shared]
    loads = {
        name: pltpu.make_async_copy(
            far, here, load_sem.at[places.index(shared.get(name, name))]
        )
        for name, (far, here) in near.items()
    }
    for load in loads.values():
        load.start()

    def loaded(*names):
        for name in names:
            loads[name].wait()

    def remote(src, dst, send, recv, where):
        return pltpu.make_async_remote_copy(
            src_ref=src,
            dst_ref=dst,
            send_sem=send,
            recv_sem=recv,
            device_id=where,
            device_id_type=MESH,
        )

    def arrived(ref, sem):
        remote(ref, ref, sem, sem, peer).wait_recv()

    def departed(ref, sem):
        remote(ref, ref, sem, sem, peer).wait_send()

    lane = lax.broadcasted_iota(jnp.int32, (1, LANES), 1)
    low = lane < HEAD_DIM
    row_id = lax.broadcasted_iota(jnp.int32, (rows, rows), 0)
    col_id = lax.broadcasted_iota(jnp.int32, (rows, rows), 1)

    def expand(columns, j):
        return jnp.where(low, columns[:, 2 * j : 2 * j + 1], columns[:, 2 * j + 1 : 2 * j + 2])

    inputs = (
        (x_ref, tapx_ref, slice(0, width)),
        (w_ref, tapw_ref, slice(width, width + STATE)),
        (r_ref, tapr_ref, slice(width + STATE, width + 2 * STATE)),
    )

    def filtered(count):
        for _, tap_ref, at in inputs:
            total = jnp.zeros((count, at.stop - at.start), F32)
            for i in range(taps):
                first = 8 - (taps - 1) + i
                total = total + tap_ref[i : i + 1, :].astype(F32) * pad_ref[first : first + count, at]
            conv[0:count, at] = (total * jax.nn.sigmoid(total)).astype(BF16)

    pad_ref[0:8, :] = jnp.zeros((8, pad_ref.shape[1]), F32)
    loaded("x", "w", "r", "tapx", "tapw", "tapr")
    for ref, _, at in inputs:
        pad_ref[8 : 8 + rows, at] = ref[0].astype(F32)
    filtered(rows)

    def decay():
        loaded("step", "extra", "shrink")
        head_row = lax.broadcasted_iota(jnp.int32, (heads, rows), 0)
        power = jnp.zeros((heads, rows), F32)
        for h in range(heads):
            power = jnp.where(head_row == h, shrink_ref[h], power)
        presoft = step_ref[0]
        step = jnp.maximum(presoft, 0.0) + jnp.log1p(jnp.exp(-jnp.abs(presoft)))
        log_decay = extra_ref[0] - jnp.exp(power) * step
        upper = (row_id <= col_id).astype(F32)
        cum = jnp.dot(log_decay, upper, precision=lax.Precision.HIGHEST, preferred_element_type=F32)
        soft_cum[0] = step
        soft_cum[1] = cum
        end_scale = (jnp.exp(cum[:, rows - 1 : rows] - cum) * step).T
        for j in range(pairs):
            end_wide[:, j * LANES : (j + 1) * LANES] = expand(end_scale, j)

    def own_states():
        turned_write = conv[:, width : width + STATE].astype(F32).T.astype(BF16)
        for p in range(pairs):
            at = slice(p * LANES, (p + 1) * LANES)
            weighted = (conv[:, at].astype(F32) * end_wide[:, at]).astype(BF16)
            own_state[p] = jnp.dot(turned_write, weighted, preferred_element_type=F32)

    @pl.when(me == 0)
    def _():
        state_in[...] = jnp.zeros(state_in.shape, BF16)
        decay()
        own_states()
        for p in range(pairs):
            state_out[p] = own_state[p].astype(BF16)

    follows = me + 1 < sp
    pl.semaphore_wait(barrier, 5 + me + jnp.where(follows, 1, 0))

    for d in range(2, sp):

        @pl.when(me - d >= 0)
        def _(d=d):
            pl.semaphore_signal(
                ready.at[d - 2], inc=1, device_id={"sp": me - d}, device_id_type=MESH
            )

    deep = wst_far.shape[0]
    lent = deep * 3 // 16 // 16 * 16
    ends = (0, lent, 2 * lent, deep * 7 // 8, deep)
    chunks = [slice(ends[c], ends[c + 1]) for c in range(4)]
    odd = lax.rem(me, 2) == 1
    even = jnp.logical_not(odd)
    top = me == sp - 1

    def weight_copies(chunk):
        at = (t, chunks[chunk])
        return [
            remote(
                src.at[at],
                dst.at[at],
                weight_send.at[0],
                weight_recv.at[chunk],
                {"fs": f ^ hop},
            )
            for src, dst, hop in ((wat, wat_x, 1), (wst, wst_y, 2))
        ]

    def own_copies():
        return [
            remote(w.at[t], w.at[t], weight_send.at[1], peer_recv.at[0], peer) for w in (wat, wst)
        ]

    def landed(chunk):
        arrived(wat_x.at[:, chunks[chunk]], weight_recv.at[chunk])

    def relay(chunk):
        for w in (wat_x, wst_y):
            at = (t, chunks[chunk])
            remote(w.at[at], w.at[at], weight_send.at[2], peer_recv.at[1], peer).start()

    def lend(chunk):
        at = (t, chunks[chunk])
        return [
            remote(
                w.at[at],
                w.at[at],
                weight_send.at[3],
                weight_recv.at[chunk],
                {"sp": lax.rem(me + sp - 1, sp)},
            )
            for w in (wat_x, wst_y)
        ]

    pltpu.make_async_copy(wst, wst, load_sem.at[places.index("wat")]).wait()
    for chunk, fits in (
        (0, odd),
        (1, even),
        (0, jnp.logical_and(even, top)),
        (1, jnp.logical_and(odd, top)),
        (2, me >= 0),
        (3, me >= 0),
    ):

        @pl.when(fits)
        def _(chunk=chunk):
            for copy in weight_copies(chunk):
                copy.start()

    for copy in own_copies():
        copy.start()

    @pl.when(me > 0)
    def _():
        decay()

    step, cum = soft_cum[0], soft_cum[1]
    decays = jnp.broadcast_to(jnp.exp(cum[:, rows - 1 : rows]), (heads, LANES))

    def state_copy(p):
        there = {"sp": lax.rem(me + 1, sp)}
        return remote(state_out.at[p], state_in.at[p], st_send, st_recv.at[p], there)

    pltpu.make_async_copy(kvall.at[me], kvall.at[me], load_sem.at[places.index("k")]).wait()
    loaded("forget")
    gall[me] = forget_ref[0]
    gate_cols = forget_ref[0].T

    tail = [
        remote(
            ref.at[0, rows - 8 : rows, :],
            tails.at[:, at],
            tail_sem.at[0],
            tail_sem.at[1],
            {"sp": lax.rem(me + 1, sp)},
        )
        for ref, _, at in inputs
    ]

    def kv_copies(d, source, kind):
        there = {"sp": lax.rem(me + d, sp)}
        return [
            remote(kvall.at[source], kvall.at[source], kv_send.at[0], kv_recv.at[kind, 0], there),
            remote(gall.at[source], gall.at[source], kv_send.at[1], kv_recv.at[kind, 1], there),
        ]

    @pl.when(follows)
    def _():
        for copy in tail:
            copy.start()

    @pl.when(me == 0)
    def _():
        for p in range(pairs):
            state_copy(p).start()

    @pl.when(follows)
    def _():
        for copy in kv_copies(1, me, jnp.where(me == 0, 2, 0)):
            copy.start()

    def far_kv(fits):
        for d in range(2, sp):

            @pl.when(jnp.logical_and(fits, me + d < sp))
            def _(d=d):
                pl.semaphore_wait(ready.at[d - 2], 1)

                @pl.when(jnp.logical_or(me == 0, d > 2))
                def _():
                    for copy in kv_copies(d, me, jnp.where(me == 0, 2, 1)):
                        copy.start()

    far_kv(me > 0)

    for j in range(1, sp):

        @pl.when(j > me)
        def _(j=j):
            kvall[j] = jnp.zeros(kvall.shape[1:], BF16)
            gall[j] = jnp.zeros(gall.shape[1:], F32)

    loaded("q")
    for h in range(heads):
        kv = h // repeat
        piece = (q_ref[0, :, h * HEAD_DIM : (h + 1) * HEAD_DIM].astype(F32) * HEAD_DIM**-0.5).astype(
            BF16
        )
        zero = jnp.zeros((rows, HEAD_DIM), BF16)
        parts = [piece if i == kv else zero for i in range(kv_heads)]
        qs[kv, (h % repeat) * rows : (h % repeat + 1) * rows, :] = jnp.concatenate(parts, axis=1)

    loaded("gate", "gain", "bypass")
    exp_cum = jnp.exp(cum).T
    cum_col = cum.T

    def within():
        conv_write = conv[:, width : width + STATE]
        conv_read = conv[:, width + STATE :]
        inner = lax.dot_general(
            conv_read, conv_write, (((1,), (1,)), ((), ())), preferred_element_type=F32
        )
        causal = row_id >= col_id
        for j in range(pairs):
            tile = conv[:, j * LANES : (j + 1) * LANES]
            parts = []
            for h in (2 * j, 2 * j + 1):
                gap = jnp.where(causal, cum_col[:, h : h + 1] - cum[h : h + 1, :], NEGATIVE)
                weights = (inner * (jnp.exp(gap) * step[h : h + 1, :])).astype(BF16)
                parts.append(jnp.dot(weights, tile, preferred_element_type=F32))
            bypass = jnp.where(low, bypass_ref[2 * j], bypass_ref[2 * j + 1])
            mix[:, j * LANES : (j + 1) * LANES] = (
                jnp.where(low, parts[0], parts[1]) + bypass * tile.astype(F32)
            )

    @pl.when(me > 0)
    def _():
        arrived(tails, tail_sem.at[1])
        pad_ref[0:8, :] = tails[...].astype(F32)
        filtered(16)
        own_states()

    @pl.when(me != 1)
    def _():
        within()

    def pass_state(which):
        for p in which:
            state_copy(p).wait_recv()
            decay = jnp.where(low, decays[2 * p : 2 * p + 1, :], decays[2 * p + 1 : 2 * p + 2, :])
            state_out[p] = (state_in[p].astype(F32) * decay + own_state[p]).astype(BF16)
            state_copy(p).start()

    @pl.when(jnp.logical_and(me == 1, follows))
    def _():
        pass_state(range(pairs))

    @pl.when(me == 1)
    def _():
        within()

    for chunk, parity in ((0, odd), (1, even)):

        @pl.when(jnp.logical_and(parity, me > 0))
        def _(chunk=chunk):
            landed(chunk)
            for copy in lend(chunk):
                copy.start()
            relay(chunk)

    @pl.when(me > 1)
    def _():
        arrived(kvall.at[0], kv_recv.at[0, 0])
        arrived(gall.at[0], kv_recv.at[0, 1])

    @pl.when(jnp.logical_and(me > 1, follows))
    def _():
        for copy in kv_copies(1, me - 1, 1):
            copy.start()

    for j in range(3, sp):

        @pl.when(me == j)
        def _(j=j):
            arrived(kvall.at[0 : j - 2], kv_recv.at[1, 0])
            arrived(gall.at[0 : j - 2], kv_recv.at[1, 1])

    visible = [j * rows + col_id <= me * rows + row_id for j in range(sp)]

    def scored(kv, blocks):
        own = lane // HEAD_DIM == kv
        count = (blocks[-1] + 1 - blocks[0]) * rows
        span = slice(blocks[0], blocks[-1] + 1)
        keys = kvall[span, :, 0:kv_width].reshape(count, -1)
        values = kvall[span, :, kv_width:].reshape(count, -1)
        scores = lax.dot_general(
            qs[kv], keys, (((1,), (1,)), ((), ())), preferred_element_type=F32
        )
        heads_tiles = []
        for i in range(repeat):
            h = kv * repeat + i
            gate_col = gate_cols[:, h : h + 1]
            heads_tiles.append(
                [
                    jnp.where(
                        visible[j],
                        scores[i * rows : (i + 1) * rows, n * rows : (n + 1) * rows]
                        + (gate_col - gall[j, h : h + 1, :]),
                        NEGATIVE,
                    )
                    for n, j in enumerate(blocks)
                ]
            )
        return heads_tiles, jnp.where(own, values, jnp.ones_like(values))

    for kv in range(kv_heads):
        heads_tiles, summed_values = scored(kv, list(range(1, sp)))
        for i, tiles in enumerate(heads_tiles):
            peak = jnp.max(functools.reduce(jnp.maximum, tiles), axis=1, keepdims=True)
            probs = jnp.concatenate([jnp.exp(tile - peak).astype(BF16) for tile in tiles], axis=1)
            early[kv * repeat + i] = jnp.dot(
                probs, summed_values, preferred_element_type=F32
            )
            peaks[kv * repeat + i] = jnp.broadcast_to(peak, (rows, LANES))

    quarter = half // 2
    spans = (slice(0, quarter), slice(quarter, half))

    def spread(src, dst, send, recv, hop, q):
        return [
            remote(
                src.at[r, spans[q]],
                dst.at[2 + t, spans[q]],
                send,
                recv.at[1 + q],
                {"fs": f ^ hop, "tp": r},
            )
            for r in range(2)
        ]

    def across(src, dst, send, recv):
        return remote(src.at[1 - t], dst.at[t], send, recv.at[0], peer)

    def second_quarter(p):
        for copy in spread(pieces_mine.at[p], pieces_in.at[p], piece_send.at[0], piece_recv, 1, 1):
            copy.start()

    def state_part():
        conv_read = conv[:, width + STATE :]
        squares = []
        for p in range(pairs):
            at = slice(p * LANES, (p + 1) * LANES)

            @pl.when(me == sp - 1)
            def _(p=p):
                state_copy(p).wait_recv()

            carried = jnp.dot(conv_read, state_in[p], preferred_element_type=F32)
            gate = gate_ref[0, :, at].astype(F32)
            u = (mix[:, at] + carried * expand(exp_cum, p)) * (gate * jax.nn.sigmoid(gate))
            squares.append(u * u)
            sent = (u * gain_ref[0:1, at]).astype(BF16)
            for r in range(2):
                pieces_mine[p, r] = sent[r * half : (r + 1) * half]
            for copy in spread(pieces_mine.at[p], pieces_in.at[p], piece_send.at[0], piece_recv, 1, 0):
                copy.start()
            across(pieces_mine.at[p], pieces_in.at[p], piece_send.at[0], piece_recv).start()

            @pl.when(top)
            def _(p=p):
                second_quarter(p)

        total = functools.reduce(jnp.add, squares)
        coarse = total.astype(BF16)
        fine = (total - coarse.astype(F32)).astype(BF16)
        mean = (
            lax.dot_general(
                jnp.ones((8, 2 * LANES), BF16),
                jnp.concatenate([coarse, fine], axis=1),
                (((1,), (1,)), ((), ())),
                preferred_element_type=F32,
            )
            / width
        )
        scale = lax.rsqrt(mean + EPSILON)
        scales_mine[0] = scale
        scales_mine[1] = pltpu.roll(scale, half, 1)
        for r in range(2):
            remote(
                scales_mine.at[r],
                scales_in.at[2 + t],
                piece_send.at[1],
                scale_recv.at[1],
                {"fs": f ^ 1, "tp": r},
            ).start()
        across(scales_mine, scales_in, piece_send.at[1], scale_recv).start()

        @pl.when(jnp.logical_not(top))
        def _():
            for p in range(pairs):
                second_quarter(p)

    middle = jnp.logical_and(me > 1, follows)
    ahead = jnp.logical_and(middle, t == 1)
    amid = jnp.logical_and(middle, t == 0)

    @pl.when(ahead)
    def _():
        pass_state(range(pairs))
        state_part()

    @pl.when(me > 0)
    def _():
        arrived(kvall.at[0], kv_recv.at[2, 0])
        arrived(gall.at[0], kv_recv.at[2, 1])

    for kv in range(kv_heads):
        heads_tiles, summed_values = scored(kv, [0])
        outs = []
        for i, (tile,) in enumerate(heads_tiles):
            h = kv * repeat + i
            before = peaks[h]
            peak = jnp.maximum(before, jnp.max(tile, axis=1, keepdims=True))
            probs = jnp.exp(tile - peak).astype(BF16)
            both = early[h] * jnp.exp(before - peak) + jnp.dot(
                probs, summed_values, preferred_element_type=F32
            )
            turned = pltpu.roll(both, HEAD_DIM, 1)
            outs.append(both / turned if h % 2 == kv else turned / both)
        for i in range(0, repeat, 2):
            at = slice((kv * repeat + i) * HEAD_DIM, (kv * repeat + i + 2) * HEAD_DIM)
            merged = jnp.where(low, outs[i], outs[i + 1]).astype(BF16)
            for r in range(2):
                acts_mine[r, :, at] = merged[r * half : (r + 1) * half]

    @pl.when(amid)
    def _():
        pass_state(range(pairs))

    for q in range(2):
        for copy in spread(acts_mine, acts_in, act_send, act_recv, 2, q):
            copy.start()
    across(acts_mine, acts_in, act_send, act_recv).start()

    def relay_middle():
        for chunk, parity in ((1, odd), (0, even)):

            @pl.when(jnp.logical_and(parity, top))
            def _(chunk=chunk):
                landed(chunk)
                relay(chunk)

        @pl.when(me == 0)
        def _():
            landed(1)
            relay(1)

        landed(2)
        relay(2)

    @pl.when(jnp.logical_not(ahead))
    def _():
        state_part()

    acts_in[t] = acts_mine[t]
    for p in range(pairs):
        pieces_in[p, t] = pieces_mine[p, t]
    scales_in[t] = scales_mine[t]

    def place(owner, h, values):
        at = pl.ds(pl.multiple_of(owner * cols + h * part, part), part)
        out_ref[0, :, at] = values.astype(BF16)

    def halves(weights):
        return [(weights, slice(h * part, (h + 1) * part)) for h in range(2)]

    def attended(blocks, weights, at):
        left = jnp.concatenate(
            [
                jnp.concatenate([acts_in[slot + s, span] for slot, span in blocks], axis=0)
                for s in range(2)
            ],
            axis=1,
        )
        right = jnp.concatenate([weights[s, :, at] for s in range(2)], axis=0)
        return jnp.dot(left, right, preferred_element_type=F32)

    def mixed(blocks, by, weights, at):
        sums = []
        for s in range(2):
            left = jnp.concatenate(
                [
                    jnp.concatenate([pieces_in[p, slot + s, span] for slot, span in blocks], axis=0)
                    for p in range(pairs)
                ],
                axis=1,
            )
            scale = jnp.concatenate([b[s] for b in by], axis=0)
            sums.append(jnp.dot(left, weights[s, :, at], preferred_element_type=F32) * scale)
        return sums[0] + sums[1]

    whole = slice(0, half)

    def own_product():
        by = columns_of(0)
        for h in range(2):
            attention = attended(((0, whole),), *halves(wat)[h])
            place(f, h, attention + mixed(((0, whole),), (by,), *halves(wst)[h]))

    def columns_of(slot):
        upright = scales_in[slot : slot + 2].reshape(2 * 8, rows).T
        return [upright[0:half, 8 * s : 8 * s + 1] for s in range(2)]

    arrived(wst, peer_recv.at[0])

    @pl.when(jnp.logical_not(top))
    def _():
        arrived(acts_in.at[0], act_recv.at[0])
        arrived(pieces_in.at[:, 0], piece_recv.at[0])
        arrived(scales_in.at[0], scale_recv.at[0])
        own_product()

    far_kv(me == 0)
    relay_middle()

    landed(3)
    relay(3)

    for chunk, parity in ((0, even), (1, odd)):

        @pl.when(jnp.logical_and(parity, jnp.logical_not(top)))
        def _(chunk=chunk):
            landed(chunk)
            relay(chunk)

    def back(out, landing, qs, picked, i, hop):
        at = (slice(qs[0], qs[-1] + 1), slice(picked[0], picked[-1] + 1))
        return remote(out.at[at], landing.at[at], sum_send.at[i], sum_recv.at[i], {"fs": f ^ hop})

    def span_of(qs):
        return slice(spans[qs[0]].start, spans[qs[-1]].stop)

    def put(out, qs, g, product):
        for q in qs:
            start = (q - qs[0]) * quarter
            out[q, g] = product[start : start + quarter].astype(BF16)

    def attended_step(qs, picked):
        if 0 in picked:
            for q in qs:
                arrived(acts_in.at[2:4, spans[q]], act_recv.at[1 + q])
        there = (2, span_of(qs))
        pairings = halves(wat) + halves(wat_x)
        for g in picked:
            if 0 in qs and g >= 2:
                product = attended(((0, whole), there), *pairings[g])
                acc[g - 2] = product[0:half]
                product = product[half:]
            else:
                product = attended((there,), *pairings[g])
            put(att_out, qs, g, product)
        back(att_out, att_in, qs, picked, 0, 2).start()

    def mixed_step(qs, picked):
        if 0 in picked:
            for q in qs:
                arrived(pieces_in.at[:, 2:4, spans[q]], piece_recv.at[1 + q])
            if 0 in qs:
                arrived(scales_in.at[2:4], scale_recv.at[1])
        there = (2, span_of(qs))
        by = [column[span_of(qs)] for column in columns_of(2)]
        pairings = halves(wst) + halves(wst_y)
        for g in picked:
            if 0 in qs and g >= 2:
                product = mixed(((0, whole), there), (columns_of(0), by), *pairings[g])
                acc[g] = product[0:half]
                product = product[half:]
            else:
                product = mixed((there,), (by,), *pairings[g])
            put(sum_out, qs, g, product)
        back(sum_out, sum_in, qs, picked, 1, 1).start()

    low_groups, high_groups = (0, 1), (2, 3)

    @pl.when(jnp.logical_not(top))
    def _():
        mixed_step((0,), low_groups)
        attended_step((0,), low_groups)
        arrived(wat, peer_recv.at[1])
        mixed_step((0,), high_groups)
        attended_step((0,), high_groups)
        mixed_step((1,), low_groups)
        mixed_step((1,), high_groups)
        attended_step((1,), low_groups)
        attended_step((1,), high_groups)

    @pl.when(top)
    def _():
        attended_step((0, 1), low_groups)
        arrived(wat, peer_recv.at[1])
        arrived(acts_in.at[0], act_recv.at[0])
        attended_step((0, 1), high_groups)
        mixed_step((0, 1), low_groups)
        arrived(pieces_in.at[:, 0], piece_recv.at[0])
        arrived(scales_in.at[0], scale_recv.at[0])
        mixed_step((0, 1), high_groups)
        own_product()

    def joined(ref, g):
        return jnp.concatenate([ref[q, g] for q in range(2)], axis=0).astype(F32)

    arrived(att_in, sum_recv.at[0])
    for h in range(2):
        place(f ^ 2, h, acc[2 + h] + joined(att_in, h))
    arrived(sum_in, sum_recv.at[1])
    for h in range(2):
        place(f ^ 1, h, acc[h] + joined(sum_in, h))
        place(f ^ 3, h, joined(att_in, 2 + h) + joined(sum_in, 2 + h))

    @pl.when(follows)
    def _():
        departed(tails, tail_sem.at[0])
        departed(state_out, st_send)

    for j in range(sp - 1):
        n = sum(1 for d in range(1, sp - j) if d != 2 or j == 0) + (j > 1)

        @pl.when(me == j)
        def _(n=n):
            departed(kvall.at[0:n], kv_send.at[0])
            departed(gall.at[0:n], kv_send.at[1])

    @pl.when(top)
    def _():
        departed(wat, weight_send.at[0])

    @pl.when(jnp.logical_not(top))
    def _():
        departed(wat.at[:, lent:], weight_send.at[0])

    departed(wst, weight_send.at[1])
    departed(wst, weight_send.at[2])

    @pl.when(me > 0)
    def _():
        departed(wat.at[:, chunks[0]], weight_send.at[3])

    departed(acts_in.at[0:3], act_send)
    departed(pieces_in.at[:, 0:3], piece_send.at[0])
    departed(scales_in.at[0:3], piece_send.at[1])
    departed(att_out, sum_send.at[0])
    departed(sum_out, sum_send.at[1])


def fused(sp, fs, *args):
    rows, width = args[0].shape[1:]
    heads = args[4].shape[1]
    deep, cols = args[16].shape
    half, part = rows // 2, cols // 2
    args = list(args)
    args[11] = args[11].reshape(1, -1)
    args[15] = jnp.swapaxes(args[15], 1, 2)
    far = pl.BlockSpec(memory_space=pl.ANY)
    dma = pltpu.SemaphoreType.DMA
    kv_width = args[13].shape[2]
    kv_heads = kv_width // HEAD_DIM
    pairs = heads // 2
    near = [
        (pltpu.SMEM if i in (6, 7) else pltpu.VMEM)(a.shape, a.dtype)
        for i, a in enumerate(args[:16])
        if i not in (13, 14)
    ]
    return pl.pallas_call(
        functools.partial(mixer_kernel, sp, fs),
        out_shape=pltpu.VMEM((1, half, cols * fs), BF16),
        in_specs=[far] * len(args),
        out_specs=pl.BlockSpec(memory_space=pltpu.VMEM),
        scratch_shapes=near
        + [
            dma((len(args) - 2,)),
            pltpu.SemaphoreType.REGULAR((max(sp - 2, 1),)),
            pltpu.VMEM((8 + rows, width + 2 * STATE), F32),
            pltpu.VMEM((8, width + 2 * STATE), BF16),
            pltpu.VMEM((rows, width + 2 * STATE), BF16),
            pltpu.VMEM((2, heads, rows), F32),
            pltpu.VMEM((rows, width), F32),
            pltpu.VMEM((sp, rows, 2 * kv_width), BF16),
            pltpu.VMEM((sp, heads, rows), F32),
            pltpu.VMEM((kv_heads, heads // kv_heads * rows, kv_width), BF16),
            pltpu.VMEM((heads, rows, LANES), F32),
            pltpu.VMEM((heads, rows, LANES), F32),
            pltpu.VMEM((pairs, STATE, LANES), F32),
            pltpu.VMEM((pairs, STATE, LANES), BF16),
            pltpu.VMEM((pairs, STATE, LANES), BF16),
            pltpu.VMEM((rows, width), F32),
            pltpu.VMEM((2, deep, cols), BF16),
            pltpu.VMEM((2, deep, cols), BF16),
            pltpu.VMEM((2, deep, cols), BF16),
            pltpu.VMEM((2, deep, cols), BF16),
            pltpu.VMEM((2, half, width), BF16),
            pltpu.VMEM((4, half, width), BF16),
            pltpu.VMEM((pairs, 2, half, LANES), BF16),
            pltpu.VMEM((pairs, 4, half, LANES), BF16),
            pltpu.VMEM((2, 8, rows), F32),
            pltpu.VMEM((4, 8, rows), F32),
            pltpu.VMEM((4, half, part), F32),
            pltpu.VMEM((2, 4, half // 2, part), BF16),
            pltpu.VMEM((2, 4, half // 2, part), BF16),
            pltpu.VMEM((2, 4, half // 2, part), BF16),
            pltpu.VMEM((2, 4, half // 2, part), BF16),
            dma((2,)),
            dma((2,)),
            dma((3, 2)),
            dma,
            dma((pairs,)),
            dma((4,)),
            dma((4,)),
            dma((2,)),
            dma,
            dma((3,)),
            dma((2,)),
            dma((3,)),
            dma((2,)),
            dma((2,)),
            dma((2,)),
        ],
        compiler_params=pltpu.CompilerParams(collective_id=0, has_side_effects=True),
    )(*args)


def one_kernel(*args, sp, fs, tp):
    rows, width = args[0].shape[1:]
    heads = args[4].shape[1]
    return (
        1 < sp <= 8
        and fs == 4
        and tp == 2
        and rows == LANES
        and args[1].shape[2] == STATE == LANES
        and width == heads * HEAD_DIM
        and args[12].shape[2] == width
        and args[13].shape[2] == 2 * HEAD_DIM
        and heads % 4 == 0
        and args[16].shape == args[17].shape == (width, args[16].shape[1])
        and args[16].shape[1] % (2 * LANES) == 0
    )


def solution(mesh):
    in_specs = (
        P("fs", "sp", "tp"),
        P("fs", "sp", "tp"),
        P("fs", "sp", "tp"),
        P("fs", "sp", "tp"),
        P("fs", "tp", "sp"),
        P("fs", "tp", "sp"),
        P("tp"),
        P("tp"),
        P(None, "tp"),
        P(None, "tp"),
        P(None, "tp"),
        P("tp"),
        P("fs", "sp", "tp"),
        P("fs", "sp", "tp"),
        P("fs", "sp", "tp"),
        P("fs", "sp", "tp"),
        P("tp", "fs"),
        P("tp", "fs"),
    )
    out_specs = P("fs", ("sp", "tp"), None)
    sp, fs, tp = (mesh.shape[name] for name in ("sp", "fs", "tp"))

    def body(*args):
        if one_kernel(*args, sp=sp, fs=fs, tp=tp):
            return fused(sp, fs, *args)
        return shards(*args)

    return jax.shard_map(body, mesh=mesh, in_specs=in_specs, out_specs=out_specs, check_vma=False)
```
